32 devices in a mesh: rep: 2 (over x), fs: 8 (over z, y), tp: 2 (over core).
Axes of the slice: x: 2, y: 2, z: 4, core: 2. Of those that a mesh axis runs over, the one named last changes fastest.
Arguments:
- stream: bfloat16 [8192, 2048], P(('rep', 'fs'), 'tp'), may hold values from -6 to 6
- recurrent_norm_gain: float32 [2048], replicated, may hold values from 0.1 to 1.9
- feedforward_norm_gain: float32 [2048], replicated, may hold values from 0.1 to 1.9
- recurrent_input_weight: bfloat16 [2048, 2048], P('fs', 'tp'), may hold values from -0.125 to 0.125
- output_gate_weight: bfloat16 [2048, 2048], P('fs', 'tp'), may hold values from -0.125 to 0.125
- causal_filter_weight: bfloat16 [4, 2048], P(None, 'tp'), may hold values from -3 to 3
- decay_gate_matrix: bfloat16 [32, 64, 64], P('tp'), may hold values from -0.75 to 0.75
- input_gate_matrix: bfloat16 [32, 64, 64], P('tp'), may hold values from -0.75 to 0.75
- channel_decay_param: float32 [2048], P('tp'), may hold values from 3 to 10
- token_decay_offset: float32 [8192, 2048], P(('rep', 'fs'), 'tp'), may hold values from -0.7 to 0, as said below
- recurrent_output_weight: bfloat16 [2048, 2048], P('tp', 'fs'), may hold values from -0.125 to 0.125
- up_projection_weight: bfloat16 [2048, 6144], P('fs', 'tp'), may hold values from -0.125 to 0.125
- down_projection_weight: bfloat16 [6144, 2048], P('tp', 'fs'), may hold values from -0.078125 to 0.078125
Outputs:
- updated: bfloat16 [8192, 2048], P(('rep', 'fs'), 'tp')
The draws below stay inside these ranges and needn't reach their ends.
Inputs may be any that keep to these rules, and one draw needn't show every extreme that they name: `token_decay_offset`: zero except at a few positions, where a whole row is negative.
All inputs are finite; a program needn't handle non-finite values.
Results may differ from the reference program's by a relative error of at most 0.015.
Values may be sent and summed in bfloat16 or wider, within the bound.
A program may use at most 128 MiB of HBM per device.

```python
import jax
import jax.numpy as jnp
from jax import lax

D = 2048
FF = 6144
BLOCK = 64
CONV = 4
SEQ_LEN = 128
TOKENS = 8192
BLOCKS = 32
N_TP = 2


def draw_channel_decay_param(key, part):
    kind_key = jax.random.fold_in(key, 11)
    slow_key = jax.random.fold_in(key, 12)
    fast_key = jax.random.fold_in(key, 13)
    fast = jax.random.uniform(kind_key, (D,), jnp.float32) < 0.5
    slow_rate = jnp.exp(jax.random.uniform(slow_key, (D,), jnp.float32, jnp.log(0.3), jnp.log(3.0))) / SEQ_LEN
    fast_rate = jnp.exp(jax.random.uniform(fast_key, (D,), jnp.float32, jnp.log(0.1), jnp.log(0.3)))
    rate = jnp.where(fast, fast_rate, slow_rate)
    return (-jnp.log(jnp.expm1(rate / 8.0))).astype(jnp.float32)


def draw_token_decay_offset(key, part):
    where_key = jax.random.fold_in(key, 21)
    depth_key = jax.random.fold_in(key, 22)
    hits = jax.random.uniform(where_key, (TOKENS, 1), jnp.float32) < 3.0 / SEQ_LEN
    depth = jax.random.uniform(depth_key, (TOKENS, D), jnp.float32, 0.22, 0.69)
    return jnp.where(hits, -depth, 0.0).astype(jnp.float32)


def block_scale(own_key, shape, cuts, least, high):
    loudness = 1.0
    for position, blocks in cuts:
        heights = jax.random.uniform(jax.random.fold_in(jax.random.fold_in(own_key, 6), position), (blocks,), jnp.float32, least / len(cuts), high / len(cuts))
        loudness = loudness * jnp.repeat(jnp.exp(heights), shape[position] // blocks).reshape((-1,) + (1,) * (len(shape) - 1 - position))
    return loudness


def noise(rng, shape, width, most, shards=(), kind=jnp.bfloat16):
    array = width * jax.random.normal(rng, shape, jnp.float32)
    if shards:
        array = array * block_scale(rng, shape, shards, -0.22, 0.18)
    return jnp.clip(array, -most, most).astype(kind)


def setup_inputs(seed: int = 0) -> dict:
    seeds = jax.random.split(jax.random.key(seed), 14)
    return {
        "stream": noise(seeds[0], (TOKENS, D), 1.0, 6.0, ((0, 16), (1, 2))),
        "recurrent_norm_gain": jnp.clip(1.0 + 0.18 * jax.random.normal(seeds[1], (D,), jnp.float32), 0.1, 1.9),
        "feedforward_norm_gain": jnp.clip(1.0 + 0.18 * jax.random.normal(seeds[2], (D,), jnp.float32), 0.1, 1.9),
        "recurrent_input_weight": noise(seeds[3], (D, D), D ** -0.5, 0.125, ((0, 8), (1, 2))),
        "output_gate_weight": noise(seeds[4], (D, D), D ** -0.5, 0.125, ((0, 8), (1, 2))),
        "causal_filter_weight": noise(seeds[5], (CONV, D), CONV ** -0.5, 3.0, ((1, 2),)),
        "decay_gate_matrix": noise(seeds[6], (BLOCKS, BLOCK, BLOCK), BLOCK ** -0.5, 0.75, ((0, 2),)),
        "input_gate_matrix": noise(seeds[7], (BLOCKS, BLOCK, BLOCK), BLOCK ** -0.5, 0.75, ((0, 2),)),
        "channel_decay_param": draw_channel_decay_param(jax.random.fold_in(seeds[13], 71), 0),
        "token_decay_offset": draw_token_decay_offset(jax.random.fold_in(seeds[13], 71), 0),
        "recurrent_output_weight": noise(seeds[10], (D, D), D ** -0.5, 0.125, ((0, 2), (1, 8))),
        "up_projection_weight": noise(seeds[11], (D, FF), D ** -0.5, 0.125, ((0, 8), (1, 2))),
        "down_projection_weight": noise(seeds[12], (FF, D), FF ** -0.5, 0.078125, ((0, 2), (1, 8))),
    }


EPSILON = 1e-06
DECAY_MULTIPLIER = 8.0

def norm_rows(values, gain):
    widened = values.astype(jnp.float32)
    inverse = lax.rsqrt(lax.optimization_barrier(jnp.mean(widened * widened, axis=-1, keepdims=True)) + EPSILON)
    return (widened * inverse * gain).astype(jnp.bfloat16)

def short_filter(values, causal_filter_weight):
    positions, channels = values.shape
    sequences = positions // SEQ_LEN
    reach = causal_filter_weight.shape[0]
    widened = lax.optimization_barrier(values).astype(jnp.float32).reshape(sequences, SEQ_LEN, channels)
    padded = jnp.pad(widened, ((0, 0), (reach - 1, 0), (0, 0)))
    taps = causal_filter_weight.astype(jnp.float32)
    total = taps[0] * padded[:, 0:SEQ_LEN]
    for offset in range(1, reach):
        total = total + taps[offset] * padded[:, offset:offset + SEQ_LEN]
    return total.reshape(positions, channels).astype(jnp.bfloat16)

def combine(earlier, later):
    return (earlier[0] * later[0], later[0] * earlier[1] + later[1])

def recurrent_states(filtered_input, output_gate_rows, decay_gate_matrix, input_gate_matrix, channel_decay_param, token_decay_offset):
    positions, channels = filtered_input.shape
    blocks, block_size, _ = decay_gate_matrix.shape
    widened = lax.optimization_barrier(filtered_input).astype(jnp.float32)
    grouped = widened.reshape(positions, blocks, block_size)
    recurrent_step = jax.nn.sigmoid(jnp.einsum('tnc,ncd->tnd', grouped, decay_gate_matrix.astype(jnp.float32)).reshape(positions, channels))
    inputs = jax.nn.sigmoid(jnp.einsum('tnc,ncd->tnd', grouped, input_gate_matrix.astype(jnp.float32)).reshape(positions, channels))
    decay_logarithm = -DECAY_MULTIPLIER * recurrent_step * jax.nn.softplus(-channel_decay_param) + token_decay_offset
    drive = jnp.sqrt(-jnp.expm1(2.0 * decay_logarithm)) * inputs * widened
    shaped = (positions // SEQ_LEN, SEQ_LEN, channels)
    _, states = lax.associative_scan(combine, (jnp.exp(decay_logarithm).reshape(shaped), drive.reshape(shaped)), axis=1)
    gate_wide = lax.optimization_barrier(output_gate_rows).astype(jnp.float32)
    return (states.reshape(positions, channels) * jax.nn.gelu(gate_wide, approximate=False)).astype(jnp.bfloat16)

def reference(stream, recurrent_norm_gain, feedforward_norm_gain, recurrent_input_weight, output_gate_weight, causal_filter_weight, decay_gate_matrix, input_gate_matrix, channel_decay_param, token_decay_offset, recurrent_output_weight, up_projection_weight, down_projection_weight):
    normed = norm_rows(stream, recurrent_norm_gain)
    span = D // N_TP
    grouped_block_rows = span // BLOCK
    mixer_update = jnp.zeros(stream.shape, jnp.float32)
    for channel_group in range(N_TP):
        lower_bound = channel_group * span
        upper_bound = lower_bound + span
        values = jnp.dot(normed, recurrent_input_weight[:, lower_bound:upper_bound], preferred_element_type=jnp.float32).astype(jnp.bfloat16)
        gate_values = jnp.dot(normed, output_gate_weight[:, lower_bound:upper_bound], preferred_element_type=jnp.float32).astype(jnp.bfloat16)
        filtered_input = short_filter(values, causal_filter_weight[:, lower_bound:upper_bound])
        mixed_rows = recurrent_states(filtered_input, gate_values, decay_gate_matrix[channel_group * grouped_block_rows:(channel_group + 1) * grouped_block_rows], input_gate_matrix[channel_group * grouped_block_rows:(channel_group + 1) * grouped_block_rows], channel_decay_param[lower_bound:upper_bound], token_decay_offset[:, lower_bound:upper_bound])
        partial_value = jnp.dot(mixed_rows, recurrent_output_weight[lower_bound:upper_bound], preferred_element_type=jnp.float32).astype(jnp.bfloat16)
        mixer_update = mixer_update + lax.optimization_barrier(partial_value).astype(jnp.float32)
    middle = (stream.astype(jnp.float32) + mixer_update).astype(jnp.bfloat16)
    normed_mid = norm_rows(middle, feedforward_norm_gain)
    hidden_span = FF // N_TP
    channel_update = jnp.zeros(stream.shape, jnp.float32)
    for channel_group in range(N_TP):
        lower_bound = channel_group * hidden_span
        upper_bound = lower_bound + hidden_span
        raised = jnp.dot(normed_mid, up_projection_weight[:, lower_bound:upper_bound], preferred_element_type=jnp.float32)
        activity = jnp.square(jax.nn.relu(raised)).astype(jnp.bfloat16)
        partial_value = jnp.dot(activity, down_projection_weight[lower_bound:upper_bound], preferred_element_type=jnp.float32).astype(jnp.bfloat16)
        channel_update = channel_update + lax.optimization_barrier(partial_value).astype(jnp.float32)
    return (middle.astype(jnp.float32) + channel_update).astype(jnp.bfloat16)
```

```python
import functools

import jax
import jax.numpy as jnp
from jax import lax
from jax.experimental import pallas as pl
from jax.experimental.pallas import tpu as pltpu
from jax.sharding import PartitionSpec as P


SEQ_LEN = 128
EPSILON = 1e-06
DECAY_MULTIPLIER = 8.0
LANES = 128


def half(values, which, axis):
    first, second = jnp.split(values, 2, axis)
    return jnp.where(which == 0, first, second)


def gather_shard(shard, ids, sizes):
    rep, fs, _ = ids
    _, n_fs, _ = sizes
    own, for_peer = shard
    hops = n_fs // 2
    place, side = fs // 2, fs % 2
    from_peer = lax.ppermute(for_peer, "fs", [(i, i ^ 1) for i in range(n_fs)])
    start = jnp.where(side == rep, own, from_peer)
    up = [(i, (i + 2) % n_fs) for i in range(n_fs)]
    down = [(i, (i + n_fs - 2) % n_fs) for i in range(n_fs)]
    pieces, places = [own, from_peer], [fs, fs ^ 1]
    below = above = start
    for step in range(1, hops):
        if step % 2:
            below = mine = lax.ppermute(below, "fs", up)
            base = 2 * ((place + hops - (step + 1) // 2) % hops)
        else:
            above = mine = lax.ppermute(above, "fs", down)
            base = 2 * ((place + step // 2) % hops)
        pieces += [mine, lax.ppermute(mine, "rep", [(0, 1), (1, 0)])]
        places += [base + rep, base + 1 - rep]
    return pieces, jnp.stack(places).astype(jnp.int32)


def gather_features(values, tp, n_tp):
    if n_tp != 2:
        return lax.all_gather(values, "tp", axis=1, tiled=True)
    other = lax.ppermute(values, "tp", [(0, 1), (1, 0)])
    return jnp.where(
        tp == 0, jnp.concatenate([values, other], 1), jnp.concatenate([other, values], 1)
    )


def sum_features(parts, tp, n_tp):
    total = lax.dynamic_index_in_dim(parts, tp, 0, False).astype(jnp.float32)
    for shift in range(1, n_tp):
        piece = lax.dynamic_index_in_dim(parts, (tp + shift) % n_tp, 0, False)
        got = lax.ppermute(piece, "tp", [(i, (i + shift) % n_tp) for i in range(n_tp)])
        total = total + got.astype(jnp.float32)
    return total.astype(jnp.bfloat16)


def norm_rows(values, gain):
    widened = values.astype(jnp.float32)
    inverse = lax.rsqrt(jnp.mean(widened * widened, axis=-1, keepdims=True) + EPSILON)
    return (widened * inverse * gain).astype(jnp.bfloat16)


ROWS = 256
CHUNK = 512


def depth_kernel(squared, places_ref, x_ref, *refs):
    *pieces, out_ref = refs
    depth, width = pieces[0].shape
    chunk = min(CHUNK, width)
    for lower in range(0, width, chunk):
        cols = slice(lower, lower + chunk)
        total = None
        for index, piece in enumerate(pieces):
            place = pl.multiple_of(places_ref[index] * depth, depth)
            term = jnp.dot(
                x_ref[:, pl.ds(place, depth)], piece[:, cols], preferred_element_type=jnp.float32
            )
            total = term if total is None else total + term
        if squared:
            total = jnp.square(jnp.maximum(total, 0.0))
        out_ref[:, cols] = total.astype(jnp.bfloat16)


def depth_matmul(x, gathered, squared=False):
    pieces, places = gathered
    tokens, width = x.shape
    shape = pieces[0].shape
    return pl.pallas_call(
        functools.partial(depth_kernel, squared),
        grid_spec=pltpu.PrefetchScalarGridSpec(
            num_scalar_prefetch=1,
            grid=(tokens // ROWS,),
            in_specs=[pl.BlockSpec((ROWS, width), lambda m, _: (m, 0))]
            + [pl.BlockSpec(shape, lambda m, _: (0, 0))] * len(pieces),
            out_specs=pl.BlockSpec((ROWS, shape[1]), lambda m, _: (m, 0)),
        ),
        out_shape=jax.ShapeDtypeStruct((tokens, shape[1]), jnp.bfloat16),
        cost_estimate=pl.CostEstimate(
            flops=2 * tokens * width * shape[1],
            bytes_accessed=2 * (tokens * width + (tokens + width) * shape[1]),
            transcendentals=0,
        ),
        name="depth_matmul",
    )(places, x, *pieces)


def columns_kernel(per, places_ref, x_ref, *refs):
    *pieces, out_ref = refs
    cols = pieces[0].shape[1]
    for index, piece in enumerate(pieces):
        place = places_ref[index]
        lower = pl.multiple_of((place % per) * cols, cols)
        out_ref[place // per, :, pl.ds(lower, cols)] = jnp.dot(
            x_ref[...], piece[...], preferred_element_type=jnp.float32
        ).astype(jnp.bfloat16)


def columns_matmul(x, gathered, n_tp, first, tokens):
    pieces, places = gathered
    depth, cols = pieces[0].shape
    per = len(pieces) // n_tp
    skip = first // ROWS
    return pl.pallas_call(
        functools.partial(columns_kernel, per),
        grid_spec=pltpu.PrefetchScalarGridSpec(
            num_scalar_prefetch=1,
            grid=(tokens // ROWS,),
            in_specs=[pl.BlockSpec((ROWS, depth), lambda m, _: (m + skip, 0))]
            + [pl.BlockSpec((depth, cols), lambda m, _: (0, 0))] * len(pieces),
            out_specs=pl.BlockSpec((n_tp, ROWS, per * cols), lambda m, _: (0, m, 0)),
        ),
        out_shape=jax.ShapeDtypeStruct((n_tp, tokens, per * cols), jnp.bfloat16),
        cost_estimate=pl.CostEstimate(
            flops=2 * tokens * depth * cols * len(pieces),
            bytes_accessed=2 * (tokens * depth + len(pieces) * cols * (depth + tokens)),
            transcendentals=0,
        ),
        name="columns_matmul",
    )(places, x, *pieces)


def shift_down(values, amount, fill):
    index = lax.broadcasted_iota(jnp.int32, values.shape, 0)
    return jnp.where(index < amount, fill, pltpu.roll(values, amount, 0))


def recurrence_kernel(
    side_ref, value_ref, gate_ref, own_ref, peer_ref, taps_ref, maps_ref, rate_ref, out_ref
):
    rows, channels = value_ref.shape
    reach = taps_ref.shape[0]
    per = LANES // maps_ref.shape[1]
    is_own = pl.program_id(0) < pl.num_programs(0) // 2
    for tile in range(channels // LANES):
        cols = slice(tile * LANES, (tile + 1) * LANES)
        values = value_ref[:, cols].astype(jnp.float32)
        filtered = taps_ref[reach - 1 : reach, cols] * values
        for back in range(1, reach):
            tap = taps_ref[reach - 1 - back : reach - back, cols]
            filtered = filtered + tap * shift_down(values, back, 0.0)
        conved = filtered.astype(jnp.bfloat16)
        maps = maps_ref[tile * per : (tile + 1) * per].reshape(LANES, 2 * LANES)
        logits = jnp.dot(conved, maps, preferred_element_type=jnp.float32)
        offset = jnp.where(is_own, own_ref[:, cols], peer_ref[:, cols].astype(jnp.float32))
        steps = 1.0 / (1.0 + jnp.exp(-logits))
        log_decay = steps[:, :LANES] * rate_ref[:, cols] + offset
        decay = jnp.exp(log_decay)
        y = -2.0 * log_decay
        series = 1.0 + y * (
            -1 / 2 + y * (1 / 6 + y * (-1 / 24 + y * (1 / 120 + y * (-1 / 720 + y * (1 / 5040)))))
        )
        lost = jnp.where(y < 0.35, y * series, 1.0 - decay * decay)
        state = jnp.sqrt(lost) * steps[:, LANES:] * conved.astype(jnp.float32)
        span = 1
        while span < rows:
            state = state + decay * shift_down(state, span, 0.0)
            if span * 2 < rows:
                decay = decay * shift_down(decay, span, 1.0)
            span *= 2
        gate = gate_ref[:, cols].astype(jnp.float32)
        gelu = 0.5 * gate * (1.0 + lax.erf(gate * 0.7071067811865476))
        out_ref[:, cols] = (state * gelu).astype(jnp.bfloat16)


def recurrence(projected, offset_own, offset_peer, taps, decay_maps, input_maps, rate, side):
    tokens = projected.shape[0]
    channels = offset_peer.shape[1]
    blocks, size, _ = decay_maps.shape
    per = LANES // size
    block = jnp.arange(blocks)[:, None, None] % per
    group = jnp.arange(LANES)[None, None, :] // size

    def diagonal(maps):
        return jnp.where(block == group, jnp.tile(maps, (1, 1, per)), 0)

    maps = jnp.concatenate([diagonal(decay_maps), diagonal(input_maps)], 2)
    sequences = tokens // SEQ_LEN
    own = sequences // 2
    return pl.pallas_call(
        recurrence_kernel,
        grid_spec=pltpu.PrefetchScalarGridSpec(
            num_scalar_prefetch=1,
            grid=(sequences,),
            in_specs=[
                pl.BlockSpec((SEQ_LEN, channels), lambda s, side: (s, 0)),
                pl.BlockSpec((SEQ_LEN, channels), lambda s, side: (s, 1)),
                pl.BlockSpec(
                    (SEQ_LEN, channels), lambda s, side: (jnp.minimum(s, own - 1), side[0])
                ),
                pl.BlockSpec((SEQ_LEN, channels), lambda s, side: (jnp.maximum(s - own, 0), 0)),
                pl.BlockSpec((taps.shape[0], channels), lambda s, side: (0, side[0])),
                pl.BlockSpec((blocks // 2, size, 2 * LANES), lambda s, side: (side[0], 0, 0)),
                pl.BlockSpec((1, channels), lambda s, side: (0, side[0])),
            ],
            out_specs=pl.BlockSpec((SEQ_LEN, channels), lambda s, side: (s, 0)),
        ),
        out_shape=jax.ShapeDtypeStruct((tokens, channels), jnp.bfloat16),
        cost_estimate=pl.CostEstimate(
            flops=tokens * channels * 700,
            bytes_accessed=tokens * channels * 10,
            transcendentals=tokens * channels * 6,
        ),
        name="recurrence",
    )(
        side.astype(jnp.int32)[None],
        projected,
        projected,
        offset_own,
        offset_peer,
        taps.astype(jnp.float32),
        maps,
        rate[None, :],
    )


def shards(
    sizes,
    stream,
    recurrent_norm_gain,
    feedforward_norm_gain,
    recurrent_input_weight,
    output_gate_weight,
    causal_filter_weight,
    decay_gate_matrix,
    input_gate_matrix,
    channel_decay_param,
    token_decay_offset,
    recurrent_output_weight,
    up_projection_weight,
    down_projection_weight,
):
    _, n_fs, n_tp = sizes
    ids = lax.axis_index("rep"), lax.axis_index("fs"), lax.axis_index("tp")
    _, fs, tp = ids
    side = fs % 2
    pairs = [(i, i ^ 1) for i in range(n_fs)]
    tokens = stream.shape[0]

    def halves(weight, axis):
        return half(weight, side, axis), half(weight, 1 - side, axis)

    def to_peer(values):
        return lax.ppermute(values, "fs", pairs)

    value_own, value_peer = halves(recurrent_input_weight, 1)
    gate_own, gate_peer = halves(output_gate_weight, 1)
    entry = (
        jnp.concatenate([value_own, gate_own], 1),
        jnp.concatenate([value_peer, gate_peer], 1),
    )
    entry_full = gather_shard(entry, ids, sizes)
    stream_peer = to_peer(stream)
    offset_peer = to_peer(half(token_decay_offset, 1 - side, 1).astype(jnp.bfloat16))
    output_full = gather_shard(halves(recurrent_output_weight, 0), ids, sizes)
    expand_full = gather_shard(halves(up_projection_weight, 1), ids, sizes)
    contract_full = gather_shard(halves(down_projection_weight, 0), ids, sizes)

    own_pair = jnp.concatenate([stream, stream_peer], 0)
    whole = gather_features(own_pair, tp, n_tp)
    normed = norm_rows(whole, recurrent_norm_gain)
    projected = depth_matmul(normed, entry_full)
    mixed = recurrence(
        projected,
        token_decay_offset,
        offset_peer,
        causal_filter_weight,
        decay_gate_matrix,
        input_gate_matrix,
        -DECAY_MULTIPLIER * jax.nn.softplus(-channel_decay_param),
        side,
    )
    mixer_terms = columns_matmul(mixed, output_full, n_tp, 0, 2 * tokens)
    mixer_chip = sum_features(mixer_terms, tp, n_tp)
    got_own = to_peer(mixer_chip[tokens:])
    got_peer = to_peer(mixer_chip[:tokens])
    update = mixer_chip.astype(jnp.float32) + jnp.concatenate([got_own, got_peer], 0).astype(
        jnp.float32
    )
    middle = (own_pair.astype(jnp.float32) + update).astype(jnp.bfloat16)
    normed_mid = norm_rows(gather_features(middle, tp, n_tp), feedforward_norm_gain)
    activity = depth_matmul(normed_mid, expand_full, squared=True)
    peer_terms = columns_matmul(activity, contract_full, n_tp, tokens, tokens)
    got = to_peer(sum_features(peer_terms, tp, n_tp))
    own_terms = columns_matmul(activity, contract_full, n_tp, 0, tokens)
    own_chip = sum_features(own_terms, tp, n_tp)
    channel_sum = own_chip.astype(jnp.float32) + got.astype(jnp.float32)
    return (middle[:tokens].astype(jnp.float32) + channel_sum).astype(jnp.bfloat16)


MESH = pl.DeviceIdType.MESH
CHUNK_ROWS = 128


def whole_kernel(
    stream_ref,
    offset_ref,
    first_gain_ref,
    second_gain_ref,
    taps_ref,
    decay_maps_ref,
    input_maps_ref,
    rate_ref,
    value_hbm,
    gate_hbm,
    output_hbm,
    raise_hbm,
    lower_hbm,
    out_ref,
    weights,
    normed,
    normed_mid,
    square_own,
    square_got,
    projected,
    mixed,
    offsets,
    offset_send,
    maps,
    kept,
    passed,
    got,
    mid_send,
    mid_got,
    middle,
    activity,
    partial,
    partial_got,
    last_send,
    last_got,
    local_sem,
    y_send,
    y_recv,
    z_send,
    z_recv,
    x_send,
    x_recv,
    act_send,
    act_recv,
):
    rep, fs, tp = lax.axis_index("rep"), lax.axis_index("fs"), lax.axis_index("tp")
    z, y = fs // 2, fs % 2
    tokens, half_width = stream_ref.shape
    width = 2 * half_width
    chunks, _, n_fs, block, _ = weights.shape
    quarter = half_width // 2
    lane_tiles = half_width // LANES
    raises = (chunks - 3) // 2
    is_mid = jnp.logical_or(z == 1, z == 2)
    low = (z // 2) == tp

    def plane(m):
        return 2 * ((z // 2 + m // 2) % 2) + (z % 2 + m % 2) % 2

    x_peer = (1 - rep, fs, tp)
    y_peer = (rep, 2 * z + 1 - y, tp)
    t_peer = (rep, fs, 1 - tp)

    def z_peer(m):
        return (rep, 2 * plane(m) + y, tp)

    barrier = pltpu.get_barrier_semaphore()
    for peer in (x_peer, y_peer, t_peer, z_peer(1), z_peer(2), z_peer(3)):
        pl.semaphore_signal(barrier, inc=1, device_id=peer, device_id_type=MESH)
    pl.semaphore_wait(barrier, 6)

    def remote(src, dst, send, recv, peer):
        return pltpu.make_async_remote_copy(
            src_ref=src, dst_ref=dst, send_sem=send, recv_sem=recv, device_id=peer, device_id_type=MESH
        )

    def shard_block(k, side, part):
        if k < 2 or 3 <= k < 3 + raises:
            ref = (value_hbm, gate_hbm)[k] if k < 2 else raise_hbm
            first = 0 if k < 2 else (k - 3) * quarter
            span = ref.shape[1] // 2
            start = pl.multiple_of(side * span + first + part * block, block)
            return ref.at[:, pl.ds(start, block)]
        ref = output_hbm if k == 2 else lower_hbm
        first = 0 if k == 2 else (k - 3 - raises) * quarter
        span = ref.shape[0] // 2
        start = pl.multiple_of(side * span + first + part * block, block)
        return ref.at[pl.ds(start, block), :]

    def part_of(q):
        return rep if q == 0 else 1 - rep

    def local_copy(k, q):
        part = part_of(q)
        return pltpu.make_async_copy(
            shard_block(k, y, part), weights.at[k, part, fs], local_sem.at[k, q]
        )

    def y_copy(k, q):
        part = part_of(q)
        return remote(
            shard_block(k, 1 - y, part), weights.at[k, part, fs], y_send.at[k, q], y_recv.at[k, q], y_peer
        )

    def z_copy(k, h, m):
        spot = weights.at[k, rep, fs if h == 0 else 2 * z + 1 - y]
        src = shard_block(k, y, rep) if h == 0 else spot
        return remote(src, spot, z_send.at[k, h, m - 1], z_recv.at[k, h, m - 1], z_peer(m))

    def z_relay(k, h):
        spot = weights.at[k, rep, 2 * plane(2) + (y if h == 0 else 1 - y)]
        return remote(spot, spot, z_send.at[k, h, 3], z_recv.at[k, h, 2], z_peer(1))

    def x_copy(k, h, m):
        spot = weights.at[k, rep, 2 * plane(m) + (y if h == 0 else 1 - y)]
        return remote(spot, spot, x_send.at[k, h, m - 1], x_recv.at[k, h, m - 1], x_peer)

    def z_start(k, h):
        z_copy(k, h, 2).start()
        z_copy(k, h, 1).start()

        @pl.when(is_mid)
        def _():
            z_copy(k, h, 3).start()

    def forward_y(k):
        y_copy(k, 0).wait_recv()
        z_start(k, 1)

    def relay(k, h, m):
        z_copy(k, h, m).wait_recv()
        x_copy(k, h, m).start()

        @pl.when(jnp.logical_and(is_mid, m == 2))
        def _():
            z_relay(k, h).start()

    def relay_all(k, h):
        for m in (1, 2, 3):
            relay(k, h, m)

    def relay_at(index, k, h):
        @pl.when(index < 3)
        def _():
            relay(k, h, index + 1)

    def wait_own(k):
        for q in range(2):
            local_copy(k, q).wait()
        y_copy(k, 1).wait_recv()

    def wait_x(k, h):
        for m in (1, 2, 3):
            x_copy(k, h, m).wait_recv()

    def tp_copy(src, dst, slot):
        return remote(src, dst, act_send.at[slot], act_recv.at[slot], t_peer)

    def y_act(src, dst, slot):
        return remote(src, dst, act_send.at[slot], act_recv.at[slot], y_peer)

    for k in range(3):
        for q in range(2):
            y_copy(k, q).start()
    for k in range(2):
        z_start(k, 0)
    for k in range(chunks):
        for q in range(2):
            local_copy(k, q).start()

    own_columns = pl.ds(pl.multiple_of(tp * half_width, half_width), half_width)

    def squares(source, phase):
        def body(step, _):
            rows = pl.ds(pl.multiple_of(step * CHUNK_ROWS, CHUNK_ROWS), CHUNK_ROWS)
            total = None
            for tile in range(lane_tiles):
                value = source[rows, tile * LANES : (tile + 1) * LANES].astype(jnp.float32)
                total = value * value if total is None else total + value * value
            square_own[phase, rows, :] = total
            return 0

        lax.fori_loop(0, tokens // CHUNK_ROWS, body, 0)

    def square_copy(phase):
        return tp_copy(square_own.at[phase], square_got.at[phase], 9 + phase)

    def norm(source, phase, gain_ref, target):
        def body(step, _):
            rows = pl.ds(pl.multiple_of(step * CHUNK_ROWS, CHUNK_ROWS), CHUNK_ROWS)
            total = jnp.sum(square_own[phase, rows, :] + square_got[phase, rows, :], axis=1, keepdims=True)
            inverse = lax.rsqrt(total * (1.0 / width) + EPSILON)
            for tile in range(lane_tiles):
                value = source[rows, tile * LANES : (tile + 1) * LANES].astype(jnp.float32)
                gain = gain_ref[pl.ds(tp * lane_tiles + tile, 1), :]
                lanes = pl.ds(pl.multiple_of(tp * half_width + tile * LANES, LANES), LANES)
                target[y, rows, lanes] = (value * inverse * gain).astype(jnp.bfloat16)
            return 0

        lax.fori_loop(0, tokens // CHUNK_ROWS, body, 0)

    def block_copies(target, base):
        own = target.at[y, :, own_columns]
        theirs = target.at[1 - y, :, own_columns]
        return (
            tp_copy(own, own, base),
            y_act(own, own, base + 1),
            tp_copy(theirs, theirs, base + 2),
        )

    squares(stream_ref, 0)
    square_copy(0).start()
    mine = pl.ds(pl.multiple_of(y * quarter, quarter), quarter)
    peers = pl.ds(pl.multiple_of((1 - y) * quarter, quarter), quarter)
    offset_send[...] = offset_ref[:, peers].astype(jnp.bfloat16)
    offsets[0] = offset_ref[:, mine].astype(jnp.bfloat16)
    square_copy(0).wait_recv()
    norm(stream_ref, 0, first_gain_ref, normed)
    first_tp, first_y, first_pass = block_copies(normed, 0)
    first_y.start()
    first_tp.start()
    offset_copy = y_act(offset_send, offsets.at[1], 3)
    offset_copy.start()
    for k in range(3, 3 + raises):
        for q in range(2):
            y_copy(k, q).start()

    forward_y(0)
    relay_all(0, 0)
    forward_y(1)
    z_start(2, 0)
    relay_all(0, 1)
    forward_y(2)
    for k in range(3, 3 + raises):
        z_start(k, 0)
    relay_all(1, 0)

    size = decay_maps_ref.shape[1]
    per = LANES // size
    tiles = quarter // LANES
    maps[...] = jnp.zeros_like(maps)
    for tile in range(tiles):
        for index in range(per):
            place = y * (tiles * per) + tile * per + index
            span = slice(index * size, (index + 1) * size)
            maps[tile, span, index * size : (index + 1) * size] = decay_maps_ref[place]
            maps[tile, span, LANES + index * size : LANES + (index + 1) * size] = input_maps_ref[place]

    relay_all(1, 1)
    first_y.wait_recv()
    first_pass.start()

    for k in range(2):
        wait_own(k)
    for k in range(2):
        for h in range(2):
            wait_x(k, h)
    first_tp.wait_recv()

    def project(which, token_block, relays):
        def body(step, _):
            relay_at(step, *relays)
            matrix = weights[step // 2, step % 2].reshape(width, block)
            projected[which, step] = jnp.dot(
                normed[token_block], matrix, preferred_element_type=jnp.float32
            ).astype(jnp.bfloat16)
            return 0

        lax.fori_loop(0, 4, body, 0)

    reach = taps_ref.shape[0]

    def recur(which, relays):
        def body(step, _):
            relay_at(step, *relays)
            rows = pl.ds(pl.multiple_of(step * SEQ_LEN, SEQ_LEN), SEQ_LEN)
            for tile in range(tiles):
                part, lane = tile * LANES // block, tile * LANES % block
                lanes = slice(lane, lane + LANES)
                taps = taps_ref[
                    :, pl.ds(pl.multiple_of(y * quarter + tile * LANES, LANES), LANES)
                ].astype(jnp.float32)
                values = projected[which, part, rows, lanes].astype(jnp.float32)
                filtered = taps[reach - 1 : reach] * values
                for back in range(1, reach):
                    tap = taps[reach - 1 - back : reach - back]
                    filtered = filtered + tap * shift_down(values, back, 0.0)
                conved = filtered.astype(jnp.bfloat16)
                logits = jnp.dot(conved, maps[tile], preferred_element_type=jnp.float32)
                offset = offsets[which, rows, tile * LANES : (tile + 1) * LANES].astype(jnp.float32)
                steps = 1.0 / (1.0 + jnp.exp(-logits))
                rate = rate_ref[pl.ds(y * tiles + tile, 1), :]
                log_decay = steps[:, :LANES] * rate + offset
                decay = jnp.exp(log_decay)
                twice = -2.0 * log_decay
                series = 1.0 + twice * (
                    -1 / 2
                    + twice
                    * (1 / 6 + twice * (-1 / 24 + twice * (1 / 120 + twice * (-1 / 720 + twice * (1 / 5040)))))
                )
                lost = jnp.where(twice < 0.35, twice * series, 1.0 - decay * decay)
                state = jnp.sqrt(lost) * steps[:, LANES:] * conved.astype(jnp.float32)
                span = 1
                while span < SEQ_LEN:
                    state = state + decay * shift_down(state, span, 0.0)
                    if span * 2 < SEQ_LEN:
                        decay = decay * shift_down(decay, span, 1.0)
                    span *= 2
                gate = projected[which, 2 + part, rows, lanes].astype(jnp.float32)
                gelu = 0.5 * gate * (1.0 + lax.erf(gate * 0.7071067811865476))
                mixed[which, rows, tile * LANES : (tile + 1) * LANES] = (state * gelu).astype(jnp.bfloat16)
            return 0

        lax.fori_loop(0, tokens // SEQ_LEN, body, 0)

    project(0, y, (2, 0))
    recur(0, (2, 1))
    first_pass.wait_recv()
    project(1, 1 - y, (3, 0))
    offset_copy.wait_recv()
    recur(1, (4, 0))

    wait_own(2)
    wait_x(2, 0)
    wait_x(2, 1)

    def mix_out(which):
        def body(step, _):
            def term(place):
                matrix = weights[2, :, place].reshape(quarter, block)
                return jnp.dot(mixed[which], matrix, preferred_element_type=jnp.float32).astype(jnp.bfloat16)

            lanes = pl.ds(pl.multiple_of(step * block, block), block)
            per_half = n_fs // 2
            passed[which, :, lanes] = term(per_half * (1 - tp) + step)
            kept[which, :, lanes] = term(per_half * tp + step)
            return 0

        lax.fori_loop(0, n_fs // 2, body, 0)

    def mix_copy(which):
        return tp_copy(passed.at[which], got.at[which], 4 + which)

    mix_out(1)
    mix_copy(1).start()
    mix_out(0)
    mix_copy(0).start()

    def add_peer(step, _):
        rows = pl.ds(pl.multiple_of(step * CHUNK_ROWS, CHUNK_ROWS), CHUNK_ROWS)
        mid_send[rows, :] = (
            kept[1, rows, :].astype(jnp.float32) + got[1, rows, :].astype(jnp.float32)
        ).astype(jnp.bfloat16)
        return 0

    mix_copy(1).wait_recv()
    lax.fori_loop(0, tokens // CHUNK_ROWS, add_peer, 0)
    mid_copy = y_act(mid_send, mid_got, 6)
    mid_copy.start()

    last_raise = 3 + raises
    for k in range(5, last_raise):
        relay_all(k, 0)
    for k in range(3, last_raise):
        forward_y(k)
    for k in range(last_raise, chunks):
        z_start(k, 0)
    mix_copy(0).wait_recv()
    relay_all(3, 1)

    mid_copy.wait_recv()

    def add_own(step, _):
        rows = pl.ds(pl.multiple_of(step * CHUNK_ROWS, CHUNK_ROWS), CHUNK_ROWS)
        total = None
        for tile in range(lane_tiles):
            lanes = slice(tile * LANES, (tile + 1) * LANES)
            update = kept[0, rows, lanes].astype(jnp.float32) + got[0, rows, lanes].astype(jnp.float32)
            update = update + mid_got[rows, lanes].astype(jnp.float32)
            value = (stream_ref[rows, lanes].astype(jnp.float32) + update).astype(jnp.bfloat16)
            middle[rows, lanes] = value
            value = value.astype(jnp.float32)
            total = value * value if total is None else total + value * value
        square_own[1, rows, :] = total
        return 0

    lax.fori_loop(0, tokens // CHUNK_ROWS, add_own, 0)
    square_copy(1).start()
    square_copy(1).wait_recv()
    norm(middle, 1, second_gain_ref, normed_mid)
    second_tp, second_y, second_pass = block_copies(normed_mid, 11)
    second_y.start()
    second_tp.start()
    for k in range(last_raise, chunks):
        for q in range(2):
            y_copy(k, q).start()

    for k in range(4, last_raise):
        relay_all(k, 1)
    for k in range(3, last_raise):
        wait_own(k)
        wait_x(k, 0)
        wait_x(k, 1)

    def lift(which, token_block, relays):
        def body(step, _):
            relay_at(step, *relays)
            matrix = weights[3 + step // 2, step % 2].reshape(width, block)
            total = jnp.dot(normed_mid[token_block], matrix, preferred_element_type=jnp.float32)
            lanes = pl.ds(pl.multiple_of(step * block, block), block)
            activity[which, :, lanes] = jnp.square(jnp.maximum(total, 0.0)).astype(jnp.bfloat16)
            return 0

        lax.fori_loop(0, 2 * raises, body, 0)

    second_tp.wait_recv()
    lift(0, y, (last_raise, 0))
    second_y.wait_recv()
    second_pass.start()
    second_pass.wait_recv()
    lift(1, 1 - y, (last_raise + 1, 0))
    for k in range(last_raise + 2, chunks):
        relay_all(k, 0)
    for k in range(last_raise, chunks):
        forward_y(k)

    depth = raises * quarter

    def lower(h, m):
        place = 2 * plane(m) + (y if h == 0 else 1 - y)

        def body(which, _):
            matrix = weights[last_raise:chunks, :, place].reshape(depth, block)
            partial[m, h, which] = jnp.dot(
                activity[which], matrix, preferred_element_type=jnp.float32
            ).astype(jnp.bfloat16)
            return 0

        lax.fori_loop(0, 2, body, 0)

    def is_owner(m):
        return low if m < 2 else jnp.logical_not(low)

    def owner_copy(h, m):
        slot = 14 + 2 * (m % 2) + h
        return tp_copy(partial.at[m, h], partial_got.at[m % 2, h], slot)

    def last_copy(h, m):
        slot = 18 + 2 * (m % 2)
        return remote(
            last_send.at[m % 2, h],
            last_got.at[m % 2, 1 - h],
            act_send.at[slot + h],
            act_recv.at[slot + 1 - h],
            y_peer,
        )

    def pass_on(h, m):
        @pl.when(jnp.logical_not(is_owner(m)))
        def _():
            owner_copy(h, m).start()

    def finish(h, m):
        @pl.when(is_owner(m))
        def _():
            owner_copy(h, m).wait_recv()

            def body(step, _):
                rows = pl.ds(pl.multiple_of(step * CHUNK_ROWS, CHUNK_ROWS), CHUNK_ROWS)
                last_send[m % 2, h, rows, :] = (
                    partial[m, h, 1, rows, :].astype(jnp.float32)
                    + partial_got[m % 2, h, 1, rows, :].astype(jnp.float32)
                ).astype(jnp.bfloat16)
                return 0

            lax.fori_loop(0, tokens // CHUNK_ROWS, body, 0)
            last_copy(h, m).start()

    def close(h, mm):
        owned = mm + 2 * (1 - low.astype(jnp.int32))
        last_copy(1 - h, mm).wait_recv()
        place = 2 * ((z % 2 + mm) % 2) + (y if h == 0 else 1 - y)
        lanes = pl.ds(pl.multiple_of(place * block, block), block)

        def body(step, _):
            rows = pl.ds(pl.multiple_of(step * CHUNK_ROWS, CHUNK_ROWS), CHUNK_ROWS)
            update = (
                partial[owned, h, 0, rows, :].astype(jnp.float32)
                + partial_got[mm, h, 0, rows, :].astype(jnp.float32)
                + last_got[mm, h, rows, :].astype(jnp.float32)
            )
            out_ref[rows, lanes] = (middle[rows, lanes].astype(jnp.float32) + update).astype(jnp.bfloat16)
            return 0

        lax.fori_loop(0, tokens // CHUNK_ROWS, body, 0)

    for k in range(last_raise, chunks):
        wait_own(k)
        wait_x(k, 0)
    order = [(0, m) for m in range(4)] + [(1, m) for m in range(4)]
    for index, (h, m) in enumerate(order):
        if index == 5:
            for k in range(last_raise, chunks):
                relay_all(k, 1)
            for k in range(last_raise, chunks):
                wait_x(k, 1)
        lower(h, m)
        pass_on(h, m)
        if index:
            finish(*order[index - 1])
    finish(*order[-1])
    for h in range(2):
        for mm in range(2):
            close(h, mm)

    for k in range(chunks):
        for q in range(2):
            y_copy(k, q).wait_send()
        for h in range(2):
            z_copy(k, h, 1).wait_send()
            z_copy(k, h, 2).wait_send()

            @pl.when(is_mid)
            def _():
                z_copy(k, h, 3).wait_send()
                z_relay(k, h).wait_send()

            for m in (1, 2, 3):
                x_copy(k, h, m).wait_send()
    for copy in (first_tp, first_y, first_pass, second_tp, second_y, second_pass, offset_copy, mid_copy):
        copy.wait_send()
    for phase in range(2):
        square_copy(phase).wait_send()
        mix_copy(phase).wait_send()
    for h, m in order:

        @pl.when(is_owner(m))
        def _():
            last_copy(h, m).wait_send()

        @pl.when(jnp.logical_not(is_owner(m)))
        def _():
            owner_copy(h, m).wait_send()


def whole_layer(
    stream,
    recurrent_norm_gain,
    feedforward_norm_gain,
    recurrent_input_weight,
    output_gate_weight,
    causal_filter_weight,
    decay_gate_matrix,
    input_gate_matrix,
    channel_decay_param,
    token_decay_offset,
    recurrent_output_weight,
    up_projection_weight,
    down_projection_weight,
):
    tokens, half_width = stream.shape
    width = 2 * half_width
    quarter = half_width // 2
    block, n_fs = quarter // 2, 8
    raises = up_projection_weight.shape[1] // half_width
    chunks = 3 + 2 * raises
    depth = raises * quarter
    tiles = quarter // LANES
    half_type, full_type = jnp.bfloat16, jnp.float32
    rate = -DECAY_MULTIPLIER * jax.nn.softplus(-channel_decay_param)
    vmem = pl.BlockSpec(memory_space=pltpu.VMEM)
    anywhere = pl.BlockSpec(memory_space=pl.ANY)
    dma = pltpu.SemaphoreType.DMA
    return pl.pallas_call(
        whole_kernel,
        out_shape=jax.ShapeDtypeStruct((tokens, half_width), half_type),
        in_specs=[vmem] * 8 + [anywhere] * 5,
        out_specs=vmem,
        scratch_shapes=[
            pltpu.VMEM((chunks, 2, n_fs, block, block), half_type),
            pltpu.VMEM((2, tokens, width), half_type),
            pltpu.VMEM((2, tokens, width), half_type),
            pltpu.VMEM((2, tokens, LANES), full_type),
            pltpu.VMEM((2, tokens, LANES), full_type),
            pltpu.VMEM((2, 4, tokens, block), half_type),
            pltpu.VMEM((2, tokens, quarter), half_type),
            pltpu.VMEM((2, tokens, quarter), half_type),
            pltpu.VMEM((tokens, quarter), half_type),
            pltpu.VMEM((tiles, LANES, 2 * LANES), half_type),
            pltpu.VMEM((2, tokens, half_width), half_type),
            pltpu.VMEM((2, tokens, half_width), half_type),
            pltpu.VMEM((2, tokens, half_width), half_type),
            pltpu.VMEM((tokens, half_width), half_type),
            pltpu.VMEM((tokens, half_width), half_type),
            pltpu.VMEM((tokens, half_width), half_type),
            pltpu.VMEM((2, tokens, depth), half_type),
            pltpu.VMEM((4, 2, 2, tokens, block), half_type),
            pltpu.VMEM((2, 2, 2, tokens, block), half_type),
            pltpu.VMEM((2, 2, tokens, block), half_type),
            pltpu.VMEM((2, 2, tokens, block), half_type),
            dma((chunks, 2)),
            dma((chunks, 2)),
            dma((chunks, 2)),
            dma((chunks, 2, 4)),
            dma((chunks, 2, 3)),
            dma((chunks, 2, 3)),
            dma((chunks, 2, 3)),
            dma((22,)),
            dma((22,)),
        ],
        compiler_params=pltpu.CompilerParams(
            collective_id=0, has_side_effects=True, vmem_limit_bytes=67043328
        ),
        name="whole_layer",
    )(
        stream,
        token_decay_offset,
        recurrent_norm_gain.reshape(-1, LANES),
        feedforward_norm_gain.reshape(-1, LANES),
        causal_filter_weight,
        decay_gate_matrix,
        input_gate_matrix,
        rate.reshape(-1, LANES),
        recurrent_input_weight,
        output_gate_weight,
        recurrent_output_weight,
        up_projection_weight,
        down_projection_weight,
    )


def fits_whole(sizes, stream, up_projection_weight, decay_gate_matrix):
    tokens, half_width = stream.shape
    return (
        sizes == (2, 8, 2)
        and half_width % (8 * LANES) == 0
        and tokens % (4 * SEQ_LEN) == 0
        and up_projection_weight.shape[1] % half_width == 0
        and up_projection_weight.shape[1] // half_width >= 2
        and LANES % decay_gate_matrix.shape[1] == 0
    )


def solution(mesh):
    in_specs = (
        P(("rep", "fs"), "tp"),
        P(),
        P(),
        P("fs", "tp"),
        P("fs", "tp"),
        P(None, "tp"),
        P("tp", None, None),
        P("tp", None, None),
        P("tp"),
        P(("rep", "fs"), "tp"),
        P("tp", "fs"),
        P("fs", "tp"),
        P("tp", "fs"),
    )
    out_specs = P(("rep", "fs"), "tp")
    sizes = tuple(mesh.shape[axis] for axis in ("rep", "fs", "tp"))

    def body(*args):
        if fits_whole(sizes, args[0], args[11], args[6]):
            return whole_layer(*args)
        return shards(sizes, *args)

    return jax.shard_map(
        body, mesh=mesh, in_specs=in_specs, out_specs=out_specs, check_vma=False
    )
```

```python
import functools

import jax
import jax.numpy as jnp
from jax import lax
from jax.experimental import pallas as pl
from jax.experimental.pallas import tpu as pltpu
from jax.sharding import PartitionSpec as P


SEQ_LEN = 128
EPSILON = 1e-06
DECAY_MULTIPLIER = 8.0
LANES = 128


def half(values, which, axis):
    first, second = jnp.split(values, 2, axis)
    return jnp.where(which == 0, first, second)


def gather_shard(shard, ids, sizes):
    rep, fs, _ = ids
    _, n_fs, _ = sizes
    own, for_peer = shard
    hops = n_fs // 2
    place, side = fs // 2, fs % 2
    from_peer = lax.ppermute(for_peer, "fs", [(i, i ^ 1) for i in range(n_fs)])
    start = jnp.where(side == rep, own, from_peer)
    up = [(i, (i + 2) % n_fs) for i in range(n_fs)]
    down = [(i, (i + n_fs - 2) % n_fs) for i in range(n_fs)]
    pieces, places = [own, from_peer], [fs, fs ^ 1]
    below = above = start
    for step in range(1, hops):
        if step % 2:
            below = mine = lax.ppermute(below, "fs", up)
            base = 2 * ((place + hops - (step + 1) // 2) % hops)
        else:
            above = mine = lax.ppermute(above, "fs", down)
            base = 2 * ((place + step // 2) % hops)
        pieces += [mine, lax.ppermute(mine, "rep", [(0, 1), (1, 0)])]
        places += [base + rep, base + 1 - rep]
    return pieces, jnp.stack(places).astype(jnp.int32)


def gather_features(values, tp, n_tp):
    if n_tp != 2:
        return lax.all_gather(values, "tp", axis=1, tiled=True)
    other = lax.ppermute(values, "tp", [(0, 1), (1, 0)])
    return jnp.where(
        tp == 0, jnp.concatenate([values, other], 1), jnp.concatenate([other, values], 1)
    )


def sum_features(parts, tp, n_tp):
    total = lax.dynamic_index_in_dim(parts, tp, 0, False).astype(jnp.float32)
    for shift in range(1, n_tp):
        piece = lax.dynamic_index_in_dim(parts, (tp + shift) % n_tp, 0, False)
        got = lax.ppermute(piece, "tp", [(i, (i + shift) % n_tp) for i in range(n_tp)])
        total = total + got.astype(jnp.float32)
    return total.astype(jnp.bfloat16)


def norm_rows(values, gain):
    widened = values.astype(jnp.float32)
    inverse = lax.rsqrt(jnp.mean(widened * widened, axis=-1, keepdims=True) + EPSILON)
    return (widened * inverse * gain).astype(jnp.bfloat16)


ROWS = 256
CHUNK = 512


def depth_kernel(squared, places_ref, x_ref, *refs):
    *pieces, out_ref = refs
    depth, width = pieces[0].shape
    chunk = min(CHUNK, width)
    for lower in range(0, width, chunk):
        cols = slice(lower, lower + chunk)
        total = None
        for index, piece in enumerate(pieces):
            place = pl.multiple_of(places_ref[index] * depth, depth)
            term = jnp.dot(
                x_ref[:, pl.ds(place, depth)], piece[:, cols], preferred_element_type=jnp.float32
            )
            total = term if total is None else total + term
        if squared:
            total = jnp.square(jnp.maximum(total, 0.0))
        out_ref[:, cols] = total.astype(jnp.bfloat16)


def depth_matmul(x, gathered, squared=False):
    pieces, places = gathered
    tokens, width = x.shape
    shape = pieces[0].shape
    return pl.pallas_call(
        functools.partial(depth_kernel, squared),
        grid_spec=pltpu.PrefetchScalarGridSpec(
            num_scalar_prefetch=1,
            grid=(tokens // ROWS,),
            in_specs=[pl.BlockSpec((ROWS, width), lambda m, _: (m, 0))]
            + [pl.BlockSpec(shape, lambda m, _: (0, 0))] * len(pieces),
            out_specs=pl.BlockSpec((ROWS, shape[1]), lambda m, _: (m, 0)),
        ),
        out_shape=jax.ShapeDtypeStruct((tokens, shape[1]), jnp.bfloat16),
        cost_estimate=pl.CostEstimate(
            flops=2 * tokens * width * shape[1],
            bytes_accessed=2 * (tokens * width + (tokens + width) * shape[1]),
            transcendentals=0,
        ),
        name="depth_matmul",
    )(places, x, *pieces)


def columns_kernel(per, places_ref, x_ref, *refs):
    *pieces, out_ref = refs
    cols = pieces[0].shape[1]
    for index, piece in enumerate(pieces):
        place = places_ref[index]
        lower = pl.multiple_of((place % per) * cols, cols)
        out_ref[place // per, :, pl.ds(lower, cols)] = jnp.dot(
            x_ref[...], piece[...], preferred_element_type=jnp.float32
        ).astype(jnp.bfloat16)


def columns_matmul(x, gathered, n_tp, first, tokens):
    pieces, places = gathered
    depth, cols = pieces[0].shape
    per = len(pieces) // n_tp
    skip = first // ROWS
    return pl.pallas_call(
        functools.partial(columns_kernel, per),
        grid_spec=pltpu.PrefetchScalarGridSpec(
            num_scalar_prefetch=1,
            grid=(tokens // ROWS,),
            in_specs=[pl.BlockSpec((ROWS, depth), lambda m, _: (m + skip, 0))]
            + [pl.BlockSpec((depth, cols), lambda m, _: (0, 0))] * len(pieces),
            out_specs=pl.BlockSpec((n_tp, ROWS, per * cols), lambda m, _: (0, m, 0)),
        ),
        out_shape=jax.ShapeDtypeStruct((n_tp, tokens, per * cols), jnp.bfloat16),
        cost_estimate=pl.CostEstimate(
            flops=2 * tokens * depth * cols * len(pieces),
            bytes_accessed=2 * (tokens * depth + len(pieces) * cols * (depth + tokens)),
            transcendentals=0,
        ),
        name="columns_matmul",
    )(places, x, *pieces)


def shift_down(values, amount, fill):
    index = lax.broadcasted_iota(jnp.int32, values.shape, 0)
    return jnp.where(index < amount, fill, pltpu.roll(values, amount, 0))


def recurrence_kernel(
    side_ref, value_ref, gate_ref, own_ref, peer_ref, taps_ref, maps_ref, rate_ref, out_ref
):
    rows, channels = value_ref.shape
    reach = taps_ref.shape[0]
    per = LANES // maps_ref.shape[1]
    is_own = pl.program_id(0) < pl.num_programs(0) // 2
    for tile in range(channels // LANES):
        cols = slice(tile * LANES, (tile + 1) * LANES)
        values = value_ref[:, cols].astype(jnp.float32)
        filtered = taps_ref[reach - 1 : reach, cols] * values
        for back in range(1, reach):
            tap = taps_ref[reach - 1 - back : reach - back, cols]
            filtered = filtered + tap * shift_down(values, back, 0.0)
        conved = filtered.astype(jnp.bfloat16)
        maps = maps_ref[tile * per : (tile + 1) * per].reshape(LANES, 2 * LANES)
        logits = jnp.dot(conved, maps, preferred_element_type=jnp.float32)
        offset = jnp.where(is_own, own_ref[:, cols], peer_ref[:, cols].astype(jnp.float32))
        steps = 1.0 / (1.0 + jnp.exp(-logits))
        log_decay = steps[:, :LANES] * rate_ref[:, cols] + offset
        decay = jnp.exp(log_decay)
        y = -2.0 * log_decay
        series = 1.0 + y * (
            -1 / 2 + y * (1 / 6 + y * (-1 / 24 + y * (1 / 120 + y * (-1 / 720 + y * (1 / 5040)))))
        )
        lost = jnp.where(y < 0.35, y * series, 1.0 - decay * decay)
        state = jnp.sqrt(lost) * steps[:, LANES:] * conved.astype(jnp.float32)
        span = 1
        while span < rows:
            state = state + decay * shift_down(state, span, 0.0)
            if span * 2 < rows:
                decay = decay * shift_down(decay, span, 1.0)
            span *= 2
        gate = gate_ref[:, cols].astype(jnp.float32)
        gelu = 0.5 * gate * (1.0 + lax.erf(gate * 0.7071067811865476))
        out_ref[:, cols] = (state * gelu).astype(jnp.bfloat16)


def recurrence(projected, offset_own, offset_peer, taps, decay_maps, input_maps, rate, side):
    tokens = projected.shape[0]
    channels = offset_peer.shape[1]
    blocks, size, _ = decay_maps.shape
    per = LANES // size
    block = jnp.arange(blocks)[:, None, None] % per
    group = jnp.arange(LANES)[None, None, :] // size

    def diagonal(maps):
        return jnp.where(block == group, jnp.tile(maps, (1, 1, per)), 0)

    maps = jnp.concatenate([diagonal(decay_maps), diagonal(input_maps)], 2)
    sequences = tokens // SEQ_LEN
    own = sequences // 2
    return pl.pallas_call(
        recurrence_kernel,
        grid_spec=pltpu.PrefetchScalarGridSpec(
            num_scalar_prefetch=1,
            grid=(sequences,),
            in_specs=[
                pl.BlockSpec((SEQ_LEN, channels), lambda s, side: (s, 0)),
                pl.BlockSpec((SEQ_LEN, channels), lambda s, side: (s, 1)),
                pl.BlockSpec(
                    (SEQ_LEN, channels), lambda s, side: (jnp.minimum(s, own - 1), side[0])
                ),
                pl.BlockSpec((SEQ_LEN, channels), lambda s, side: (jnp.maximum(s - own, 0), 0)),
                pl.BlockSpec((taps.shape[0], channels), lambda s, side: (0, side[0])),
                pl.BlockSpec((blocks // 2, size, 2 * LANES), lambda s, side: (side[0], 0, 0)),
                pl.BlockSpec((1, channels), lambda s, side: (0, side[0])),
            ],
            out_specs=pl.BlockSpec((SEQ_LEN, channels), lambda s, side: (s, 0)),
        ),
        out_shape=jax.ShapeDtypeStruct((tokens, channels), jnp.bfloat16),
        cost_estimate=pl.CostEstimate(
            flops=tokens * channels * 700,
            bytes_accessed=tokens * channels * 10,
            transcendentals=tokens * channels * 6,
        ),
        name="recurrence",
    )(
        side.astype(jnp.int32)[None],
        projected,
        projected,
        offset_own,
        offset_peer,
        taps.astype(jnp.float32),
        maps,
        rate[None, :],
    )


def shards(
    sizes,
    stream,
    recurrent_norm_gain,
    feedforward_norm_gain,
    recurrent_input_weight,
    output_gate_weight,
    causal_filter_weight,
    decay_gate_matrix,
    input_gate_matrix,
    channel_decay_param,
    token_decay_offset,
    recurrent_output_weight,
    up_projection_weight,
    down_projection_weight,
):
    _, n_fs, n_tp = sizes
    ids = lax.axis_index("rep"), lax.axis_index("fs"), lax.axis_index("tp")
    _, fs, tp = ids
    side = fs % 2
    pairs = [(i, i ^ 1) for i in range(n_fs)]
    tokens = stream.shape[0]

    def halves(weight, axis):
        return half(weight, side, axis), half(weight, 1 - side, axis)

    def to_peer(values):
        return lax.ppermute(values, "fs", pairs)

    value_own, value_peer = halves(recurrent_input_weight, 1)
    gate_own, gate_peer = halves(output_gate_weight, 1)
    entry = (
        jnp.concatenate([value_own, gate_own], 1),
        jnp.concatenate([value_peer, gate_peer], 1),
    )
    entry_full = gather_shard(entry, ids, sizes)
    stream_peer = to_peer(stream)
    offset_peer = to_peer(half(token_decay_offset, 1 - side, 1).astype(jnp.bfloat16))
    output_full = gather_shard(halves(recurrent_output_weight, 0), ids, sizes)
    expand_full = gather_shard(halves(up_projection_weight, 1), ids, sizes)
    contract_full = gather_shard(halves(down_projection_weight, 0), ids, sizes)

    own_pair = jnp.concatenate([stream, stream_peer], 0)
    whole = gather_features(own_pair, tp, n_tp)
    normed = norm_rows(whole, recurrent_norm_gain)
    projected = depth_matmul(normed, entry_full)
    mixed = recurrence(
        projected,
        token_decay_offset,
        offset_peer,
        causal_filter_weight,
        decay_gate_matrix,
        input_gate_matrix,
        -DECAY_MULTIPLIER * jax.nn.softplus(-channel_decay_param),
        side,
    )
    mixer_terms = columns_matmul(mixed, output_full, n_tp, 0, 2 * tokens)
    mixer_chip = sum_features(mixer_terms, tp, n_tp)
    got_own = to_peer(mixer_chip[tokens:])
    got_peer = to_peer(mixer_chip[:tokens])
    update = mixer_chip.astype(jnp.float32) + jnp.concatenate([got_own, got_peer], 0).astype(
        jnp.float32
    )
    middle = (own_pair.astype(jnp.float32) + update).astype(jnp.bfloat16)
    normed_mid = norm_rows(gather_features(middle, tp, n_tp), feedforward_norm_gain)
    activity = depth_matmul(normed_mid, expand_full, squared=True)
    peer_terms = columns_matmul(activity, contract_full, n_tp, tokens, tokens)
    got = to_peer(sum_features(peer_terms, tp, n_tp))
    own_terms = columns_matmul(activity, contract_full, n_tp, 0, tokens)
    own_chip = sum_features(own_terms, tp, n_tp)
    channel_sum = own_chip.astype(jnp.float32) + got.astype(jnp.float32)
    return (middle[:tokens].astype(jnp.float32) + channel_sum).astype(jnp.bfloat16)


MESH = pl.DeviceIdType.MESH
CHUNK_ROWS = 128
AHEAD = (2, 2, 2, 3)


def whole_kernel(
    stream_hbm,
    offset_hbm,
    first_gain_ref,
    second_gain_ref,
    taps_ref,
    decay_maps_ref,
    input_maps_ref,
    param_ref,
    value_hbm,
    gate_hbm,
    output_hbm,
    raise_hbm,
    lower_hbm,
    out_ref,
    stream_ref,
    offset_ref,
    rate_ref,
    weights,
    normed,
    normed_mid,
    square_own,
    square_got,
    projected,
    mixed,
    offsets,
    offset_send,
    maps,
    kept,
    passed,
    got,
    mid_send,
    mid_got,
    middle,
    activity,
    partial,
    partial_got,
    last_send,
    last_got,
    local_sem,
    y_send,
    y_recv,
    z_send,
    z_recv,
    x_send,
    x_recv,
    act_send,
    act_recv,
    load_sem,
):
    rep, fs, tp = lax.axis_index("rep"), lax.axis_index("fs"), lax.axis_index("tp")
    z, y = fs // 2, fs % 2
    tokens, half_width = stream_ref.shape
    width = 2 * half_width
    chunks, _, n_fs, block, _ = weights.shape
    quarter = half_width // 2
    lane_tiles = half_width // LANES
    raises = (chunks - 3) // 2
    is_mid = jnp.logical_or(z == 1, z == 2)
    low = (z // 2) == tp

    def plane(m):
        return 2 * ((z // 2 + m // 2) % 2) + (z % 2 + m % 2) % 2

    x_peer = (1 - rep, fs, tp)
    y_peer = (rep, 2 * z + 1 - y, tp)
    t_peer = (rep, fs, 1 - tp)

    def z_peer(m):
        return (rep, 2 * plane(m) + y, tp)

    loads = (
        pltpu.make_async_copy(stream_hbm, stream_ref, load_sem.at[0]),
        pltpu.make_async_copy(offset_hbm, offset_ref, load_sem.at[1]),
    )
    for load in loads:
        load.start()

    barrier = pltpu.get_barrier_semaphore()
    for peer in (x_peer, y_peer, t_peer, z_peer(1), z_peer(2), z_peer(3)):
        pl.semaphore_signal(barrier, inc=1, device_id=peer, device_id_type=MESH)
    pl.semaphore_wait(barrier, 6)

    def remote(src, dst, send, recv, peer):
        return pltpu.make_async_remote_copy(
            src_ref=src, dst_ref=dst, send_sem=send, recv_sem=recv, device_id=peer, device_id_type=MESH
        )

    def shard_block(k, side, part):
        if k < 2 or 3 <= k < 3 + raises:
            ref = (value_hbm, gate_hbm)[k] if k < 2 else raise_hbm
            first = 0 if k < 2 else (k - 3) * quarter
            span = ref.shape[1] // 2
            start = pl.multiple_of(side * span + first + part * block, block)
            return ref.at[:, pl.ds(start, block)]
        ref = output_hbm if k == 2 else lower_hbm
        first = 0 if k == 2 else (k - 3 - raises) * quarter
        span = ref.shape[0] // 2
        start = pl.multiple_of(side * span + first + part * block, block)
        return ref.at[pl.ds(start, block), :]

    def part_of(q):
        return rep if q == 0 else 1 - rep

    def local_copy(k, q):
        part = part_of(q)
        return pltpu.make_async_copy(
            shard_block(k, y, part), weights.at[k, part, fs], local_sem.at[k, q]
        )

    def y_copy(k, q):
        part = part_of(q)
        return remote(
            shard_block(k, 1 - y, part), weights.at[k, part, fs], y_send.at[k, q], y_recv.at[k, q], y_peer
        )

    def z_copy(k, h, m):
        spot = weights.at[k, rep, fs if h == 0 else 2 * z + 1 - y]
        src = shard_block(k, y, rep) if h == 0 else spot
        return remote(src, spot, z_send.at[k, h, m - 1], z_recv.at[k, h, m - 1], z_peer(m))

    def z_relay(k, h):
        spot = weights.at[k, rep, 2 * plane(2) + (y if h == 0 else 1 - y)]
        return remote(spot, spot, z_send.at[k, h, 3], z_recv.at[k, h, 2], z_peer(1))

    def x_copy(k, h, m):
        spot = weights.at[k, rep, 2 * plane(m) + (y if h == 0 else 1 - y)]
        return remote(spot, spot, x_send.at[k, h, m - 1], x_recv.at[k, h, m - 1], x_peer)

    last_raise = 3 + raises
    lowers = range(last_raise, chunks)
    every = (2, 1, 3)
    events = [(k, h, every) for k, h in ((0, 0), (1, 0), (0, 1), (1, 1), (2, 0), (2, 1))]
    events += [(k, h, every) for h in range(2) for k in range(3, last_raise)]
    events += [(k, 0, every) for k in lowers]
    events += [(k, 1, (2, 3)) for k in lowers] + [(k, 1, (1,)) for k in lowers]

    def reach_of(index):
        return index + AHEAD[min(index, len(AHEAD) - 1)]

    def start_after(index):
        for later in range(reach_of(index - 1) + 1 if index else 2, reach_of(index) + 1):
            start(later)

    def start(index):
        if index >= len(events):
            return
        k, h, sources = events[index]
        if h == 1 and 2 in sources:
            y_copy(k, 0).wait_recv()
        for m in sources:
            if m < 3:
                z_copy(k, h, m).start()
            else:

                @pl.when(is_mid)
                def _():
                    z_copy(k, h, 3).start()

    def relay(k, h, m):
        z_copy(k, h, m).wait_recv()
        x_copy(k, h, m).start()

        @pl.when(jnp.logical_and(is_mid, m == 2))
        def _():
            z_relay(k, h).start()

    def advance(index):
        k, h, sources = events[index]
        for place, m in enumerate(sorted(sources)):
            relay(k, h, m)
            if place == 0:
                start_after(index)

    def advance_at(step, index):
        k, h, _ = events[index]

        @pl.when(step < 3)
        def _():
            relay(k, h, step + 1)

        @pl.when(step == 0)
        def _():
            start_after(index)

    def wait_own(k):
        for q in range(2):
            local_copy(k, q).wait()
        y_copy(k, 1).wait_recv()

    def wait_x(k, h):
        for m in (1, 2, 3):
            x_copy(k, h, m).wait_recv()

    def tp_copy(src, dst, slot):
        return remote(src, dst, act_send.at[slot], act_recv.at[slot], t_peer)

    def y_act(src, dst, slot):
        return remote(src, dst, act_send.at[slot], act_recv.at[slot], y_peer)

    def y_start(k):
        for q in range(2):
            y_copy(k, q).start()

    y_start(0)
    y_start(1)
    start(0)
    for k in range(chunks):
        for q in range(2):
            local_copy(k, q).start()

    own_columns = pl.ds(pl.multiple_of(tp * half_width, half_width), half_width)

    def squares(source, phase):
        def body(step, _):
            rows = pl.ds(pl.multiple_of(step * CHUNK_ROWS, CHUNK_ROWS), CHUNK_ROWS)
            total = None
            for tile in range(lane_tiles):
                value = source[rows, tile * LANES : (tile + 1) * LANES].astype(jnp.float32)
                total = value * value if total is None else total + value * value
            square_own[phase, rows, :] = total
            return 0

        lax.fori_loop(0, tokens // CHUNK_ROWS, body, 0)

    def square_copy(phase):
        return tp_copy(square_own.at[phase], square_got.at[phase], 9 + phase)

    def norm(source, phase, gain_ref, target):
        def body(step, _):
            rows = pl.ds(pl.multiple_of(step * CHUNK_ROWS, CHUNK_ROWS), CHUNK_ROWS)
            total = jnp.sum(square_own[phase, rows, :] + square_got[phase, rows, :], axis=1, keepdims=True)
            inverse = lax.rsqrt(total * (1.0 / width) + EPSILON)
            for tile in range(lane_tiles):
                value = source[rows, tile * LANES : (tile + 1) * LANES].astype(jnp.float32)
                gain = gain_ref[pl.ds(tp * lane_tiles + tile, 1), :]
                lanes = pl.ds(pl.multiple_of(tp * half_width + tile * LANES, LANES), LANES)
                target[y, rows, lanes] = (value * inverse * gain).astype(jnp.bfloat16)
            return 0

        lax.fori_loop(0, tokens // CHUNK_ROWS, body, 0)

    def block_copies(target, base):
        own = target.at[y, :, own_columns]
        theirs = target.at[1 - y, :, own_columns]
        return (
            tp_copy(own, own, base),
            y_act(own, own, base + 1),
            tp_copy(theirs, theirs, base + 2),
        )

    loads[0].wait()
    squares(stream_ref, 0)
    square_copy(0).start()
    loads[1].wait()
    mine = pl.ds(pl.multiple_of(y * quarter, quarter), quarter)
    peers = pl.ds(pl.multiple_of((1 - y) * quarter, quarter), quarter)
    offset_send[...] = offset_ref[:, peers].astype(jnp.bfloat16)
    offsets[0] = offset_ref[:, mine].astype(jnp.bfloat16)
    square_copy(0).wait_recv()
    norm(stream_ref, 0, first_gain_ref, normed)
    first_tp, first_y, first_pass = block_copies(normed, 0)
    first_tp.start()
    offset_copy = y_act(offset_send, offsets.at[1], 3)

    y_start(2)
    start(1)
    advance(0)
    first_y.start()
    advance(1)
    offset_copy.start()

    wide = jnp.exp(-jnp.abs(param_ref[...]))
    ratio = wide / (2.0 + wide)
    ratio_square = ratio * ratio
    log_sum = jnp.ones_like(ratio) * (1.0 / 17.0)
    for odd in (15.0, 13.0, 11.0, 9.0, 7.0, 5.0, 3.0, 1.0):
        log_sum = log_sum * ratio_square + 1.0 / odd
    rate_ref[...] = -DECAY_MULTIPLIER * (jnp.maximum(-param_ref[...], 0.0) + 2.0 * ratio * log_sum)

    size = decay_maps_ref.shape[1]
    per = LANES // size
    tiles = quarter // LANES
    maps[...] = jnp.zeros_like(maps)
    for tile in range(tiles):
        for index in range(per):
            place = y * (tiles * per) + tile * per + index
            span = slice(index * size, (index + 1) * size)
            maps[tile, span, index * size : (index + 1) * size] = decay_maps_ref[place]
            maps[tile, span, LANES + index * size : LANES + (index + 1) * size] = input_maps_ref[place]

    advance(2)
    for k in range(3, last_raise):
        y_start(k)
    advance(3)
    first_y.wait_recv()
    first_pass.start()

    for k in range(2):
        wait_own(k)
    for k in range(2):
        for h in range(2):
            wait_x(k, h)
    first_tp.wait_recv()

    def project(which, token_block, event):
        def body(step, _):
            if event is not None:
                advance_at(step, event)
            matrix = weights[step // 2, step % 2].reshape(width, block)
            projected[which, step] = jnp.dot(
                normed[token_block], matrix, preferred_element_type=jnp.float32
            ).astype(jnp.bfloat16)
            return 0

        lax.fori_loop(0, 4, body, 0)

    reach = taps_ref.shape[0]

    def recur(which, event):
        def body(step, _):
            if event is not None:
                advance_at(step, event)
            rows = pl.ds(pl.multiple_of(step * SEQ_LEN, SEQ_LEN), SEQ_LEN)
            for tile in range(tiles):
                part, lane = tile * LANES // block, tile * LANES % block
                lanes = slice(lane, lane + LANES)
                taps = taps_ref[
                    :, pl.ds(pl.multiple_of(y * quarter + tile * LANES, LANES), LANES)
                ].astype(jnp.float32)
                values = projected[which, part, rows, lanes].astype(jnp.float32)
                filtered = taps[reach - 1 : reach] * values
                for back in range(1, reach):
                    tap = taps[reach - 1 - back : reach - back]
                    filtered = filtered + tap * shift_down(values, back, 0.0)
                conved = filtered.astype(jnp.bfloat16)
                logits = jnp.dot(conved, maps[tile], preferred_element_type=jnp.float32)
                offset = offsets[which, rows, tile * LANES : (tile + 1) * LANES].astype(jnp.float32)
                steps = 1.0 / (1.0 + jnp.exp(-logits))
                rate = rate_ref[pl.ds(y * tiles + tile, 1), :]
                log_decay = steps[:, :LANES] * rate + offset
                decay = jnp.exp(log_decay)
                twice = -2.0 * log_decay
                series = 1.0 + twice * (
                    -1 / 2
                    + twice
                    * (1 / 6 + twice * (-1 / 24 + twice * (1 / 120 + twice * (-1 / 720 + twice * (1 / 5040)))))
                )
                lost = jnp.where(twice < 0.35, twice * series, 1.0 - decay * decay)
                state = jnp.sqrt(lost) * steps[:, LANES:] * conved.astype(jnp.float32)
                span = 1
                while span < SEQ_LEN:
                    state = state + decay * shift_down(state, span, 0.0)
                    if span * 2 < SEQ_LEN:
                        decay = decay * shift_down(decay, span, 1.0)
                    span *= 2
                gate = projected[which, 2 + part, rows, lanes].astype(jnp.float32)
                gelu = 0.5 * gate * (1.0 + lax.erf(gate * 0.7071067811865476))
                mixed[which, rows, tile * LANES : (tile + 1) * LANES] = (state * gelu).astype(jnp.bfloat16)
            return 0

        lax.fori_loop(0, tokens // SEQ_LEN, body, 0)

    project(0, y, 4)
    recur(0, None)
    first_pass.wait_recv()
    project(1, 1 - y, None)
    offset_copy.wait_recv()
    recur(1, 5)

    wait_own(2)
    wait_x(2, 0)
    wait_x(2, 1)

    def mix_out(which):
        def body(step, _):
            def term(place):
                matrix = weights[2, :, place].reshape(quarter, block)
                return jnp.dot(mixed[which], matrix, preferred_element_type=jnp.float32).astype(jnp.bfloat16)

            lanes = pl.ds(pl.multiple_of(step * block, block), block)
            per_half = n_fs // 2
            passed[which, :, lanes] = term(per_half * (1 - tp) + step)
            kept[which, :, lanes] = term(per_half * tp + step)
            return 0

        lax.fori_loop(0, n_fs // 2, body, 0)

    def mix_copy(which):
        return tp_copy(passed.at[which], got.at[which], 4 + which)

    mix_out(1)
    mix_copy(1).start()
    mix_out(0)
    mix_copy(0).start()

    def add_peer(step, _):
        rows = pl.ds(pl.multiple_of(step * CHUNK_ROWS, CHUNK_ROWS), CHUNK_ROWS)
        mid_send[rows, :] = (
            kept[1, rows, :].astype(jnp.float32) + got[1, rows, :].astype(jnp.float32)
        ).astype(jnp.bfloat16)
        return 0

    mix_copy(1).wait_recv()
    lax.fori_loop(0, tokens // CHUNK_ROWS, add_peer, 0)
    mid_copy = y_act(mid_send, mid_got, 6)
    mid_copy.start()

    y_start(last_raise)
    up = 6
    for index in range(raises):
        advance(up + index)
    mix_copy(0).wait_recv()

    mid_copy.wait_recv()

    def add_own(step, _):
        rows = pl.ds(pl.multiple_of(step * CHUNK_ROWS, CHUNK_ROWS), CHUNK_ROWS)
        total = None
        for tile in range(lane_tiles):
            lanes = slice(tile * LANES, (tile + 1) * LANES)
            update = kept[0, rows, lanes].astype(jnp.float32) + got[0, rows, lanes].astype(jnp.float32)
            update = update + mid_got[rows, lanes].astype(jnp.float32)
            value = (stream_ref[rows, lanes].astype(jnp.float32) + update).astype(jnp.bfloat16)
            middle[rows, lanes] = value
            value = value.astype(jnp.float32)
            total = value * value if total is None else total + value * value
        square_own[1, rows, :] = total
        return 0

    lax.fori_loop(0, tokens // CHUNK_ROWS, add_own, 0)
    square_copy(1).start()
    square_copy(1).wait_recv()
    norm(middle, 1, second_gain_ref, normed_mid)
    second_tp, second_y, second_pass = block_copies(normed_mid, 11)
    second_y.start()
    second_tp.start()
    for k in range(last_raise + 1, chunks):
        y_start(k)
    for index in range(raises):
        advance(up + raises + index)
    down = up + 2 * raises
    for k in range(3, last_raise):
        if k == last_raise - 1:
            advance(down)
        wait_own(k)
        wait_x(k, 0)
        wait_x(k, 1)

    def lift(which, token_block, event):
        def body(step, _):
            if event is not None:
                advance_at(step, event)
            matrix = weights[3 + step // 2, step % 2].reshape(width, block)
            total = jnp.dot(normed_mid[token_block], matrix, preferred_element_type=jnp.float32)
            lanes = pl.ds(pl.multiple_of(step * block, block), block)
            activity[which, :, lanes] = jnp.square(jnp.maximum(total, 0.0)).astype(jnp.bfloat16)
            return 0

        lax.fori_loop(0, 2 * raises, body, 0)

    second_tp.wait_recv()
    lift(0, y, None)
    second_y.wait_recv()
    second_pass.start()
    second_pass.wait_recv()
    lift(1, 1 - y, down + 1)
    for index in range(2, raises):
        advance(down + index)

    depth = raises * quarter

    def lower(h, m):
        place = 2 * plane(m) + (y if h == 0 else 1 - y)

        def body(which, _):
            matrix = weights[last_raise:chunks, :, place].reshape(depth, block)
            partial[m, h, which] = jnp.dot(
                activity[which], matrix, preferred_element_type=jnp.float32
            ).astype(jnp.bfloat16)
            return 0

        lax.fori_loop(0, 2, body, 0)

    def is_owner(m):
        return low if m < 2 else jnp.logical_not(low)

    def owner_copy(h, m):
        slot = 14 + 2 * (m % 2) + h
        return tp_copy(partial.at[m, h], partial_got.at[m % 2, h], slot)

    def last_copy(h, m):
        slot = 18 + 2 * (m % 2)
        return remote(
            last_send.at[m % 2, h],
            last_got.at[m % 2, 1 - h],
            act_send.at[slot + h],
            act_recv.at[slot + 1 - h],
            y_peer,
        )

    def pass_on(h, m):
        @pl.when(jnp.logical_not(is_owner(m)))
        def _():
            owner_copy(h, m).start()

    def finish(h, m):
        @pl.when(is_owner(m))
        def _():
            owner_copy(h, m).wait_recv()

            def body(step, _):
                rows = pl.ds(pl.multiple_of(step * CHUNK_ROWS, CHUNK_ROWS), CHUNK_ROWS)
                last_send[m % 2, h, rows, :] = (
                    partial[m, h, 1, rows, :].astype(jnp.float32)
                    + partial_got[m % 2, h, 1, rows, :].astype(jnp.float32)
                ).astype(jnp.bfloat16)
                return 0

            lax.fori_loop(0, tokens // CHUNK_ROWS, body, 0)
            last_copy(h, m).start()

    def close(h, mm):
        owned = mm + 2 * (1 - low.astype(jnp.int32))
        last_copy(1 - h, mm).wait_recv()
        place = 2 * ((z % 2 + mm) % 2) + (y if h == 0 else 1 - y)
        lanes = pl.ds(pl.multiple_of(place * block, block), block)

        def body(step, _):
            rows = pl.ds(pl.multiple_of(step * CHUNK_ROWS, CHUNK_ROWS), CHUNK_ROWS)
            update = (
                partial[owned, h, 0, rows, :].astype(jnp.float32)
                + partial_got[mm, h, 0, rows, :].astype(jnp.float32)
                + last_got[mm, h, rows, :].astype(jnp.float32)
            )
            out_ref[rows, lanes] = (middle[rows, lanes].astype(jnp.float32) + update).astype(jnp.bfloat16)
            return 0

        lax.fori_loop(0, tokens // CHUNK_ROWS, body, 0)

    def wait_sends(places):
        for k in places:
            for q in range(2):
                y_copy(k, q).wait_send()
            for h in range(2):
                z_copy(k, h, 1).wait_send()
                z_copy(k, h, 2).wait_send()

                @pl.when(is_mid)
                def _():
                    z_copy(k, h, 3).wait_send()
                    z_relay(k, h).wait_send()

                for m in (1, 2, 3):
                    x_copy(k, h, m).wait_send()

    order = [(0, m) for m in range(4)] + [(1, m) for m in (0, 2, 3, 1)]
    far, near = down + raises, down + 2 * raises
    advance(far)
    for k in lowers:
        wait_own(k)
        wait_x(k, 0)
    wait_sends(range(last_raise))
    for index, (h, m) in enumerate(order):
        if index in (2, 4):
            advance(far + index // 2)
        if index >= 5:
            advance(near + index - 5)
        if h == 1 and m:
            for k in lowers:
                x_copy(k, 1, m).wait_recv()
        lower(h, m)
        pass_on(h, m)
        if index:
            finish(*order[index - 1])
    finish(*order[-1])
    for h in range(2):
        for mm in range(2):
            close(h, mm)

    wait_sends(lowers)
    for copy in (first_tp, first_y, first_pass, second_tp, second_y, second_pass, offset_copy, mid_copy):
        copy.wait_send()
    for phase in range(2):
        square_copy(phase).wait_send()
        mix_copy(phase).wait_send()
    for h, m in order:

        @pl.when(is_owner(m))
        def _():
            last_copy(h, m).wait_send()

        @pl.when(jnp.logical_not(is_owner(m)))
        def _():
            owner_copy(h, m).wait_send()


def whole_layer(
    stream,
    recurrent_norm_gain,
    feedforward_norm_gain,
    recurrent_input_weight,
    output_gate_weight,
    causal_filter_weight,
    decay_gate_matrix,
    input_gate_matrix,
    channel_decay_param,
    token_decay_offset,
    recurrent_output_weight,
    up_projection_weight,
    down_projection_weight,
):
    tokens, half_width = stream.shape
    width = 2 * half_width
    quarter = half_width // 2
    block, n_fs = quarter // 2, 8
    raises = up_projection_weight.shape[1] // half_width
    chunks = 3 + 2 * raises
    depth = raises * quarter
    tiles = quarter // LANES
    half_type, full_type = jnp.bfloat16, jnp.float32
    vmem = pl.BlockSpec(memory_space=pltpu.VMEM)
    anywhere = pl.BlockSpec(memory_space=pl.ANY)
    dma = pltpu.SemaphoreType.DMA
    return pl.pallas_call(
        whole_kernel,
        out_shape=jax.ShapeDtypeStruct((tokens, half_width), half_type),
        in_specs=[anywhere] * 2 + [vmem] * 6 + [anywhere] * 5,
        out_specs=vmem,
        scratch_shapes=[
            pltpu.VMEM((tokens, half_width), half_type),
            pltpu.VMEM((tokens, half_width), full_type),
            pltpu.VMEM((half_width // LANES, LANES), full_type),
            pltpu.VMEM((chunks, 2, n_fs, block, block), half_type),
            pltpu.VMEM((2, tokens, width), half_type),
            pltpu.VMEM((2, tokens, width), half_type),
            pltpu.VMEM((2, tokens, LANES), full_type),
            pltpu.VMEM((2, tokens, LANES), full_type),
            pltpu.VMEM((2, 4, tokens, block), half_type),
            pltpu.VMEM((2, tokens, quarter), half_type),
            pltpu.VMEM((2, tokens, quarter), half_type),
            pltpu.VMEM((tokens, quarter), half_type),
            pltpu.VMEM((tiles, LANES, 2 * LANES), half_type),
            pltpu.VMEM((2, tokens, half_width), half_type),
            pltpu.VMEM((2, tokens, half_width), half_type),
            pltpu.VMEM((2, tokens, half_width), half_type),
            pltpu.VMEM((tokens, half_width), half_type),
            pltpu.VMEM((tokens, half_width), half_type),
            pltpu.VMEM((tokens, half_width), half_type),
            pltpu.VMEM((2, tokens, depth), half_type),
            pltpu.VMEM((4, 2, 2, tokens, block), half_type),
            pltpu.VMEM((2, 2, 2, tokens, block), half_type),
            pltpu.VMEM((2, 2, tokens, block), half_type),
            pltpu.VMEM((2, 2, tokens, block), half_type),
            dma((chunks, 2)),
            dma((chunks, 2)),
            dma((chunks, 2)),
            dma((chunks, 2, 4)),
            dma((chunks, 2, 3)),
            dma((chunks, 2, 3)),
            dma((chunks, 2, 3)),
            dma((22,)),
            dma((22,)),
            dma((2,)),
        ],
        compiler_params=pltpu.CompilerParams(
            collective_id=0, has_side_effects=True, vmem_limit_bytes=67043328
        ),
        name="whole_layer",
    )(
        stream,
        token_decay_offset,
        recurrent_norm_gain.reshape(-1, LANES),
        feedforward_norm_gain.reshape(-1, LANES),
        causal_filter_weight,
        decay_gate_matrix,
        input_gate_matrix,
        channel_decay_param.reshape(-1, LANES),
        recurrent_input_weight,
        output_gate_weight,
        recurrent_output_weight,
        up_projection_weight,
        down_projection_weight,
    )


def fits_whole(sizes, stream, up_projection_weight, decay_gate_matrix):
    tokens, half_width = stream.shape
    return (
        sizes == (2, 8, 2)
        and half_width % (8 * LANES) == 0
        and tokens % (4 * SEQ_LEN) == 0
        and up_projection_weight.shape[1] % half_width == 0
        and up_projection_weight.shape[1] // half_width >= 2
        and LANES % decay_gate_matrix.shape[1] == 0
    )


def solution(mesh):
    in_specs = (
        P(("rep", "fs"), "tp"),
        P(),
        P(),
        P("fs", "tp"),
        P("fs", "tp"),
        P(None, "tp"),
        P("tp", None, None),
        P("tp", None, None),
        P("tp"),
        P(("rep", "fs"), "tp"),
        P("tp", "fs"),
        P("fs", "tp"),
        P("tp", "fs"),
    )
    out_specs = P(("rep", "fs"), "tp")
    sizes = tuple(mesh.shape[axis] for axis in ("rep", "fs", "tp"))

    def body(*args):
        if fits_whole(sizes, args[0], args[11], args[6]):
            return whole_layer(*args)
        return shards(sizes, *args)

    return jax.shard_map(
        body, mesh=mesh, in_specs=in_specs, out_specs=out_specs, check_vma=False
    )
```

```python
import functools

import jax
import jax.numpy as jnp
from jax import lax
from jax.experimental import pallas as pl
from jax.experimental.pallas import tpu as pltpu
from jax.sharding import PartitionSpec as P


SEQ_LEN = 128
EPSILON = 1e-06
DECAY_MULTIPLIER = 8.0
LANES = 128


def half(values, which, axis):
    first, second = jnp.split(values, 2, axis)
    return jnp.where(which == 0, first, second)


def gather_shard(shard, ids, sizes):
    rep, fs, _ = ids
    _, n_fs, _ = sizes
    own, for_peer = shard
    hops = n_fs // 2
    place, side = fs // 2, fs % 2
    from_peer = lax.ppermute(for_peer, "fs", [(i, i ^ 1) for i in range(n_fs)])
    start = jnp.where(side == rep, own, from_peer)
    up = [(i, (i + 2) % n_fs) for i in range(n_fs)]
    down = [(i, (i + n_fs - 2) % n_fs) for i in range(n_fs)]
    pieces, places = [own, from_peer], [fs, fs ^ 1]
    below = above = start
    for step in range(1, hops):
        if step % 2:
            below = mine = lax.ppermute(below, "fs", up)
            base = 2 * ((place + hops - (step + 1) // 2) % hops)
        else:
            above = mine = lax.ppermute(above, "fs", down)
            base = 2 * ((place + step // 2) % hops)
        pieces += [mine, lax.ppermute(mine, "rep", [(0, 1), (1, 0)])]
        places += [base + rep, base + 1 - rep]
    return pieces, jnp.stack(places).astype(jnp.int32)


def gather_features(values, tp, n_tp):
    if n_tp != 2:
        return lax.all_gather(values, "tp", axis=1, tiled=True)
    other = lax.ppermute(values, "tp", [(0, 1), (1, 0)])
    return jnp.where(
        tp == 0, jnp.concatenate([values, other], 1), jnp.concatenate([other, values], 1)
    )


def sum_features(parts, tp, n_tp):
    total = lax.dynamic_index_in_dim(parts, tp, 0, False).astype(jnp.float32)
    for shift in range(1, n_tp):
        piece = lax.dynamic_index_in_dim(parts, (tp + shift) % n_tp, 0, False)
        got = lax.ppermute(piece, "tp", [(i, (i + shift) % n_tp) for i in range(n_tp)])
        total = total + got.astype(jnp.float32)
    return total.astype(jnp.bfloat16)


def norm_rows(values, gain):
    widened = values.astype(jnp.float32)
    inverse = lax.rsqrt(jnp.mean(widened * widened, axis=-1, keepdims=True) + EPSILON)
    return (widened * inverse * gain).astype(jnp.bfloat16)


ROWS = 256
CHUNK = 512


def depth_kernel(squared, places_ref, x_ref, *refs):
    *pieces, out_ref = refs
    depth, width = pieces[0].shape
    chunk = min(CHUNK, width)
    for lower in range(0, width, chunk):
        cols = slice(lower, lower + chunk)
        total = None
        for index, piece in enumerate(pieces):
            place = pl.multiple_of(places_ref[index] * depth, depth)
            term = jnp.dot(
                x_ref[:, pl.ds(place, depth)], piece[:, cols], preferred_element_type=jnp.float32
            )
            total = term if total is None else total + term
        if squared:
            total = jnp.square(jnp.maximum(total, 0.0))
        out_ref[:, cols] = total.astype(jnp.bfloat16)


def depth_matmul(x, gathered, squared=False):
    pieces, places = gathered
    tokens, width = x.shape
    shape = pieces[0].shape
    return pl.pallas_call(
        functools.partial(depth_kernel, squared),
        grid_spec=pltpu.PrefetchScalarGridSpec(
            num_scalar_prefetch=1,
            grid=(tokens // ROWS,),
            in_specs=[pl.BlockSpec((ROWS, width), lambda m, _: (m, 0))]
            + [pl.BlockSpec(shape, lambda m, _: (0, 0))] * len(pieces),
            out_specs=pl.BlockSpec((ROWS, shape[1]), lambda m, _: (m, 0)),
        ),
        out_shape=jax.ShapeDtypeStruct((tokens, shape[1]), jnp.bfloat16),
        cost_estimate=pl.CostEstimate(
            flops=2 * tokens * width * shape[1],
            bytes_accessed=2 * (tokens * width + (tokens + width) * shape[1]),
            transcendentals=0,
        ),
        name="depth_matmul",
    )(places, x, *pieces)


def columns_kernel(per, places_ref, x_ref, *refs):
    *pieces, out_ref = refs
    cols = pieces[0].shape[1]
    for index, piece in enumerate(pieces):
        place = places_ref[index]
        lower = pl.multiple_of((place % per) * cols, cols)
        out_ref[place // per, :, pl.ds(lower, cols)] = jnp.dot(
            x_ref[...], piece[...], preferred_element_type=jnp.float32
        ).astype(jnp.bfloat16)


def columns_matmul(x, gathered, n_tp, first, tokens):
    pieces, places = gathered
    depth, cols = pieces[0].shape
    per = len(pieces) // n_tp
    skip = first // ROWS
    return pl.pallas_call(
        functools.partial(columns_kernel, per),
        grid_spec=pltpu.PrefetchScalarGridSpec(
            num_scalar_prefetch=1,
            grid=(tokens // ROWS,),
            in_specs=[pl.BlockSpec((ROWS, depth), lambda m, _: (m + skip, 0))]
            + [pl.BlockSpec((depth, cols), lambda m, _: (0, 0))] * len(pieces),
            out_specs=pl.BlockSpec((n_tp, ROWS, per * cols), lambda m, _: (0, m, 0)),
        ),
        out_shape=jax.ShapeDtypeStruct((n_tp, tokens, per * cols), jnp.bfloat16),
        cost_estimate=pl.CostEstimate(
            flops=2 * tokens * depth * cols * len(pieces),
            bytes_accessed=2 * (tokens * depth + len(pieces) * cols * (depth + tokens)),
            transcendentals=0,
        ),
        name="columns_matmul",
    )(places, x, *pieces)


def shift_down(values, amount, fill):
    index = lax.broadcasted_iota(jnp.int32, values.shape, 0)
    return jnp.where(index < amount, fill, pltpu.roll(values, amount, 0))


def recurrence_kernel(
    side_ref, value_ref, gate_ref, own_ref, peer_ref, taps_ref, maps_ref, rate_ref, out_ref
):
    rows, channels = value_ref.shape
    reach = taps_ref.shape[0]
    per = LANES // maps_ref.shape[1]
    is_own = pl.program_id(0) < pl.num_programs(0) // 2
    for tile in range(channels // LANES):
        cols = slice(tile * LANES, (tile + 1) * LANES)
        values = value_ref[:, cols].astype(jnp.float32)
        filtered = taps_ref[reach - 1 : reach, cols] * values
        for back in range(1, reach):
            tap = taps_ref[reach - 1 - back : reach - back, cols]
            filtered = filtered + tap * shift_down(values, back, 0.0)
        conved = filtered.astype(jnp.bfloat16)
        maps = maps_ref[tile * per : (tile + 1) * per].reshape(LANES, 2 * LANES)
        logits = jnp.dot(conved, maps, preferred_element_type=jnp.float32)
        offset = jnp.where(is_own, own_ref[:, cols], peer_ref[:, cols].astype(jnp.float32))
        steps = 1.0 / (1.0 + jnp.exp(-logits))
        log_decay = steps[:, :LANES] * rate_ref[:, cols] + offset
        decay = jnp.exp(log_decay)
        y = -2.0 * log_decay
        series = 1.0 + y * (
            -1 / 2 + y * (1 / 6 + y * (-1 / 24 + y * (1 / 120 + y * (-1 / 720 + y * (1 / 5040)))))
        )
        lost = jnp.where(y < 0.35, y * series, 1.0 - decay * decay)
        state = jnp.sqrt(lost) * steps[:, LANES:] * conved.astype(jnp.float32)
        span = 1
        while span < rows:
            state = state + decay * shift_down(state, span, 0.0)
            if span * 2 < rows:
                decay = decay * shift_down(decay, span, 1.0)
            span *= 2
        gate = gate_ref[:, cols].astype(jnp.float32)
        gelu = 0.5 * gate * (1.0 + lax.erf(gate * 0.7071067811865476))
        out_ref[:, cols] = (state * gelu).astype(jnp.bfloat16)


def recurrence(projected, offset_own, offset_peer, taps, decay_maps, input_maps, rate, side):
    tokens = projected.shape[0]
    channels = offset_peer.shape[1]
    blocks, size, _ = decay_maps.shape
    per = LANES // size
    block = jnp.arange(blocks)[:, None, None] % per
    group = jnp.arange(LANES)[None, None, :] // size

    def diagonal(maps):
        return jnp.where(block == group, jnp.tile(maps, (1, 1, per)), 0)

    maps = jnp.concatenate([diagonal(decay_maps), diagonal(input_maps)], 2)
    sequences = tokens // SEQ_LEN
    own = sequences // 2
    return pl.pallas_call(
        recurrence_kernel,
        grid_spec=pltpu.PrefetchScalarGridSpec(
            num_scalar_prefetch=1,
            grid=(sequences,),
            in_specs=[
                pl.BlockSpec((SEQ_LEN, channels), lambda s, side: (s, 0)),
                pl.BlockSpec((SEQ_LEN, channels), lambda s, side: (s, 1)),
                pl.BlockSpec(
                    (SEQ_LEN, channels), lambda s, side: (jnp.minimum(s, own - 1), side[0])
                ),
                pl.BlockSpec((SEQ_LEN, channels), lambda s, side: (jnp.maximum(s - own, 0), 0)),
                pl.BlockSpec((taps.shape[0], channels), lambda s, side: (0, side[0])),
                pl.BlockSpec((blocks // 2, size, 2 * LANES), lambda s, side: (side[0], 0, 0)),
                pl.BlockSpec((1, channels), lambda s, side: (0, side[0])),
            ],
            out_specs=pl.BlockSpec((SEQ_LEN, channels), lambda s, side: (s, 0)),
        ),
        out_shape=jax.ShapeDtypeStruct((tokens, channels), jnp.bfloat16),
        cost_estimate=pl.CostEstimate(
            flops=tokens * channels * 700,
            bytes_accessed=tokens * channels * 10,
            transcendentals=tokens * channels * 6,
        ),
        name="recurrence",
    )(
        side.astype(jnp.int32)[None],
        projected,
        projected,
        offset_own,
        offset_peer,
        taps.astype(jnp.float32),
        maps,
        rate[None, :],
    )


def shards(
    sizes,
    stream,
    recurrent_norm_gain,
    feedforward_norm_gain,
    recurrent_input_weight,
    output_gate_weight,
    causal_filter_weight,
    decay_gate_matrix,
    input_gate_matrix,
    channel_decay_param,
    token_decay_offset,
    recurrent_output_weight,
    up_projection_weight,
    down_projection_weight,
):
    _, n_fs, n_tp = sizes
    ids = lax.axis_index("rep"), lax.axis_index("fs"), lax.axis_index("tp")
    _, fs, tp = ids
    side = fs % 2
    pairs = [(i, i ^ 1) for i in range(n_fs)]
    tokens = stream.shape[0]

    def halves(weight, axis):
        return half(weight, side, axis), half(weight, 1 - side, axis)

    def to_peer(values):
        return lax.ppermute(values, "fs", pairs)

    value_own, value_peer = halves(recurrent_input_weight, 1)
    gate_own, gate_peer = halves(output_gate_weight, 1)
    entry = (
        jnp.concatenate([value_own, gate_own], 1),
        jnp.concatenate([value_peer, gate_peer], 1),
    )
    entry_full = gather_shard(entry, ids, sizes)
    stream_peer = to_peer(stream)
    offset_peer = to_peer(half(token_decay_offset, 1 - side, 1).astype(jnp.bfloat16))
    output_full = gather_shard(halves(recurrent_output_weight, 0), ids, sizes)
    expand_full = gather_shard(halves(up_projection_weight, 1), ids, sizes)
    contract_full = gather_shard(halves(down_projection_weight, 0), ids, sizes)

    own_pair = jnp.concatenate([stream, stream_peer], 0)
    whole = gather_features(own_pair, tp, n_tp)
    normed = norm_rows(whole, recurrent_norm_gain)
    projected = depth_matmul(normed, entry_full)
    mixed = recurrence(
        projected,
        token_decay_offset,
        offset_peer,
        causal_filter_weight,
        decay_gate_matrix,
        input_gate_matrix,
        -DECAY_MULTIPLIER * jax.nn.softplus(-channel_decay_param),
        side,
    )
    mixer_terms = columns_matmul(mixed, output_full, n_tp, 0, 2 * tokens)
    mixer_chip = sum_features(mixer_terms, tp, n_tp)
    got_own = to_peer(mixer_chip[tokens:])
    got_peer = to_peer(mixer_chip[:tokens])
    update = mixer_chip.astype(jnp.float32) + jnp.concatenate([got_own, got_peer], 0).astype(
        jnp.float32
    )
    middle = (own_pair.astype(jnp.float32) + update).astype(jnp.bfloat16)
    normed_mid = norm_rows(gather_features(middle, tp, n_tp), feedforward_norm_gain)
    activity = depth_matmul(normed_mid, expand_full, squared=True)
    peer_terms = columns_matmul(activity, contract_full, n_tp, tokens, tokens)
    got = to_peer(sum_features(peer_terms, tp, n_tp))
    own_terms = columns_matmul(activity, contract_full, n_tp, 0, tokens)
    own_chip = sum_features(own_terms, tp, n_tp)
    channel_sum = own_chip.astype(jnp.float32) + got.astype(jnp.float32)
    return (middle[:tokens].astype(jnp.float32) + channel_sum).astype(jnp.bfloat16)


MESH = pl.DeviceIdType.MESH
CHUNK_ROWS = 128
AHEAD = (1, 1, 1, 2, 3)
END_AHEAD = (1, 1, 1, 2, 3)
LEAD = 2
END_ORDER = (
    (0, 1), (0, 2), (1, 1), (0, 3), (1, 2), (2, 1), (1, 3), (2, 2), (3, 1), (2, 3), (3, 2), (3, 3),
)


def whole_kernel(
    stream_hbm,
    offset_hbm,
    first_gain_ref,
    second_gain_ref,
    taps_ref,
    decay_maps_ref,
    input_maps_ref,
    param_ref,
    value_hbm,
    gate_hbm,
    output_hbm,
    raise_hbm,
    lower_hbm,
    out_ref,
    stream_ref,
    offset_ref,
    rate_ref,
    weights,
    normed,
    normed_mid,
    square_own,
    square_got,
    projected,
    mixed,
    offsets,
    offset_send,
    maps,
    kept,
    passed,
    got,
    mid_send,
    mid_got,
    middle,
    activity,
    partial,
    partial_got,
    last_send,
    last_got,
    local_sem,
    y_send,
    y_recv,
    z_send,
    z_recv,
    x_send,
    x_recv,
    act_send,
    act_recv,
    load_sem,
):
    rep, fs, tp = lax.axis_index("rep"), lax.axis_index("fs"), lax.axis_index("tp")
    z, y = fs // 2, fs % 2
    tokens, half_width = stream_ref.shape
    width = 2 * half_width
    chunks, _, n_fs, block, _ = weights.shape
    quarter = half_width // 2
    lane_tiles = half_width // LANES
    raises = (chunks - 3) // 2
    last_raise = 3 + raises
    lowers = range(last_raise, chunks)
    is_mid = jnp.logical_or(z == 1, z == 2)
    is_end = jnp.logical_not(is_mid)
    low = (z // 2) == tp

    def plane(m):
        return 2 * ((z // 2 + m // 2) % 2) + (z % 2 + m % 2) % 2

    x_peer = (1 - rep, fs, tp)
    y_peer = (rep, 2 * z + 1 - y, tp)
    t_peer = (rep, fs, 1 - tp)

    def z_peer(m):
        return (rep, 2 * plane(m) + y, tp)

    loads = (
        pltpu.make_async_copy(stream_hbm, stream_ref, load_sem.at[0]),
        pltpu.make_async_copy(offset_hbm, offset_ref, load_sem.at[1]),
    )
    for load in loads:
        load.start()

    barrier = pltpu.get_barrier_semaphore()
    for peer in (x_peer, y_peer, t_peer, z_peer(1), z_peer(2), z_peer(3)):
        pl.semaphore_signal(barrier, inc=1, device_id=peer, device_id_type=MESH)
    pl.semaphore_wait(barrier, 6)

    def remote(src, dst, send, recv, peer):
        return pltpu.make_async_remote_copy(
            src_ref=src, dst_ref=dst, send_sem=send, recv_sem=recv, device_id=peer, device_id_type=MESH
        )

    def shard_block(k, side, part):
        if k < 2 or 3 <= k < 3 + raises:
            ref = (value_hbm, gate_hbm)[k] if k < 2 else raise_hbm
            first = 0 if k < 2 else (k - 3) * quarter
            span = ref.shape[1] // 2
            start = pl.multiple_of(side * span + first + part * block, block)
            return ref.at[:, pl.ds(start, block)]
        ref = output_hbm if k == 2 else lower_hbm
        first = 0 if k == 2 else (k - 3 - raises) * quarter
        span = ref.shape[0] // 2
        start = pl.multiple_of(side * span + first + part * block, block)
        return ref.at[pl.ds(start, block), :]

    def part_of(q):
        return rep if q == 0 else 1 - rep

    def local_copy(k, q):
        part = part_of(q)
        return pltpu.make_async_copy(
            shard_block(k, y, part), weights.at[k, part, fs], local_sem.at[0]
        )

    def group_of(k):
        return 0 if k < 2 else 1 if k == 2 else 2 if k < last_raise else 3

    def y_slot(k, q):
        return k if q == 0 else chunks + group_of(k)

    def x_slot(k, h, m):
        if k < last_raise:
            return group_of(k) if k < 3 else k - 1
        return 1 + raises + (1 if h == 0 else 1 + m)

    def count_wait(ref, sem):
        pltpu.make_async_copy(ref, ref, sem).wait()

    def y_copy(k, q):
        part = part_of(q)
        return remote(
            shard_block(k, 1 - y, part), weights.at[k, part, fs], y_send.at[0], y_recv.at[y_slot(k, q)], y_peer
        )

    def z_copy(k, h, m):
        spot = weights.at[k, rep, fs if h == 0 else 2 * z + 1 - y]
        src = shard_block(k, y, rep) if h == 0 else spot
        return remote(src, spot, z_send.at[0], z_recv.at[k, h, m - 1], z_peer(m))

    def z_relay(k, h):
        spot = weights.at[k, rep, 2 * plane(2) + (y if h == 0 else 1 - y)]
        return remote(spot, spot, z_send.at[0], z_recv.at[k, h, 2], z_peer(1))

    def x_copy(k, h, m):
        spot = weights.at[k, rep, 2 * plane(m) + (y if h == 0 else 1 - y)]
        return remote(spot, spot, x_send.at[0], x_recv.at[x_slot(k, h, m)], x_peer)

    every = (2, 1, 3)
    events = [(k, h, every) for k, h in ((0, 0), (1, 0), (0, 1), (1, 1), (2, 0), (2, 1))]
    events += [(k, h, every) for h in range(2) for k in range(3, last_raise)]
    events += [(k, 0, every) for k in lowers]
    events += [(k, 1, (2, 3)) for k in lowers] + [(k, 1, (1,)) for k in lowers]

    def start_after(index):
        for role, ahead in ((is_mid, AHEAD), (is_end, END_AHEAD)):

            def reach_of(place, ahead=ahead):
                return place + ahead[min(place, len(ahead) - 1)] if place >= 0 else 0

            @pl.when(role)
            def _():
                for later in range(reach_of(index - 1) + 1, reach_of(index) + 1):
                    start(later)

    def start(index):
        if index >= len(events):
            return
        k, h, sources = events[index]
        if h == 1 and 2 in sources:
            y_copy(k, 0).wait_recv()
        for m in sources:
            if m == 1 and sources == every and index >= 1:

                @pl.when(is_end)
                def _():
                    z_copy(k, h, 1).start()

            elif m < 3:
                z_copy(k, h, m).start()
            else:

                @pl.when(is_mid)
                def _():
                    z_copy(k, h, 3).start()

    def relay(index, m):
        k, h, _ = events[index]
        z_copy(k, h, m).wait_recv()
        x_copy(k, h, m).start()

        @pl.when(jnp.logical_and(is_mid, m == 2))
        def _():
            z_relay(k, h).start()
            lead = index + (1 if index < 2 else LEAD)
            for place in (lead,) if index != 2 else (lead - 1, lead):
                next_k, next_h, next_sources = events[min(place, len(events) - 1)]
                if next_sources == every:
                    z_copy(next_k, next_h, 1).start()

    def advance(index):
        for place, m in enumerate(sorted(events[index][2])):
            relay(index, m)
            if place == 0:
                start_after(index)

    def advance_for(role, index):
        @pl.when(role)
        def _():
            advance(index)

    def advance_at(step, role, index):
        @pl.when(jnp.logical_and(role, step < 3))
        def _():
            relay(index, step + 1)

        @pl.when(jnp.logical_and(role, step == 0))
        def _():
            start_after(index)

    def wait_y(first, last):
        count_wait(weights.at[first:last, 0, 0], y_recv.at[y_slot(first, 1)])

    def wait_x(first, last, h, sources):
        parts = 1 if h is not None else 2
        sample = weights.at[first:last, 0:parts, 0 : len(sources)]
        count_wait(sample, x_recv.at[x_slot(first, h, sources[0])])

    def tp_copy(src, dst, slot):
        return remote(src, dst, act_send.at[slot], act_recv.at[slot], t_peer)

    def y_act(src, dst, slot):
        return remote(src, dst, act_send.at[slot], act_recv.at[slot], y_peer)

    def y_start(places, parts=(0, 1)):
        for q in parts:
            for k in places:
                y_copy(k, q).start()

    y_start((0,), (0,))
    start(0)
    y_start((1,), (0,))
    y_start((0, 1), (1,))
    for k in range(chunks):
        for q in range(2):
            local_copy(k, q).start()

    own_columns = pl.ds(pl.multiple_of(tp * half_width, half_width), half_width)

    def squares(source, phase):
        def body(step, _):
            rows = pl.ds(pl.multiple_of(step * CHUNK_ROWS, CHUNK_ROWS), CHUNK_ROWS)
            total = None
            for tile in range(lane_tiles):
                value = source[rows, tile * LANES : (tile + 1) * LANES].astype(jnp.float32)
                total = value * value if total is None else total + value * value
            square_own[phase, rows, :] = total
            return 0

        lax.fori_loop(0, tokens // CHUNK_ROWS, body, 0)

    def square_copy(phase):
        return tp_copy(square_own.at[phase], square_got.at[phase], 9 + phase)

    def norm(source, phase, gain_ref, target):
        def body(step, _):
            rows = pl.ds(pl.multiple_of(step * CHUNK_ROWS, CHUNK_ROWS), CHUNK_ROWS)
            total = jnp.sum(square_own[phase, rows, :] + square_got[phase, rows, :], axis=1, keepdims=True)
            inverse = lax.rsqrt(total * (1.0 / width) + EPSILON)
            for tile in range(lane_tiles):
                value = source[rows, tile * LANES : (tile + 1) * LANES].astype(jnp.float32)
                gain = gain_ref[pl.ds(tp * lane_tiles + tile, 1), :]
                lanes = pl.ds(pl.multiple_of(tp * half_width + tile * LANES, LANES), LANES)
                target[y, rows, lanes] = (value * inverse * gain).astype(jnp.bfloat16)
            return 0

        lax.fori_loop(0, tokens // CHUNK_ROWS, body, 0)

    def block_copies(target, base):
        own = target.at[y, :, own_columns]
        theirs = target.at[1 - y, :, own_columns]
        return (
            tp_copy(own, own, base),
            y_act(own, own, base + 1),
            tp_copy(theirs, theirs, base + 2),
        )

    loads[0].wait()
    squares(stream_ref, 0)
    square_copy(0).start()
    loads[1].wait()
    mine = pl.ds(pl.multiple_of(y * quarter, quarter), quarter)
    peers = pl.ds(pl.multiple_of((1 - y) * quarter, quarter), quarter)
    offset_send[...] = offset_ref[:, peers].astype(jnp.bfloat16)
    offsets[0] = offset_ref[:, mine].astype(jnp.bfloat16)
    square_copy(0).wait_recv()
    norm(stream_ref, 0, first_gain_ref, normed)
    first_tp, first_y, first_pass = block_copies(normed, 0)
    first_tp.start()
    offset_copy = y_act(offset_send, offsets.at[1], 3)

    y_start((2,))
    wide = jnp.exp(-jnp.abs(param_ref[...]))
    ratio = wide / (2.0 + wide)
    ratio_square = ratio * ratio
    log_sum = jnp.ones_like(ratio) * (1.0 / 17.0)
    for odd in (15.0, 13.0, 11.0, 9.0, 7.0, 5.0, 3.0, 1.0):
        log_sum = log_sum * ratio_square + 1.0 / odd
    rate_ref[...] = -DECAY_MULTIPLIER * (jnp.maximum(-param_ref[...], 0.0) + 2.0 * ratio * log_sum)

    size = decay_maps_ref.shape[1]
    per = LANES // size
    tiles = quarter // LANES
    maps[...] = jnp.zeros_like(maps)
    for tile in range(tiles):
        for index in range(per):
            place = y * (tiles * per) + tile * per + index
            span = slice(index * size, (index + 1) * size)
            maps[tile, span, index * size : (index + 1) * size] = decay_maps_ref[place]
            maps[tile, span, LANES + index * size : LANES + (index + 1) * size] = input_maps_ref[place]

    @pl.when(is_mid)
    def _():
        advance(0)
        first_y.start()
        advance(1)
        offset_copy.start()
        advance(2)
        y_start(range(3, last_raise))
        advance(3)

    @pl.when(is_end)
    def _():
        for place, (index, m) in enumerate(END_ORDER):
            relay(index, m)
            if m == 1:
                start_after(index)
            if place == 1:
                first_y.start()
            if place == 4:
                offset_copy.start()
            if place == 7:
                y_start(range(3, last_raise))

    first_y.wait_recv()
    first_pass.start()

    count_wait(weights.at[:, :, 0], local_sem.at[0])
    wait_y(0, 2)
    advance_for(is_mid, 4)
    wait_x(0, 2, None, every)
    first_tp.wait_recv()

    def project(which, token_block, *relays):
        def body(step, _):
            for role, index in relays:
                advance_at(step, role, index)
            matrix = weights[step // 2, step % 2].reshape(width, block)
            projected[which, step] = jnp.dot(
                normed[token_block], matrix, preferred_element_type=jnp.float32
            ).astype(jnp.bfloat16)
            return 0

        lax.fori_loop(0, 4, body, 0)

    reach = taps_ref.shape[0]

    def recur(which, *relays):
        def body(step, _):
            for role, index in relays:
                advance_at(step, role, index)
            rows = pl.ds(pl.multiple_of(step * SEQ_LEN, SEQ_LEN), SEQ_LEN)
            for tile in range(tiles):
                part, lane = tile * LANES // block, tile * LANES % block
                lanes = slice(lane, lane + LANES)
                taps = taps_ref[
                    :, pl.ds(pl.multiple_of(y * quarter + tile * LANES, LANES), LANES)
                ].astype(jnp.float32)
                values = projected[which, part, rows, lanes].astype(jnp.float32)
                filtered = taps[reach - 1 : reach] * values
                for back in range(1, reach):
                    tap = taps[reach - 1 - back : reach - back]
                    filtered = filtered + tap * shift_down(values, back, 0.0)
                conved = filtered.astype(jnp.bfloat16)
                logits = jnp.dot(conved, maps[tile], preferred_element_type=jnp.float32)
                offset = offsets[which, rows, tile * LANES : (tile + 1) * LANES].astype(jnp.float32)
                steps = 1.0 / (1.0 + jnp.exp(-logits))
                rate = rate_ref[pl.ds(y * tiles + tile, 1), :]
                log_decay = steps[:, :LANES] * rate + offset
                decay = jnp.exp(log_decay)
                twice = -2.0 * log_decay
                series = 1.0 + twice * (
                    -1 / 2
                    + twice
                    * (1 / 6 + twice * (-1 / 24 + twice * (1 / 120 + twice * (-1 / 720 + twice * (1 / 5040)))))
                )
                lost = jnp.where(twice < 0.35, twice * series, 1.0 - decay * decay)
                state = jnp.sqrt(lost) * steps[:, LANES:] * conved.astype(jnp.float32)
                span = 1
                while span < SEQ_LEN:
                    state = state + decay * shift_down(state, span, 0.0)
                    if span * 2 < SEQ_LEN:
                        decay = decay * shift_down(decay, span, 1.0)
                    span *= 2
                gate = projected[which, 2 + part, rows, lanes].astype(jnp.float32)
                gelu = 0.5 * gate * (1.0 + lax.erf(gate * 0.7071067811865476))
                mixed[which, rows, tile * LANES : (tile + 1) * LANES] = (state * gelu).astype(jnp.bfloat16)
            return 0

        lax.fori_loop(0, tokens // SEQ_LEN, body, 0)

    project(0, y, (is_end, 4))
    recur(0)
    first_pass.wait_recv()
    project(1, 1 - y, (is_mid, 5))
    offset_copy.wait_recv()
    recur(1, (is_end, 5))

    advance_for(is_mid, 6)
    wait_y(2, 3)
    wait_x(2, 3, None, every)

    def mix_out(which, *relays):
        def body(step, _):
            for role, index in relays:
                advance_at(step, role, index)

            def term(place):
                matrix = weights[2, :, place].reshape(quarter, block)
                return jnp.dot(mixed[which], matrix, preferred_element_type=jnp.float32).astype(jnp.bfloat16)

            lanes = pl.ds(pl.multiple_of(step * block, block), block)
            per_half = n_fs // 2
            passed[which, :, lanes] = term(per_half * (1 - tp) + step)
            kept[which, :, lanes] = term(per_half * tp + step)
            return 0

        lax.fori_loop(0, n_fs // 2, body, 0)

    def mix_copy(which):
        return tp_copy(passed.at[which], got.at[which], 4 + which)

    mix_out(1, (is_end, 6))
    mix_copy(1).start()
    mix_out(0)
    mix_copy(0).start()

    def add_peer(step, _):
        rows = pl.ds(pl.multiple_of(step * CHUNK_ROWS, CHUNK_ROWS), CHUNK_ROWS)
        mid_send[rows, :] = (
            kept[1, rows, :].astype(jnp.float32) + got[1, rows, :].astype(jnp.float32)
        ).astype(jnp.bfloat16)
        return 0

    mix_copy(1).wait_recv()
    lax.fori_loop(0, tokens // CHUNK_ROWS, add_peer, 0)
    mid_copy = y_act(mid_send, mid_got, 6)
    mid_copy.start()
    y_start(lowers, (0,))

    up = 6
    for index in range(1, raises):
        advance(up + index)
    mix_copy(0).wait_recv()
    advance(up + raises)
    advance_for(is_mid, up + raises + 1)

    mid_copy.wait_recv()

    def add_own(step, _):
        rows = pl.ds(pl.multiple_of(step * CHUNK_ROWS, CHUNK_ROWS), CHUNK_ROWS)
        total = None
        for tile in range(lane_tiles):
            lanes = slice(tile * LANES, (tile + 1) * LANES)
            update = kept[0, rows, lanes].astype(jnp.float32) + got[0, rows, lanes].astype(jnp.float32)
            update = update + mid_got[rows, lanes].astype(jnp.float32)
            value = (stream_ref[rows, lanes].astype(jnp.float32) + update).astype(jnp.bfloat16)
            middle[rows, lanes] = value
            value = value.astype(jnp.float32)
            total = value * value if total is None else total + value * value
        square_own[1, rows, :] = total
        return 0

    lax.fori_loop(0, tokens // CHUNK_ROWS, add_own, 0)
    square_copy(1).start()
    square_copy(1).wait_recv()
    norm(middle, 1, second_gain_ref, normed_mid)
    second_tp, second_y, second_pass = block_copies(normed_mid, 11)
    second_y.start()
    second_tp.start()
    advance_for(is_end, up + raises + 1)
    for index in range(2, raises):
        advance(up + raises + index)
    down = up + 2 * raises
    wait_y(3, last_raise)
    for k in range(3, last_raise):
        if k == last_raise - 1:
            advance(down)
        wait_x(k, k + 1, None, every)

    def lift(which, token_block, *relays):
        def body(step, _):
            for role, index in relays:
                advance_at(step, role, index)
            matrix = weights[3 + step // 2, step % 2].reshape(width, block)
            total = jnp.dot(normed_mid[token_block], matrix, preferred_element_type=jnp.float32)
            lanes = pl.ds(pl.multiple_of(step * block, block), block)
            activity[which, :, lanes] = jnp.square(jnp.maximum(total, 0.0)).astype(jnp.bfloat16)
            return 0

        lax.fori_loop(0, 2 * raises, body, 0)

    second_tp.wait_recv()
    lift(0, y)
    advance_for(is_mid, down + 1)
    second_y.wait_recv()
    y_start(lowers, (1,))
    second_pass.start()
    second_pass.wait_recv()
    lift(1, 1 - y, (is_end, down + 1), (is_mid, down + 2))
    advance_for(is_end, down + 2)
    for index in range(3, raises):
        advance(down + index)

    depth = raises * quarter

    def lower(h, m):
        place = 2 * plane(m) + (y if h == 0 else 1 - y)

        def body(which, _):
            matrix = weights[last_raise:chunks, :, place].reshape(depth, block)
            partial[m, h, which] = jnp.dot(
                activity[which], matrix, preferred_element_type=jnp.float32
            ).astype(jnp.bfloat16)
            return 0

        lax.fori_loop(0, 2, body, 0)

    def is_owner(m):
        return low if m < 2 else jnp.logical_not(low)

    def owner_copy(h, m):
        slot = 14 + 2 * (m % 2) + h
        return tp_copy(partial.at[m, h], partial_got.at[m % 2, h], slot)

    def last_copy(h, m):
        slot = 18 + 2 * (m % 2)
        return remote(
            last_send.at[m % 2, h],
            last_got.at[m % 2, 1 - h],
            act_send.at[slot + h],
            act_recv.at[slot + 1 - h],
            y_peer,
        )

    def pass_on(h, m):
        @pl.when(jnp.logical_not(is_owner(m)))
        def _():
            owner_copy(h, m).start()

    def finish(h, m):
        @pl.when(is_owner(m))
        def _():
            owner_copy(h, m).wait_recv()

            def body(step, _):
                rows = pl.ds(pl.multiple_of(step * CHUNK_ROWS, CHUNK_ROWS), CHUNK_ROWS)
                last_send[m % 2, h, rows, :] = (
                    partial[m, h, 1, rows, :].astype(jnp.float32)
                    + partial_got[m % 2, h, 1, rows, :].astype(jnp.float32)
                ).astype(jnp.bfloat16)
                return 0

            lax.fori_loop(0, tokens // CHUNK_ROWS, body, 0)
            last_copy(h, m).start()

    def close(h, mm):
        owned = mm + 2 * (1 - low.astype(jnp.int32))
        last_copy(1 - h, mm).wait_recv()
        place = 2 * ((z % 2 + mm) % 2) + (y if h == 0 else 1 - y)
        lanes = pl.ds(pl.multiple_of(place * block, block), block)

        def body(step, _):
            rows = pl.ds(pl.multiple_of(step * CHUNK_ROWS, CHUNK_ROWS), CHUNK_ROWS)
            update = (
                partial[owned, h, 0, rows, :].astype(jnp.float32)
                + partial_got[mm, h, 0, rows, :].astype(jnp.float32)
                + last_got[mm, h, rows, :].astype(jnp.float32)
            )
            out_ref[rows, lanes] = (middle[rows, lanes].astype(jnp.float32) + update).astype(jnp.bfloat16)
            return 0

        lax.fori_loop(0, tokens // CHUNK_ROWS, body, 0)

    order = [(0, m) for m in range(4)] + [(1, m) for m in (0, 2, 3, 1)]
    far, near = down + raises, down + 2 * raises
    advance(far)
    wait_y(last_raise, chunks)
    wait_x(last_raise, chunks, 0, every)
    for index, (h, m) in enumerate(order):
        if index in (2, 4):
            advance(far + index // 2)
        if index >= 5:
            advance(near + index - 5)
        if h == 1 and m:
            wait_x(last_raise, chunks, 1, (m,))
        lower(h, m)
        pass_on(h, m)
        if index and index < 5:
            finish(*order[index - 1])
        if index >= 4:
            finish(h, m)
    for h in range(2):
        for mm in range(2):
            close(h, mm)

    count_wait(weights.at[:, :, 0], y_send.at[0])
    count_wait(weights.at[:, 0, 0:6], x_send.at[0])
    count_wait(weights.at[:, 0, 0:4], z_send.at[0])

    @pl.when(is_mid)
    def _():
        count_wait(weights.at[:, 0, 0:4], z_send.at[0])

    for copy in (first_tp, first_y, first_pass, second_tp, second_y, second_pass, offset_copy, mid_copy):
        copy.wait_send()
    for phase in range(2):
        square_copy(phase).wait_send()
        mix_copy(phase).wait_send()
    for h, m in order:

        @pl.when(is_owner(m))
        def _():
            last_copy(h, m).wait_send()

        @pl.when(jnp.logical_not(is_owner(m)))
        def _():
            owner_copy(h, m).wait_send()


def whole_layer(
    stream,
    recurrent_norm_gain,
    feedforward_norm_gain,
    recurrent_input_weight,
    output_gate_weight,
    causal_filter_weight,
    decay_gate_matrix,
    input_gate_matrix,
    channel_decay_param,
    token_decay_offset,
    recurrent_output_weight,
    up_projection_weight,
    down_projection_weight,
):
    tokens, half_width = stream.shape
    width = 2 * half_width
    quarter = half_width // 2
    block, n_fs = quarter // 2, 8
    raises = up_projection_weight.shape[1] // half_width
    chunks = 3 + 2 * raises
    depth = raises * quarter
    tiles = quarter // LANES
    half_type, full_type = jnp.bfloat16, jnp.float32
    vmem = pl.BlockSpec(memory_space=pltpu.VMEM)
    anywhere = pl.BlockSpec(memory_space=pl.ANY)
    dma = pltpu.SemaphoreType.DMA
    return pl.pallas_call(
        whole_kernel,
        out_shape=jax.ShapeDtypeStruct((tokens, half_width), half_type),
        in_specs=[anywhere] * 2 + [vmem] * 6 + [anywhere] * 5,
        out_specs=vmem,
        scratch_shapes=[
            pltpu.VMEM((tokens, half_width), half_type),
            pltpu.VMEM((tokens, half_width), full_type),
            pltpu.VMEM((half_width // LANES, LANES), full_type),
            pltpu.VMEM((chunks, 2, n_fs, block, block), half_type),
            pltpu.VMEM((2, tokens, width), half_type),
            pltpu.VMEM((2, tokens, width), half_type),
            pltpu.VMEM((2, tokens, LANES), full_type),
            pltpu.VMEM((2, tokens, LANES), full_type),
            pltpu.VMEM((2, 4, tokens, block), half_type),
            pltpu.VMEM((2, tokens, quarter), half_type),
            pltpu.VMEM((2, tokens, quarter), half_type),
            pltpu.VMEM((tokens, quarter), half_type),
            pltpu.VMEM((tiles, LANES, 2 * LANES), half_type),
            pltpu.VMEM((2, tokens, half_width), half_type),
            pltpu.VMEM((2, tokens, half_width), half_type),
            pltpu.VMEM((2, tokens, half_width), half_type),
            pltpu.VMEM((tokens, half_width), half_type),
            pltpu.VMEM((tokens, half_width), half_type),
            pltpu.VMEM((tokens, half_width), half_type),
            pltpu.VMEM((2, tokens, depth), half_type),
            pltpu.VMEM((4, 2, 2, tokens, block), half_type),
            pltpu.VMEM((2, 2, 2, tokens, block), half_type),
            pltpu.VMEM((2, 2, tokens, block), half_type),
            pltpu.VMEM((2, 2, tokens, block), half_type),
            dma((1,)),
            dma((1,)),
            dma((chunks + 4,)),
            dma((1,)),
            dma((chunks, 2, 3)),
            dma((1,)),
            dma((raises + 6,)),
            dma((22,)),
            dma((22,)),
            dma((2,)),
        ],
        compiler_params=pltpu.CompilerParams(
            collective_id=0, has_side_effects=True, vmem_limit_bytes=67043328
        ),
        name="whole_layer",
    )(
        stream,
        token_decay_offset,
        recurrent_norm_gain.reshape(-1, LANES),
        feedforward_norm_gain.reshape(-1, LANES),
        causal_filter_weight,
        decay_gate_matrix,
        input_gate_matrix,
        channel_decay_param.reshape(-1, LANES),
        recurrent_input_weight,
        output_gate_weight,
        recurrent_output_weight,
        up_projection_weight,
        down_projection_weight,
    )


def fits_whole(sizes, stream, up_projection_weight, decay_gate_matrix):
    tokens, half_width = stream.shape
    return (
        sizes == (2, 8, 2)
        and half_width % (8 * LANES) == 0
        and tokens % (4 * SEQ_LEN) == 0
        and up_projection_weight.shape[1] % half_width == 0
        and up_projection_weight.shape[1] // half_width >= 3
        and LANES % decay_gate_matrix.shape[1] == 0
    )


def solution(mesh):
    in_specs = (
        P(("rep", "fs"), "tp"),
        P(),
        P(),
        P("fs", "tp"),
        P("fs", "tp"),
        P(None, "tp"),
        P("tp", None, None),
        P("tp", None, None),
        P("tp"),
        P(("rep", "fs"), "tp"),
        P("tp", "fs"),
        P("fs", "tp"),
        P("tp", "fs"),
    )
    out_specs = P(("rep", "fs"), "tp")
    sizes = tuple(mesh.shape[axis] for axis in ("rep", "fs", "tp"))

    def body(*args):
        if fits_whole(sizes, args[0], args[11], args[6]):
            return whole_layer(*args)
        return shards(sizes, *args)

    return jax.shard_map(
        body, mesh=mesh, in_specs=in_specs, out_specs=out_specs, check_vma=False
    )
```

```python
import functools

import jax
import jax.numpy as jnp
from jax import lax
from jax.experimental import pallas as pl
from jax.experimental.pallas import tpu as pltpu
from jax.sharding import PartitionSpec as P


SEQ_LEN = 128
EPSILON = 1e-06
DECAY_MULTIPLIER = 8.0
LANES = 128


def half(values, which, axis):
    first, second = jnp.split(values, 2, axis)
    return jnp.where(which == 0, first, second)


def gather_shard(shard, ids, sizes):
    rep, fs, _ = ids
    _, n_fs, _ = sizes
    own, for_peer = shard
    hops = n_fs // 2
    place, side = fs // 2, fs % 2
    from_peer = lax.ppermute(for_peer, "fs", [(i, i ^ 1) for i in range(n_fs)])
    start = jnp.where(side == rep, own, from_peer)
    up = [(i, (i + 2) % n_fs) for i in range(n_fs)]
    down = [(i, (i + n_fs - 2) % n_fs) for i in range(n_fs)]
    pieces, places = [own, from_peer], [fs, fs ^ 1]
    below = above = start
    for step in range(1, hops):
        if step % 2:
            below = mine = lax.ppermute(below, "fs", up)
            base = 2 * ((place + hops - (step + 1) // 2) % hops)
        else:
            above = mine = lax.ppermute(above, "fs", down)
            base = 2 * ((place + step // 2) % hops)
        pieces += [mine, lax.ppermute(mine, "rep", [(0, 1), (1, 0)])]
        places += [base + rep, base + 1 - rep]
    return pieces, jnp.stack(places).astype(jnp.int32)


def gather_features(values, tp, n_tp):
    if n_tp != 2:
        return lax.all_gather(values, "tp", axis=1, tiled=True)
    other = lax.ppermute(values, "tp", [(0, 1), (1, 0)])
    return jnp.where(
        tp == 0, jnp.concatenate([values, other], 1), jnp.concatenate([other, values], 1)
    )


def sum_features(parts, tp, n_tp):
    total = lax.dynamic_index_in_dim(parts, tp, 0, False).astype(jnp.float32)
    for shift in range(1, n_tp):
        piece = lax.dynamic_index_in_dim(parts, (tp + shift) % n_tp, 0, False)
        got = lax.ppermute(piece, "tp", [(i, (i + shift) % n_tp) for i in range(n_tp)])
        total = total + got.astype(jnp.float32)
    return total.astype(jnp.bfloat16)


def norm_rows(values, gain):
    widened = values.astype(jnp.float32)
    inverse = lax.rsqrt(jnp.mean(widened * widened, axis=-1, keepdims=True) + EPSILON)
    return (widened * inverse * gain).astype(jnp.bfloat16)


ROWS = 256
CHUNK = 512


def depth_kernel(squared, places_ref, x_ref, *refs):
    *pieces, out_ref = refs
    depth, width = pieces[0].shape
    chunk = min(CHUNK, width)
    for lower in range(0, width, chunk):
        cols = slice(lower, lower + chunk)
        total = None
        for index, piece in enumerate(pieces):
            place = pl.multiple_of(places_ref[index] * depth, depth)
            term = jnp.dot(
                x_ref[:, pl.ds(place, depth)], piece[:, cols], preferred_element_type=jnp.float32
            )
            total = term if total is None else total + term
        if squared:
            total = jnp.square(jnp.maximum(total, 0.0))
        out_ref[:, cols] = total.astype(jnp.bfloat16)


def depth_matmul(x, gathered, squared=False):
    pieces, places = gathered
    tokens, width = x.shape
    shape = pieces[0].shape
    return pl.pallas_call(
        functools.partial(depth_kernel, squared),
        grid_spec=pltpu.PrefetchScalarGridSpec(
            num_scalar_prefetch=1,
            grid=(tokens // ROWS,),
            in_specs=[pl.BlockSpec((ROWS, width), lambda m, _: (m, 0))]
            + [pl.BlockSpec(shape, lambda m, _: (0, 0))] * len(pieces),
            out_specs=pl.BlockSpec((ROWS, shape[1]), lambda m, _: (m, 0)),
        ),
        out_shape=jax.ShapeDtypeStruct((tokens, shape[1]), jnp.bfloat16),
        cost_estimate=pl.CostEstimate(
            flops=2 * tokens * width * shape[1],
            bytes_accessed=2 * (tokens * width + (tokens + width) * shape[1]),
            transcendentals=0,
        ),
        name="depth_matmul",
    )(places, x, *pieces)


def columns_kernel(per, places_ref, x_ref, *refs):
    *pieces, out_ref = refs
    cols = pieces[0].shape[1]
    for index, piece in enumerate(pieces):
        place = places_ref[index]
        lower = pl.multiple_of((place % per) * cols, cols)
        out_ref[place // per, :, pl.ds(lower, cols)] = jnp.dot(
            x_ref[...], piece[...], preferred_element_type=jnp.float32
        ).astype(jnp.bfloat16)


def columns_matmul(x, gathered, n_tp, first, tokens):
    pieces, places = gathered
    depth, cols = pieces[0].shape
    per = len(pieces) // n_tp
    skip = first // ROWS
    return pl.pallas_call(
        functools.partial(columns_kernel, per),
        grid_spec=pltpu.PrefetchScalarGridSpec(
            num_scalar_prefetch=1,
            grid=(tokens // ROWS,),
            in_specs=[pl.BlockSpec((ROWS, depth), lambda m, _: (m + skip, 0))]
            + [pl.BlockSpec((depth, cols), lambda m, _: (0, 0))] * len(pieces),
            out_specs=pl.BlockSpec((n_tp, ROWS, per * cols), lambda m, _: (0, m, 0)),
        ),
        out_shape=jax.ShapeDtypeStruct((n_tp, tokens, per * cols), jnp.bfloat16),
        cost_estimate=pl.CostEstimate(
            flops=2 * tokens * depth * cols * len(pieces),
            bytes_accessed=2 * (tokens * depth + len(pieces) * cols * (depth + tokens)),
            transcendentals=0,
        ),
        name="columns_matmul",
    )(places, x, *pieces)


def shift_down(values, amount, fill):
    index = lax.broadcasted_iota(jnp.int32, values.shape, 0)
    return jnp.where(index < amount, fill, pltpu.roll(values, amount, 0))


def recurrence_kernel(
    side_ref, value_ref, gate_ref, own_ref, peer_ref, taps_ref, maps_ref, rate_ref, out_ref
):
    rows, channels = value_ref.shape
    reach = taps_ref.shape[0]
    per = LANES // maps_ref.shape[1]
    is_own = pl.program_id(0) < pl.num_programs(0) // 2
    for tile in range(channels // LANES):
        cols = slice(tile * LANES, (tile + 1) * LANES)
        values = value_ref[:, cols].astype(jnp.float32)
        filtered = taps_ref[reach - 1 : reach, cols] * values
        for back in range(1, reach):
            tap = taps_ref[reach - 1 - back : reach - back, cols]
            filtered = filtered + tap * shift_down(values, back, 0.0)
        conved = filtered.astype(jnp.bfloat16)
        maps = maps_ref[tile * per : (tile + 1) * per].reshape(LANES, 2 * LANES)
        logits = jnp.dot(conved, maps, preferred_element_type=jnp.float32)
        offset = jnp.where(is_own, own_ref[:, cols], peer_ref[:, cols].astype(jnp.float32))
        steps = 1.0 / (1.0 + jnp.exp(-logits))
        log_decay = steps[:, :LANES] * rate_ref[:, cols] + offset
        decay = jnp.exp(log_decay)
        y = -2.0 * log_decay
        series = 1.0 + y * (
            -1 / 2 + y * (1 / 6 + y * (-1 / 24 + y * (1 / 120 + y * (-1 / 720 + y * (1 / 5040)))))
        )
        lost = jnp.where(y < 0.35, y * series, 1.0 - decay * decay)
        state = jnp.sqrt(lost) * steps[:, LANES:] * conved.astype(jnp.float32)
        span = 1
        while span < rows:
            state = state + decay * shift_down(state, span, 0.0)
            if span * 2 < rows:
                decay = decay * shift_down(decay, span, 1.0)
            span *= 2
        gate = gate_ref[:, cols].astype(jnp.float32)
        gelu = 0.5 * gate * (1.0 + lax.erf(gate * 0.7071067811865476))
        out_ref[:, cols] = (state * gelu).astype(jnp.bfloat16)


def recurrence(projected, offset_own, offset_peer, taps, decay_maps, input_maps, rate, side):
    tokens = projected.shape[0]
    channels = offset_peer.shape[1]
    blocks, size, _ = decay_maps.shape
    per = LANES // size
    block = jnp.arange(blocks)[:, None, None] % per
    group = jnp.arange(LANES)[None, None, :] // size

    def diagonal(maps):
        return jnp.where(block == group, jnp.tile(maps, (1, 1, per)), 0)

    maps = jnp.concatenate([diagonal(decay_maps), diagonal(input_maps)], 2)
    sequences = tokens // SEQ_LEN
    own = sequences // 2
    return pl.pallas_call(
        recurrence_kernel,
        grid_spec=pltpu.PrefetchScalarGridSpec(
            num_scalar_prefetch=1,
            grid=(sequences,),
            in_specs=[
                pl.BlockSpec((SEQ_LEN, channels), lambda s, side: (s, 0)),
                pl.BlockSpec((SEQ_LEN, channels), lambda s, side: (s, 1)),
                pl.BlockSpec(
                    (SEQ_LEN, channels), lambda s, side: (jnp.minimum(s, own - 1), side[0])
                ),
                pl.BlockSpec((SEQ_LEN, channels), lambda s, side: (jnp.maximum(s - own, 0), 0)),
                pl.BlockSpec((taps.shape[0], channels), lambda s, side: (0, side[0])),
                pl.BlockSpec((blocks // 2, size, 2 * LANES), lambda s, side: (side[0], 0, 0)),
                pl.BlockSpec((1, channels), lambda s, side: (0, side[0])),
            ],
            out_specs=pl.BlockSpec((SEQ_LEN, channels), lambda s, side: (s, 0)),
        ),
        out_shape=jax.ShapeDtypeStruct((tokens, channels), jnp.bfloat16),
        cost_estimate=pl.CostEstimate(
            flops=tokens * channels * 700,
            bytes_accessed=tokens * channels * 10,
            transcendentals=tokens * channels * 6,
        ),
        name="recurrence",
    )(
        side.astype(jnp.int32)[None],
        projected,
        projected,
        offset_own,
        offset_peer,
        taps.astype(jnp.float32),
        maps,
        rate[None, :],
    )


def shards(
    sizes,
    stream,
    recurrent_norm_gain,
    feedforward_norm_gain,
    recurrent_input_weight,
    output_gate_weight,
    causal_filter_weight,
    decay_gate_matrix,
    input_gate_matrix,
    channel_decay_param,
    token_decay_offset,
    recurrent_output_weight,
    up_projection_weight,
    down_projection_weight,
):
    _, n_fs, n_tp = sizes
    ids = lax.axis_index("rep"), lax.axis_index("fs"), lax.axis_index("tp")
    _, fs, tp = ids
    side = fs % 2
    pairs = [(i, i ^ 1) for i in range(n_fs)]
    tokens = stream.shape[0]

    def halves(weight, axis):
        return half(weight, side, axis), half(weight, 1 - side, axis)

    def to_peer(values):
        return lax.ppermute(values, "fs", pairs)

    value_own, value_peer = halves(recurrent_input_weight, 1)
    gate_own, gate_peer = halves(output_gate_weight, 1)
    entry = (
        jnp.concatenate([value_own, gate_own], 1),
        jnp.concatenate([value_peer, gate_peer], 1),
    )
    entry_full = gather_shard(entry, ids, sizes)
    stream_peer = to_peer(stream)
    offset_peer = to_peer(half(token_decay_offset, 1 - side, 1).astype(jnp.bfloat16))
    output_full = gather_shard(halves(recurrent_output_weight, 0), ids, sizes)
    expand_full = gather_shard(halves(up_projection_weight, 1), ids, sizes)
    contract_full = gather_shard(halves(down_projection_weight, 0), ids, sizes)

    own_pair = jnp.concatenate([stream, stream_peer], 0)
    whole = gather_features(own_pair, tp, n_tp)
    normed = norm_rows(whole, recurrent_norm_gain)
    projected = depth_matmul(normed, entry_full)
    mixed = recurrence(
        projected,
        token_decay_offset,
        offset_peer,
        causal_filter_weight,
        decay_gate_matrix,
        input_gate_matrix,
        -DECAY_MULTIPLIER * jax.nn.softplus(-channel_decay_param),
        side,
    )
    mixer_terms = columns_matmul(mixed, output_full, n_tp, 0, 2 * tokens)
    mixer_chip = sum_features(mixer_terms, tp, n_tp)
    got_own = to_peer(mixer_chip[tokens:])
    got_peer = to_peer(mixer_chip[:tokens])
    update = mixer_chip.astype(jnp.float32) + jnp.concatenate([got_own, got_peer], 0).astype(
        jnp.float32
    )
    middle = (own_pair.astype(jnp.float32) + update).astype(jnp.bfloat16)
    normed_mid = norm_rows(gather_features(middle, tp, n_tp), feedforward_norm_gain)
    activity = depth_matmul(normed_mid, expand_full, squared=True)
    peer_terms = columns_matmul(activity, contract_full, n_tp, tokens, tokens)
    got = to_peer(sum_features(peer_terms, tp, n_tp))
    own_terms = columns_matmul(activity, contract_full, n_tp, 0, tokens)
    own_chip = sum_features(own_terms, tp, n_tp)
    channel_sum = own_chip.astype(jnp.float32) + got.astype(jnp.float32)
    return (middle[:tokens].astype(jnp.float32) + channel_sum).astype(jnp.bfloat16)


MESH = pl.DeviceIdType.MESH
CHUNK_ROWS = 128
AHEAD = (1, 1, 1, 1, 2, 3)
END_AHEAD = (1, 1, 1, 1, 2, 3)
STEADY = 4
LEAD = 2
END_ORDER = (
    (0, 1), (0, 2), (0, 3), (1, 2), (1, 1), (1, 3), (2, 2), (2, 1), (2, 3), (3, 2), (3, 1), (3, 3),
)


def whole_kernel(
    stream_hbm,
    offset_hbm,
    first_gain_ref,
    second_gain_ref,
    taps_ref,
    decay_maps_ref,
    input_maps_ref,
    param_ref,
    value_hbm,
    gate_hbm,
    output_hbm,
    raise_hbm,
    lower_hbm,
    out_ref,
    stream_ref,
    offset_ref,
    rate_ref,
    weights,
    normed,
    normed_mid,
    square_own,
    square_got,
    projected,
    mixed,
    offsets,
    offset_send,
    maps,
    kept,
    passed,
    got,
    mid_send,
    mid_got,
    middle,
    activity,
    partial,
    partial_got,
    total,
    last_send,
    last_got,
    local_sem,
    y_send,
    y_recv,
    z_send,
    z_recv,
    x_send,
    x_recv,
    act_send,
    act_recv,
    load_sem,
):
    rep, fs, tp = lax.axis_index("rep"), lax.axis_index("fs"), lax.axis_index("tp")
    z, y = fs // 2, fs % 2
    tokens, half_width = stream_ref.shape
    width = 2 * half_width
    chunks, _, n_fs, block, _ = weights.shape
    quarter = half_width // 2
    lane_tiles = half_width // LANES
    raises = (chunks - 3) // 2
    last_raise = 3 + raises
    lowers = range(last_raise, chunks)
    is_mid = jnp.logical_or(z == 1, z == 2)
    is_end = jnp.logical_not(is_mid)
    low = (z // 2) == tp

    def plane(m):
        return 2 * ((z // 2 + m // 2) % 2) + (z % 2 + m % 2) % 2

    x_peer = (1 - rep, fs, tp)
    y_peer = (rep, 2 * z + 1 - y, tp)
    t_peer = (rep, fs, 1 - tp)

    def z_peer(m):
        return (rep, 2 * plane(m) + y, tp)

    loads = (
        pltpu.make_async_copy(stream_hbm, stream_ref, load_sem.at[0]),
        pltpu.make_async_copy(offset_hbm, offset_ref, load_sem.at[1]),
    )
    for load in loads:
        load.start()

    barrier = pltpu.get_barrier_semaphore()
    for peer in (x_peer, y_peer, t_peer, z_peer(1), z_peer(2), z_peer(3)):
        pl.semaphore_signal(barrier, inc=1, device_id=peer, device_id_type=MESH)
    pl.semaphore_wait(barrier, 6)

    def remote(src, dst, send, recv, peer):
        return pltpu.make_async_remote_copy(
            src_ref=src, dst_ref=dst, send_sem=send, recv_sem=recv, device_id=peer, device_id_type=MESH
        )

    def shard_block(k, side, part):
        if k < 2 or 3 <= k < 3 + raises:
            ref = (value_hbm, gate_hbm)[k] if k < 2 else raise_hbm
            first = 0 if k < 2 else (k - 3) * quarter
            span = ref.shape[1] // 2
            start = pl.multiple_of(side * span + first + part * block, block)
            return ref.at[:, pl.ds(start, block)]
        ref = output_hbm if k == 2 else lower_hbm
        first = 0 if k == 2 else (k - 3 - raises) * quarter
        span = ref.shape[0] // 2
        start = pl.multiple_of(side * span + first + part * block, block)
        return ref.at[pl.ds(start, block), :]

    def part_of(q):
        return rep if q == 0 else 1 - rep

    def local_copy(k, q):
        part = part_of(q)
        return pltpu.make_async_copy(
            shard_block(k, y, part), weights.at[k, part, fs], local_sem.at[0]
        )

    def group_of(k):
        return 0 if k < 2 else 1 if k == 2 else 2 if k < last_raise else 3

    def y_slot(k, q):
        return k if q == 0 else chunks + group_of(k)

    def x_slot(k, h, m):
        if k < last_raise:
            return group_of(k) if k < 3 else k - 1
        return 2 + raises + (0 if h == 0 else m - 1 if m > 1 else 3 + k - last_raise)

    def count_wait(ref, sem):
        pltpu.make_async_copy(ref, ref, sem).wait()

    def y_copy(k, q):
        part = part_of(q)
        return remote(
            shard_block(k, 1 - y, part), weights.at[k, part, fs], y_send.at[0], y_recv.at[y_slot(k, q)], y_peer
        )

    def z_copy(k, h, m):
        spot = weights.at[k, rep, fs if h == 0 else 2 * z + 1 - y]
        src = shard_block(k, y, rep) if h == 0 else spot
        return remote(src, spot, z_send.at[0], z_recv.at[k, h, m - 1], z_peer(m))

    def z_relay(k, h):
        spot = weights.at[k, rep, 2 * plane(2) + (y if h == 0 else 1 - y)]
        return remote(spot, spot, z_send.at[0], z_recv.at[k, h, 2], z_peer(1))

    def x_copy(k, h, m):
        spot = weights.at[k, rep, 2 * plane(m) + (y if h == 0 else 1 - y)]
        return remote(spot, spot, x_send.at[0], x_recv.at[x_slot(k, h, m)], x_peer)

    every = (2, 1, 3)
    up = 6
    events = [(k, h, every) for k, h in ((0, 0), (1, 0), (0, 1), (1, 1), (2, 0), (2, 1))]
    events += [(k, h, every) for h in range(2) for k in range(3, last_raise)]
    events += [(k, 0, every) for k in lowers]
    events += [(k, 1, (2, 3)) for k in lowers] + [(k, 1, (1,)) for k in lowers]

    def start_after(index):
        for role, ahead in ((is_mid, AHEAD), (is_end, END_AHEAD)):

            def reach_of(place, ahead=ahead):
                return place + ahead[min(place, len(ahead) - 1)] if place >= 0 else 0

            @pl.when(role)
            def _():
                for later in range(reach_of(index - 1) + 1, reach_of(index) + 1):
                    start(later)

    def start(index):
        if index >= len(events):
            return
        k, h, sources = events[index]
        if h == 1 and 2 in sources:
            y_copy(k, 0).wait_recv()
        for m in sources:
            if m == 1 and index >= 1:

                @pl.when(is_end)
                def _():
                    z_copy(k, h, 1).start()

            elif m < 3:
                z_copy(k, h, m).start()
            else:

                @pl.when(is_mid)
                def _():
                    z_copy(k, h, 3).start()

    def relay(index, m):
        k, h, _ = events[index]
        z_copy(k, h, m).wait_recv()
        x_copy(k, h, m).start()

        @pl.when(jnp.logical_and(is_mid, m == 2))
        def _():
            z_relay(k, h).start()
            lead = index + (1 if index < STEADY else LEAD)
            for place in (lead,) if index != STEADY else (lead - 1, lead):
                next_k, next_h, next_sources = events[min(place, len(events) - 1)]
                if next_sources == every:
                    z_copy(next_k, next_h, 1).start()
            far_step = index - up - 3 * raises
            if far_step == raises - 2:
                z_copy(last_raise, 1, 1).start()
            if far_step == raises - 1:
                for later_k in range(last_raise + 1, chunks):
                    z_copy(later_k, 1, 1).start()

    def advance(index):
        for place, m in enumerate(sorted(events[index][2])):
            relay(index, m)
            if place == 0:
                start_after(index)

    def skewed(index):
        relay(index, 1)
        start_after(index)
        relay(index, 2)
        if index > up:
            relay(index - 1, 3)

    def advance_both(index):
        @pl.when(is_mid)
        def _():
            skewed(index)

        @pl.when(is_end)
        def _():
            advance(index)

    def advance_for(role, index):
        @pl.when(role)
        def _():
            advance(index)

    def advance_at(step, role, index):
        @pl.when(jnp.logical_and(role, step < 3))
        def _():
            relay(index, step + 1)

        @pl.when(jnp.logical_and(role, step == 0))
        def _():
            start_after(index)

    def wait_y(first, last):
        count_wait(weights.at[first:last, 0, 0], y_recv.at[y_slot(first, 1)])

    def wait_x(first, last, h, sources):
        parts = 1 if h is not None else 2
        sample = weights.at[first:last, 0:parts, 0 : len(sources)]
        count_wait(sample, x_recv.at[x_slot(first, h, sources[0])])

    def tp_copy(src, dst, slot):
        return remote(src, dst, act_send.at[slot], act_recv.at[slot], t_peer)

    def y_act(src, dst, slot):
        return remote(src, dst, act_send.at[slot], act_recv.at[slot], y_peer)

    def y_start(places, parts=(0, 1)):
        for q in parts:
            for k in places:
                y_copy(k, q).start()

    y_start((0,), (0,))
    start(0)
    y_start((1,), (0,))
    y_start((0, 1), (1,))
    for k in range(chunks):
        for q in range(2):
            local_copy(k, q).start()

    own_columns = pl.ds(pl.multiple_of(tp * half_width, half_width), half_width)

    def squares(source, phase):
        def body(step, _):
            rows = pl.ds(pl.multiple_of(step * CHUNK_ROWS, CHUNK_ROWS), CHUNK_ROWS)
            total = None
            for tile in range(lane_tiles):
                value = source[rows, tile * LANES : (tile + 1) * LANES].astype(jnp.float32)
                total = value * value if total is None else total + value * value
            square_own[phase, rows, :] = total
            return 0

        lax.fori_loop(0, tokens // CHUNK_ROWS, body, 0)

    def square_copy(phase):
        return tp_copy(square_own.at[phase], square_got.at[phase], 9 + phase)

    def norm(source, phase, gain_ref, target):
        def body(step, _):
            rows = pl.ds(pl.multiple_of(step * CHUNK_ROWS, CHUNK_ROWS), CHUNK_ROWS)
            total = jnp.sum(square_own[phase, rows, :] + square_got[phase, rows, :], axis=1, keepdims=True)
            inverse = lax.rsqrt(total * (1.0 / width) + EPSILON)
            for tile in range(lane_tiles):
                value = source[rows, tile * LANES : (tile + 1) * LANES].astype(jnp.float32)
                gain = gain_ref[pl.ds(tp * lane_tiles + tile, 1), :]
                lanes = pl.ds(pl.multiple_of(tp * half_width + tile * LANES, LANES), LANES)
                target[y, rows, lanes] = (value * inverse * gain).astype(jnp.bfloat16)
            return 0

        lax.fori_loop(0, tokens // CHUNK_ROWS, body, 0)

    def block_copies(target, base):
        own = target.at[y, :, own_columns]
        theirs = target.at[1 - y, :, own_columns]
        return (
            tp_copy(own, own, base),
            y_act(own, own, base + 1),
            tp_copy(theirs, theirs, base + 2),
        )

    loads[0].wait()
    squares(stream_ref, 0)
    square_copy(0).start()
    loads[1].wait()
    mine = pl.ds(pl.multiple_of(y * quarter, quarter), quarter)
    peers = pl.ds(pl.multiple_of((1 - y) * quarter, quarter), quarter)
    offset_send[...] = offset_ref[:, peers].astype(jnp.bfloat16)
    offsets[0] = offset_ref[:, mine].astype(jnp.bfloat16)
    square_copy(0).wait_recv()
    norm(stream_ref, 0, first_gain_ref, normed)
    first_tp, first_y, first_pass = block_copies(normed, 0)
    first_tp.start()
    offset_copy = y_act(offset_send, offsets.at[1], 3)

    y_start((2,))
    wide = jnp.exp(-jnp.abs(param_ref[...]))
    ratio = wide / (2.0 + wide)
    ratio_square = ratio * ratio
    log_sum = jnp.ones_like(ratio) * (1.0 / 17.0)
    for odd in (15.0, 13.0, 11.0, 9.0, 7.0, 5.0, 3.0, 1.0):
        log_sum = log_sum * ratio_square + 1.0 / odd
    rate_ref[...] = -DECAY_MULTIPLIER * (jnp.maximum(-param_ref[...], 0.0) + 2.0 * ratio * log_sum)

    size = decay_maps_ref.shape[1]
    per = LANES // size
    tiles = quarter // LANES
    maps[...] = jnp.zeros_like(maps)
    for tile in range(tiles):
        for index in range(per):
            place = y * (tiles * per) + tile * per + index
            span = slice(index * size, (index + 1) * size)
            maps[tile, span, index * size : (index + 1) * size] = decay_maps_ref[place]
            maps[tile, span, LANES + index * size : LANES + (index + 1) * size] = input_maps_ref[place]

    @pl.when(is_mid)
    def _():
        advance(0)
        first_y.start()
        advance(1)
        offset_copy.start()
        advance(2)
        y_start(range(3, last_raise))
        advance(3)

    @pl.when(is_end)
    def _():
        for place, (index, m) in enumerate(END_ORDER):
            relay(index, m)
            if place % 3 == 0:
                start_after(index)
            if place == 1:
                first_y.start()
            if place == 4:
                offset_copy.start()
            if place == 7:
                y_start(range(3, last_raise))

    first_y.wait_recv()
    first_pass.start()

    count_wait(weights.at[:, :, 0], local_sem.at[0])
    wait_y(0, 2)
    advance_for(is_mid, 4)
    wait_x(0, 2, None, every)
    first_tp.wait_recv()

    def project(which, token_block, *relays):
        def body(step, _):
            for role, index in relays:
                advance_at(step, role, index)
            matrix = weights[step // 2, step % 2].reshape(width, block)
            projected[which, step] = jnp.dot(
                normed[token_block], matrix, preferred_element_type=jnp.float32
            ).astype(jnp.bfloat16)
            return 0

        lax.fori_loop(0, 4, body, 0)

    reach = taps_ref.shape[0]

    def recur(which, *relays):
        def body(step, _):
            for role, index in relays:
                advance_at(step, role, index)
            rows = pl.ds(pl.multiple_of(step * SEQ_LEN, SEQ_LEN), SEQ_LEN)
            for tile in range(tiles):
                part, lane = tile * LANES // block, tile * LANES % block
                lanes = slice(lane, lane + LANES)
                taps = taps_ref[
                    :, pl.ds(pl.multiple_of(y * quarter + tile * LANES, LANES), LANES)
                ].astype(jnp.float32)
                values = projected[which, part, rows, lanes].astype(jnp.float32)
                filtered = taps[reach - 1 : reach] * values
                for back in range(1, reach):
                    tap = taps[reach - 1 - back : reach - back]
                    filtered = filtered + tap * shift_down(values, back, 0.0)
                conved = filtered.astype(jnp.bfloat16)
                logits = jnp.dot(conved, maps[tile], preferred_element_type=jnp.float32)
                offset = offsets[which, rows, tile * LANES : (tile + 1) * LANES].astype(jnp.float32)
                steps = 1.0 / (1.0 + jnp.exp(-logits))
                rate = rate_ref[pl.ds(y * tiles + tile, 1), :]
                log_decay = steps[:, :LANES] * rate + offset
                decay = jnp.exp(log_decay)
                twice = -2.0 * log_decay
                series = 1.0 + twice * (
                    -1 / 2
                    + twice
                    * (1 / 6 + twice * (-1 / 24 + twice * (1 / 120 + twice * (-1 / 720 + twice * (1 / 5040)))))
                )
                lost = jnp.where(twice < 0.35, twice * series, 1.0 - decay * decay)
                state = jnp.sqrt(lost) * steps[:, LANES:] * conved.astype(jnp.float32)
                span = 1
                while span < SEQ_LEN:
                    state = state + decay * shift_down(state, span, 0.0)
                    if span * 2 < SEQ_LEN:
                        decay = decay * shift_down(decay, span, 1.0)
                    span *= 2
                gate = projected[which, 2 + part, rows, lanes].astype(jnp.float32)
                gelu = 0.5 * gate * (1.0 + lax.erf(gate * 0.7071067811865476))
                mixed[which, rows, tile * LANES : (tile + 1) * LANES] = (state * gelu).astype(jnp.bfloat16)
            return 0

        lax.fori_loop(0, tokens // SEQ_LEN, body, 0)

    project(0, y, (is_end, 4))
    recur(0)
    first_pass.wait_recv()
    project(1, 1 - y, (is_mid, 5))
    offset_copy.wait_recv()
    recur(1, (is_end, 5))


    @pl.when(is_mid)
    def _():
        skewed(up)

    wait_y(2, 3)
    wait_x(2, 3, None, every)

    def mix_out(which, *relays):
        def body(step, _):
            for role, index in relays:
                advance_at(step, role, index)

            def term(place):
                matrix = weights[2, :, place].reshape(quarter, block)
                return jnp.dot(mixed[which], matrix, preferred_element_type=jnp.float32).astype(jnp.bfloat16)

            lanes = pl.ds(pl.multiple_of(step * block, block), block)
            per_half = n_fs // 2
            passed[which, :, lanes] = term(per_half * (1 - tp) + step)
            kept[which, :, lanes] = term(per_half * tp + step)
            return 0

        lax.fori_loop(0, n_fs // 2, body, 0)

    def mix_copy(which):
        return tp_copy(passed.at[which], got.at[which], 4 + which)

    mix_out(1, (is_end, 6))
    mix_copy(1).start()
    mix_out(0)
    mix_copy(0).start()

    def add_peer(step, _):
        rows = pl.ds(pl.multiple_of(step * CHUNK_ROWS, CHUNK_ROWS), CHUNK_ROWS)
        mid_send[rows, :] = (
            kept[1, rows, :].astype(jnp.float32) + got[1, rows, :].astype(jnp.float32)
        ).astype(jnp.bfloat16)
        return 0

    mix_copy(1).wait_recv()
    lax.fori_loop(0, tokens // CHUNK_ROWS, add_peer, 0)
    mid_copy = y_act(mid_send, mid_got, 6)
    mid_copy.start()
    y_start(lowers, (0,))

    for index in range(1, raises + 1):
        advance_both(up + index)
    mix_copy(0).wait_recv()
    relay(up + raises + 1, 1)
    start_after(up + raises + 1)
    relay(up + raises + 1, 2)

    @pl.when(is_mid)
    def _():
        relay(up + raises, 3)

    mid_copy.wait_recv()

    def add_own(step, _):
        rows = pl.ds(pl.multiple_of(step * CHUNK_ROWS, CHUNK_ROWS), CHUNK_ROWS)
        total = None
        for tile in range(lane_tiles):
            lanes = slice(tile * LANES, (tile + 1) * LANES)
            update = kept[0, rows, lanes].astype(jnp.float32) + got[0, rows, lanes].astype(jnp.float32)
            update = update + mid_got[rows, lanes].astype(jnp.float32)
            value = (stream_ref[rows, lanes].astype(jnp.float32) + update).astype(jnp.bfloat16)
            middle[rows, lanes] = value
            value = value.astype(jnp.float32)
            total = value * value if total is None else total + value * value
        square_own[1, rows, :] = total
        return 0

    lax.fori_loop(0, tokens // CHUNK_ROWS, add_own, 0)
    square_copy(1).start()
    square_copy(1).wait_recv()
    norm(middle, 1, second_gain_ref, normed_mid)
    second_tp, second_y, second_pass = block_copies(normed_mid, 11)
    second_y.start()
    second_tp.start()

    @pl.when(is_end)
    def _():
        relay(up + raises + 1, 3)

    for index in range(2, raises):
        advance_both(up + raises + index)
    down = up + 2 * raises
    wait_y(3, last_raise)
    for k in range(3, last_raise):
        if k == last_raise - 1:
            advance_both(down)

            @pl.when(is_mid)
            def _():
                skewed(down + 1)

        wait_x(k, k + 1, None, every)

    def lift(which, token_block, *relays):
        def body(step, _):
            for role, index in relays:
                advance_at(step, role, index)
            matrix = weights[3 + step // 2, step % 2].reshape(width, block)
            total = jnp.dot(normed_mid[token_block], matrix, preferred_element_type=jnp.float32)
            lanes = pl.ds(pl.multiple_of(step * block, block), block)
            activity[which, :, lanes] = jnp.square(jnp.maximum(total, 0.0)).astype(jnp.bfloat16)
            return 0

        lax.fori_loop(0, 2 * raises, body, 0)

    second_tp.wait_recv()
    lift(0, y)

    @pl.when(is_mid)
    def _():
        skewed(down + 2)

    advance_for(is_end, down + 1)

    second_y.wait_recv()
    y_start(lowers, (1,))
    second_pass.start()
    second_pass.wait_recv()
    lift(1, 1 - y, (is_end, down + 2))

    for index in range(3, raises):
        advance(down + index)

    depth = raises * quarter

    def lower(h, m):
        place = 2 * plane(m) + (y if h == 0 else 1 - y)

        def body(which, _):
            matrix = weights[last_raise:chunks, :, place].reshape(depth, block)
            partial[m, h, which] = jnp.dot(
                activity[which], matrix, preferred_element_type=jnp.float32
            ).astype(jnp.bfloat16)
            return 0

        lax.fori_loop(0, 2, body, 0)

    def is_owner(m):
        return low if m < 2 else jnp.logical_not(low)

    def owner_copy(h, m):
        slot = 14 + 2 * (m % 2) + h
        return tp_copy(partial.at[m, h], partial_got.at[m % 2, h], slot)

    def last_copy(h, m):
        slot = 18 + 2 * (m % 2)
        return remote(
            last_send.at[m % 2, h],
            last_got.at[m % 2, 1 - h],
            act_send.at[slot + h],
            act_recv.at[slot + 1 - h],
            y_peer,
        )

    def pass_on(h, m):
        @pl.when(jnp.logical_not(is_owner(m)))
        def _():
            owner_copy(h, m).start()

    def finish(h, m):
        @pl.when(is_owner(m))
        def _():
            (last_part(1) if (h, m) == (1, 1) else owner_copy(h, m)).wait_recv()

            def body(step, _):
                rows = pl.ds(pl.multiple_of(step * CHUNK_ROWS, CHUNK_ROWS), CHUNK_ROWS)
                last_send[m % 2, h, rows, :] = (
                    partial[m, h, 1, rows, :].astype(jnp.float32)
                    + partial_got[m % 2, h, 1, rows, :].astype(jnp.float32)
                ).astype(jnp.bfloat16)
                return 0

            lax.fori_loop(0, tokens // CHUNK_ROWS, body, 0)
            last_copy(h, m).start()

    def last_part(which):
        return tp_copy(partial.at[1, 1, which], partial_got.at[1, 1, which], 17 if which else 22)

    def lower_last():
        place = 2 * plane(1) + 1 - y
        split = (raises - 1) * quarter
        for k in range(last_raise, chunks - 1):
            wait_x(k, k + 1, 1, (1,))

        def early(which, _):
            matrix = weights[last_raise : chunks - 1, :, place].reshape(split, block)
            total[which] = jnp.dot(activity[which, :, :split], matrix, preferred_element_type=jnp.float32)
            return 0

        lax.fori_loop(0, 2, early, 0)
        wait_x(chunks - 1, chunks, 1, (1,))
        for which in (1, 0):
            matrix = weights[chunks - 1, :, place].reshape(quarter, block)
            term = jnp.dot(activity[which, :, split:], matrix, preferred_element_type=jnp.float32)
            partial[1, 1, which] = (total[which] + term).astype(jnp.bfloat16)

            @pl.when(jnp.logical_not(low))
            def _():
                last_part(which).start()

    def close(h, mm):
        owned = mm + 2 * (1 - low.astype(jnp.int32))
        last_copy(1 - h, mm).wait_recv()
        place = 2 * ((z % 2 + mm) % 2) + (y if h == 0 else 1 - y)
        lanes = pl.ds(pl.multiple_of(place * block, block), block)

        def body(step, _):
            rows = pl.ds(pl.multiple_of(step * CHUNK_ROWS, CHUNK_ROWS), CHUNK_ROWS)
            update = (
                partial[owned, h, 0, rows, :].astype(jnp.float32)
                + partial_got[mm, h, 0, rows, :].astype(jnp.float32)
                + last_got[mm, h, rows, :].astype(jnp.float32)
            )
            out_ref[rows, lanes] = (middle[rows, lanes].astype(jnp.float32) + update).astype(jnp.bfloat16)
            return 0

        lax.fori_loop(0, tokens // CHUNK_ROWS, body, 0)

    order = [(0, m) for m in range(4)] + [(1, m) for m in (0, 2, 3, 1)]
    far, near = down + raises, down + 2 * raises

    def first_far(index):
        relay(index, 2)
        start_after(index)

    @pl.when(is_mid)
    def _():
        first_far(far)
        relay(far - 1, 3)
        first_far(far + 1)
        relay(far, 3)

    advance_for(is_end, far)
    wait_y(last_raise, chunks)
    wait_x(last_raise, chunks, 0, every)
    for index, (h, m) in enumerate(order):
        if index == 2:

            @pl.when(is_mid)
            def _():
                first_far(far + 2)
                relay(far + 1, 3)

        if index == 4:

            @pl.when(is_mid)
            def _():
                relay(far + 2, 3)

        if index in (2, 4):
            advance_for(is_end, far + index // 2)
        if index >= 5:
            advance(near + index - 5)
        if (h, m) == (1, 1):
            lower_last()
            finish(1, 1)
            continue
        if h == 1 and m:
            wait_x(last_raise, chunks, 1, (m,))
        lower(h, m)
        pass_on(h, m)
        if index and index < 5:
            finish(*order[index - 1])
        if index >= 4:
            finish(h, m)
    close(1, 0)
    close(0, 0)

    @pl.when(low)
    def _():
        last_part(0).wait_recv()

    close(1, 1)
    close(0, 1)

    count_wait(weights.at[:, :, 0], y_send.at[0])
    count_wait(weights.at[:, 0, 0:6], x_send.at[0])
    count_wait(weights.at[:, 0, 0:4], z_send.at[0])

    @pl.when(is_mid)
    def _():
        count_wait(weights.at[:, 0, 0:4], z_send.at[0])

    for copy in (first_tp, first_y, first_pass, second_tp, second_y, second_pass, offset_copy, mid_copy):
        copy.wait_send()
    for phase in range(2):
        square_copy(phase).wait_send()
        mix_copy(phase).wait_send()
    for h, m in order:

        @pl.when(is_owner(m))
        def _():
            last_copy(h, m).wait_send()

        @pl.when(jnp.logical_not(is_owner(m)))
        def _():
            if (h, m) == (1, 1):
                last_part(0).wait_send()
                last_part(1).wait_send()
            else:
                owner_copy(h, m).wait_send()


def whole_layer(
    stream,
    recurrent_norm_gain,
    feedforward_norm_gain,
    recurrent_input_weight,
    output_gate_weight,
    causal_filter_weight,
    decay_gate_matrix,
    input_gate_matrix,
    channel_decay_param,
    token_decay_offset,
    recurrent_output_weight,
    up_projection_weight,
    down_projection_weight,
):
    tokens, half_width = stream.shape
    width = 2 * half_width
    quarter = half_width // 2
    block, n_fs = quarter // 2, 8
    raises = up_projection_weight.shape[1] // half_width
    chunks = 3 + 2 * raises
    depth = raises * quarter
    tiles = quarter // LANES
    half_type, full_type = jnp.bfloat16, jnp.float32
    vmem = pl.BlockSpec(memory_space=pltpu.VMEM)
    anywhere = pl.BlockSpec(memory_space=pl.ANY)
    dma = pltpu.SemaphoreType.DMA
    return pl.pallas_call(
        whole_kernel,
        out_shape=jax.ShapeDtypeStruct((tokens, half_width), half_type),
        in_specs=[anywhere] * 2 + [vmem] * 6 + [anywhere] * 5,
        out_specs=vmem,
        scratch_shapes=[
            pltpu.VMEM((tokens, half_width), half_type),
            pltpu.VMEM((tokens, half_width), full_type),
            pltpu.VMEM((half_width // LANES, LANES), full_type),
            pltpu.VMEM((chunks, 2, n_fs, block, block), half_type),
            pltpu.VMEM((2, tokens, width), half_type),
            pltpu.VMEM((2, tokens, width), half_type),
            pltpu.VMEM((2, tokens, LANES), full_type),
            pltpu.VMEM((2, tokens, LANES), full_type),
            pltpu.VMEM((2, 4, tokens, block), half_type),
            pltpu.VMEM((2, tokens, quarter), half_type),
            pltpu.VMEM((2, tokens, quarter), half_type),
            pltpu.VMEM((tokens, quarter), half_type),
            pltpu.VMEM((tiles, LANES, 2 * LANES), half_type),
            pltpu.VMEM((2, tokens, half_width), half_type),
            pltpu.VMEM((2, tokens, half_width), half_type),
            pltpu.VMEM((2, tokens, half_width), half_type),
            pltpu.VMEM((tokens, half_width), half_type),
            pltpu.VMEM((tokens, half_width), half_type),
            pltpu.VMEM((tokens, half_width), half_type),
            pltpu.VMEM((2, tokens, depth), half_type),
            pltpu.VMEM((4, 2, 2, tokens, block), half_type),
            pltpu.VMEM((2, 2, 2, tokens, block), half_type),
            pltpu.VMEM((2, tokens, block), full_type),
            pltpu.VMEM((2, 2, tokens, block), half_type),
            pltpu.VMEM((2, 2, tokens, block), half_type),
            dma((1,)),
            dma((1,)),
            dma((chunks + 4,)),
            dma((1,)),
            dma((chunks, 2, 3)),
            dma((1,)),
            dma((2 * raises + 5,)),
            dma((23,)),
            dma((23,)),
            dma((2,)),
        ],
        compiler_params=pltpu.CompilerParams(
            collective_id=0, has_side_effects=True, vmem_limit_bytes=67043328
        ),
        name="whole_layer",
    )(
        stream,
        token_decay_offset,
        recurrent_norm_gain.reshape(-1, LANES),
        feedforward_norm_gain.reshape(-1, LANES),
        causal_filter_weight,
        decay_gate_matrix,
        input_gate_matrix,
        channel_decay_param.reshape(-1, LANES),
        recurrent_input_weight,
        output_gate_weight,
        recurrent_output_weight,
        up_projection_weight,
        down_projection_weight,
    )


def fits_whole(sizes, stream, up_projection_weight, decay_gate_matrix):
    tokens, half_width = stream.shape
    return (
        sizes == (2, 8, 2)
        and half_width % (8 * LANES) == 0
        and tokens % (4 * SEQ_LEN) == 0
        and up_projection_weight.shape[1] % half_width == 0
        and up_projection_weight.shape[1] // half_width >= 3
        and LANES % decay_gate_matrix.shape[1] == 0
    )


def solution(mesh):
    in_specs = (
        P(("rep", "fs"), "tp"),
        P(),
        P(),
        P("fs", "tp"),
        P("fs", "tp"),
        P(None, "tp"),
        P("tp", None, None),
        P("tp", None, None),
        P("tp"),
        P(("rep", "fs"), "tp"),
        P("tp", "fs"),
        P("fs", "tp"),
        P("tp", "fs"),
    )
    out_specs = P(("rep", "fs"), "tp")
    sizes = tuple(mesh.shape[axis] for axis in ("rep", "fs", "tp"))

    def body(*args):
        if fits_whole(sizes, args[0], args[11], args[6]):
            return whole_layer(*args)
        return shards(sizes, *args)

    return jax.shard_map(
        body, mesh=mesh, in_specs=in_specs, out_specs=out_specs, check_vma=False
    )
```

```python
import functools

import jax
import jax.numpy as jnp
from jax import lax
from jax.experimental import pallas as pl
from jax.experimental.pallas import tpu as pltpu
from jax.sharding import PartitionSpec as P


SEQ_LEN = 128
EPSILON = 1e-06
DECAY_MULTIPLIER = 8.0
LANES = 128


def half(values, which, axis):
    first, second = jnp.split(values, 2, axis)
    return jnp.where(which == 0, first, second)


def gather_shard(shard, ids, sizes):
    rep, fs, _ = ids
    _, n_fs, _ = sizes
    own, for_peer = shard
    hops = n_fs // 2
    place, side = fs // 2, fs % 2
    from_peer = lax.ppermute(for_peer, "fs", [(i, i ^ 1) for i in range(n_fs)])
    start = jnp.where(side == rep, own, from_peer)
    up = [(i, (i + 2) % n_fs) for i in range(n_fs)]
    down = [(i, (i + n_fs - 2) % n_fs) for i in range(n_fs)]
    pieces, places = [own, from_peer], [fs, fs ^ 1]
    below = above = start
    for step in range(1, hops):
        if step % 2:
            below = mine = lax.ppermute(below, "fs", up)
            base = 2 * ((place + hops - (step + 1) // 2) % hops)
        else:
            above = mine = lax.ppermute(above, "fs", down)
            base = 2 * ((place + step // 2) % hops)
        pieces += [mine, lax.ppermute(mine, "rep", [(0, 1), (1, 0)])]
        places += [base + rep, base + 1 - rep]
    return pieces, jnp.stack(places).astype(jnp.int32)


def gather_features(values, tp, n_tp):
    if n_tp != 2:
        return lax.all_gather(values, "tp", axis=1, tiled=True)
    other = lax.ppermute(values, "tp", [(0, 1), (1, 0)])
    return jnp.where(
        tp == 0, jnp.concatenate([values, other], 1), jnp.concatenate([other, values], 1)
    )


def sum_features(parts, tp, n_tp):
    total = lax.dynamic_index_in_dim(parts, tp, 0, False).astype(jnp.float32)
    for shift in range(1, n_tp):
        piece = lax.dynamic_index_in_dim(parts, (tp + shift) % n_tp, 0, False)
        got = lax.ppermute(piece, "tp", [(i, (i + shift) % n_tp) for i in range(n_tp)])
        total = total + got.astype(jnp.float32)
    return total.astype(jnp.bfloat16)


def norm_rows(values, gain):
    widened = values.astype(jnp.float32)
    inverse = lax.rsqrt(jnp.mean(widened * widened, axis=-1, keepdims=True) + EPSILON)
    return (widened * inverse * gain).astype(jnp.bfloat16)


ROWS = 256
CHUNK = 512


def depth_kernel(squared, places_ref, x_ref, *refs):
    *pieces, out_ref = refs
    depth, width = pieces[0].shape
    chunk = min(CHUNK, width)
    for lower in range(0, width, chunk):
        cols = slice(lower, lower + chunk)
        total = None
        for index, piece in enumerate(pieces):
            place = pl.multiple_of(places_ref[index] * depth, depth)
            term = jnp.dot(
                x_ref[:, pl.ds(place, depth)], piece[:, cols], preferred_element_type=jnp.float32
            )
            total = term if total is None else total + term
        if squared:
            total = jnp.square(jnp.maximum(total, 0.0))
        out_ref[:, cols] = total.astype(jnp.bfloat16)


def depth_matmul(x, gathered, squared=False):
    pieces, places = gathered
    tokens, width = x.shape
    shape = pieces[0].shape
    return pl.pallas_call(
        functools.partial(depth_kernel, squared),
        grid_spec=pltpu.PrefetchScalarGridSpec(
            num_scalar_prefetch=1,
            grid=(tokens // ROWS,),
            in_specs=[pl.BlockSpec((ROWS, width), lambda m, _: (m, 0))]
            + [pl.BlockSpec(shape, lambda m, _: (0, 0))] * len(pieces),
            out_specs=pl.BlockSpec((ROWS, shape[1]), lambda m, _: (m, 0)),
        ),
        out_shape=jax.ShapeDtypeStruct((tokens, shape[1]), jnp.bfloat16),
        cost_estimate=pl.CostEstimate(
            flops=2 * tokens * width * shape[1],
            bytes_accessed=2 * (tokens * width + (tokens + width) * shape[1]),
            transcendentals=0,
        ),
        name="depth_matmul",
    )(places, x, *pieces)


def columns_kernel(per, places_ref, x_ref, *refs):
    *pieces, out_ref = refs
    cols = pieces[0].shape[1]
    for index, piece in enumerate(pieces):
        place = places_ref[index]
        lower = pl.multiple_of((place % per) * cols, cols)
        out_ref[place // per, :, pl.ds(lower, cols)] = jnp.dot(
            x_ref[...], piece[...], preferred_element_type=jnp.float32
        ).astype(jnp.bfloat16)


def columns_matmul(x, gathered, n_tp, first, tokens):
    pieces, places = gathered
    depth, cols = pieces[0].shape
    per = len(pieces) // n_tp
    skip = first // ROWS
    return pl.pallas_call(
        functools.partial(columns_kernel, per),
        grid_spec=pltpu.PrefetchScalarGridSpec(
            num_scalar_prefetch=1,
            grid=(tokens // ROWS,),
            in_specs=[pl.BlockSpec((ROWS, depth), lambda m, _: (m + skip, 0))]
            + [pl.BlockSpec((depth, cols), lambda m, _: (0, 0))] * len(pieces),
            out_specs=pl.BlockSpec((n_tp, ROWS, per * cols), lambda m, _: (0, m, 0)),
        ),
        out_shape=jax.ShapeDtypeStruct((n_tp, tokens, per * cols), jnp.bfloat16),
        cost_estimate=pl.CostEstimate(
            flops=2 * tokens * depth * cols * len(pieces),
            bytes_accessed=2 * (tokens * depth + len(pieces) * cols * (depth + tokens)),
            transcendentals=0,
        ),
        name="columns_matmul",
    )(places, x, *pieces)


def shift_down(values, amount, fill):
    index = lax.broadcasted_iota(jnp.int32, values.shape, 0)
    return jnp.where(index < amount, fill, pltpu.roll(values, amount, 0))


def recurrence_kernel(
    side_ref, value_ref, gate_ref, own_ref, peer_ref, taps_ref, maps_ref, rate_ref, out_ref
):
    rows, channels = value_ref.shape
    reach = taps_ref.shape[0]
    per = LANES // maps_ref.shape[1]
    is_own = pl.program_id(0) < pl.num_programs(0) // 2
    for tile in range(channels // LANES):
        cols = slice(tile * LANES, (tile + 1) * LANES)
        values = value_ref[:, cols].astype(jnp.float32)
        filtered = taps_ref[reach - 1 : reach, cols] * values
        for back in range(1, reach):
            tap = taps_ref[reach - 1 - back : reach - back, cols]
            filtered = filtered + tap * shift_down(values, back, 0.0)
        conved = filtered.astype(jnp.bfloat16)
        maps = maps_ref[tile * per : (tile + 1) * per].reshape(LANES, 2 * LANES)
        logits = jnp.dot(conved, maps, preferred_element_type=jnp.float32)
        offset = jnp.where(is_own, own_ref[:, cols], peer_ref[:, cols].astype(jnp.float32))
        steps = 1.0 / (1.0 + jnp.exp(-logits))
        log_decay = steps[:, :LANES] * rate_ref[:, cols] + offset
        decay = jnp.exp(log_decay)
        y = -2.0 * log_decay
        series = 1.0 + y * (
            -1 / 2 + y * (1 / 6 + y * (-1 / 24 + y * (1 / 120 + y * (-1 / 720 + y * (1 / 5040)))))
        )
        lost = jnp.where(y < 0.35, y * series, 1.0 - decay * decay)
        state = jnp.sqrt(lost) * steps[:, LANES:] * conved.astype(jnp.float32)
        span = 1
        while span < rows:
            state = state + decay * shift_down(state, span, 0.0)
            if span * 2 < rows:
                decay = decay * shift_down(decay, span, 1.0)
            span *= 2
        gate = gate_ref[:, cols].astype(jnp.float32)
        gelu = 0.5 * gate * (1.0 + lax.erf(gate * 0.7071067811865476))
        out_ref[:, cols] = (state * gelu).astype(jnp.bfloat16)


def recurrence(projected, offset_own, offset_peer, taps, decay_maps, input_maps, rate, side):
    tokens = projected.shape[0]
    channels = offset_peer.shape[1]
    blocks, size, _ = decay_maps.shape
    per = LANES // size
    block = jnp.arange(blocks)[:, None, None] % per
    group = jnp.arange(LANES)[None, None, :] // size

    def diagonal(maps):
        return jnp.where(block == group, jnp.tile(maps, (1, 1, per)), 0)

    maps = jnp.concatenate([diagonal(decay_maps), diagonal(input_maps)], 2)
    sequences = tokens // SEQ_LEN
    own = sequences // 2
    return pl.pallas_call(
        recurrence_kernel,
        grid_spec=pltpu.PrefetchScalarGridSpec(
            num_scalar_prefetch=1,
            grid=(sequences,),
            in_specs=[
                pl.BlockSpec((SEQ_LEN, channels), lambda s, side: (s, 0)),
                pl.BlockSpec((SEQ_LEN, channels), lambda s, side: (s, 1)),
                pl.BlockSpec(
                    (SEQ_LEN, channels), lambda s, side: (jnp.minimum(s, own - 1), side[0])
                ),
                pl.BlockSpec((SEQ_LEN, channels), lambda s, side: (jnp.maximum(s - own, 0), 0)),
                pl.BlockSpec((taps.shape[0], channels), lambda s, side: (0, side[0])),
                pl.BlockSpec((blocks // 2, size, 2 * LANES), lambda s, side: (side[0], 0, 0)),
                pl.BlockSpec((1, channels), lambda s, side: (0, side[0])),
            ],
            out_specs=pl.BlockSpec((SEQ_LEN, channels), lambda s, side: (s, 0)),
        ),
        out_shape=jax.ShapeDtypeStruct((tokens, channels), jnp.bfloat16),
        cost_estimate=pl.CostEstimate(
            flops=tokens * channels * 700,
            bytes_accessed=tokens * channels * 10,
            transcendentals=tokens * channels * 6,
        ),
        name="recurrence",
    )(
        side.astype(jnp.int32)[None],
        projected,
        projected,
        offset_own,
        offset_peer,
        taps.astype(jnp.float32),
        maps,
        rate[None, :],
    )


def shards(
    sizes,
    stream,
    recurrent_norm_gain,
    feedforward_norm_gain,
    recurrent_input_weight,
    output_gate_weight,
    causal_filter_weight,
    decay_gate_matrix,
    input_gate_matrix,
    channel_decay_param,
    token_decay_offset,
    recurrent_output_weight,
    up_projection_weight,
    down_projection_weight,
):
    _, n_fs, n_tp = sizes
    ids = lax.axis_index("rep"), lax.axis_index("fs"), lax.axis_index("tp")
    _, fs, tp = ids
    side = fs % 2
    pairs = [(i, i ^ 1) for i in range(n_fs)]
    tokens = stream.shape[0]

    def halves(weight, axis):
        return half(weight, side, axis), half(weight, 1 - side, axis)

    def to_peer(values):
        return lax.ppermute(values, "fs", pairs)

    value_own, value_peer = halves(recurrent_input_weight, 1)
    gate_own, gate_peer = halves(output_gate_weight, 1)
    entry = (
        jnp.concatenate([value_own, gate_own], 1),
        jnp.concatenate([value_peer, gate_peer], 1),
    )
    entry_full = gather_shard(entry, ids, sizes)
    stream_peer = to_peer(stream)
    offset_peer = to_peer(half(token_decay_offset, 1 - side, 1).astype(jnp.bfloat16))
    output_full = gather_shard(halves(recurrent_output_weight, 0), ids, sizes)
    expand_full = gather_shard(halves(up_projection_weight, 1), ids, sizes)
    contract_full = gather_shard(halves(down_projection_weight, 0), ids, sizes)

    own_pair = jnp.concatenate([stream, stream_peer], 0)
    whole = gather_features(own_pair, tp, n_tp)
    normed = norm_rows(whole, recurrent_norm_gain)
    projected = depth_matmul(normed, entry_full)
    mixed = recurrence(
        projected,
        token_decay_offset,
        offset_peer,
        causal_filter_weight,
        decay_gate_matrix,
        input_gate_matrix,
        -DECAY_MULTIPLIER * jax.nn.softplus(-channel_decay_param),
        side,
    )
    mixer_terms = columns_matmul(mixed, output_full, n_tp, 0, 2 * tokens)
    mixer_chip = sum_features(mixer_terms, tp, n_tp)
    got_own = to_peer(mixer_chip[tokens:])
    got_peer = to_peer(mixer_chip[:tokens])
    update = mixer_chip.astype(jnp.float32) + jnp.concatenate([got_own, got_peer], 0).astype(
        jnp.float32
    )
    middle = (own_pair.astype(jnp.float32) + update).astype(jnp.bfloat16)
    normed_mid = norm_rows(gather_features(middle, tp, n_tp), feedforward_norm_gain)
    activity = depth_matmul(normed_mid, expand_full, squared=True)
    peer_terms = columns_matmul(activity, contract_full, n_tp, tokens, tokens)
    got = to_peer(sum_features(peer_terms, tp, n_tp))
    own_terms = columns_matmul(activity, contract_full, n_tp, 0, tokens)
    own_chip = sum_features(own_terms, tp, n_tp)
    channel_sum = own_chip.astype(jnp.float32) + got.astype(jnp.float32)
    return (middle[:tokens].astype(jnp.float32) + channel_sum).astype(jnp.bfloat16)


MESH = pl.DeviceIdType.MESH
CHUNK_ROWS = 128
AHEAD = (1, 1, 1, 1, 2, 3)
STEADY = 4
LEAD = 2
END_ORDER = (
    (0, 1), (0, 2), (0, 3), (1, 2), (1, 1), (1, 3), (2, 2), (2, 1), (2, 3), (3, 2), (3, 1), (3, 3),
)


def whole_kernel(
    stream_hbm,
    offset_hbm,
    first_gain_hbm,
    second_gain_hbm,
    taps_hbm,
    decay_maps_hbm,
    input_maps_hbm,
    param_hbm,
    value_hbm,
    gate_hbm,
    output_hbm,
    raise_hbm,
    lower_hbm,
    out_ref,
    stream_ref,
    offset_ref,
    first_gain_ref,
    second_gain_ref,
    taps_ref,
    decay_maps_ref,
    input_maps_ref,
    param_ref,
    rate_ref,
    weights,
    normed,
    normed_mid,
    square_own,
    square_got,
    projected,
    mixed,
    offsets,
    offset_send,
    maps,
    kept,
    passed,
    got,
    mid_send,
    mid_got,
    middle,
    activity,
    partial,
    partial_got,
    total,
    last_send,
    last_got,
    local_sem,
    y_send,
    y_recv,
    z_send,
    z_recv,
    x_send,
    x_recv,
    act_send,
    act_recv,
    load_sem,
):
    rep, fs, tp = lax.axis_index("rep"), lax.axis_index("fs"), lax.axis_index("tp")
    z, y = fs // 2, fs % 2
    tokens, half_width = stream_ref.shape
    width = 2 * half_width
    chunks, _, n_fs, block, _ = weights.shape
    quarter = half_width // 2
    lane_tiles = half_width // LANES
    raises = (chunks - 3) // 2
    last_raise = 3 + raises
    lowers = range(last_raise, chunks)
    is_mid = jnp.logical_or(z == 1, z == 2)
    is_end = jnp.logical_not(is_mid)
    low = (z // 2) == tp

    def plane(m):
        return 2 * ((z // 2 + m // 2) % 2) + (z % 2 + m % 2) % 2

    x_peer = (1 - rep, fs, tp)
    y_peer = (rep, 2 * z + 1 - y, tp)
    t_peer = (rep, fs, 1 - tp)

    def z_peer(m):
        return (rep, 2 * plane(m) + y, tp)

    places = (
        (stream_hbm, stream_ref),
        (first_gain_hbm, first_gain_ref),
        (offset_hbm, offset_ref),
        (second_gain_hbm, second_gain_ref),
        (taps_hbm, taps_ref),
        (decay_maps_hbm, decay_maps_ref),
        (input_maps_hbm, input_maps_ref),
        (param_hbm, param_ref),
    )
    loads = [
        pltpu.make_async_copy(source, target, load_sem.at[index])
        for index, (source, target) in enumerate(places)
    ]
    for load in loads:
        load.start()

    barrier = pltpu.get_barrier_semaphore()
    for peer in (x_peer, y_peer, t_peer, z_peer(1), z_peer(2), z_peer(3)):
        pl.semaphore_signal(barrier, inc=1, device_id=peer, device_id_type=MESH)
    pl.semaphore_wait(barrier, 6)

    def remote(src, dst, send, recv, peer):
        return pltpu.make_async_remote_copy(
            src_ref=src, dst_ref=dst, send_sem=send, recv_sem=recv, device_id=peer, device_id_type=MESH
        )

    def shard_block(k, side, part):
        if k < 2 or 3 <= k < 3 + raises:
            ref = (value_hbm, gate_hbm)[k] if k < 2 else raise_hbm
            first = 0 if k < 2 else (k - 3) * quarter
            span = ref.shape[1] // 2
            start = pl.multiple_of(side * span + first + part * block, block)
            return ref.at[:, pl.ds(start, block)]
        ref = output_hbm if k == 2 else lower_hbm
        first = 0 if k == 2 else (k - 3 - raises) * quarter
        span = ref.shape[0] // 2
        start = pl.multiple_of(side * span + first + part * block, block)
        return ref.at[pl.ds(start, block), :]

    def part_of(q):
        return rep if q == 0 else 1 - rep

    def local_copy(k, q):
        part = part_of(q)
        return pltpu.make_async_copy(
            shard_block(k, y, part), weights.at[k, part, fs], local_sem.at[0]
        )

    def group_of(k):
        return 0 if k < 2 else 1 if k == 2 else 2 if k < last_raise else 3

    def y_slot(k, q):
        return k if q == 0 else chunks + group_of(k)

    def x_slot(k, h, m):
        if k < last_raise:
            return group_of(k) if k < 3 else k - 1
        return 2 + raises + (0 if h == 0 else m - 1 if m > 1 else 3 + k - last_raise)

    def count_wait(ref, sem):
        pltpu.make_async_copy(ref, ref, sem).wait()

    def y_copy(k, q):
        part = part_of(q)
        return remote(
            shard_block(k, 1 - y, part), weights.at[k, part, fs], y_send.at[0], y_recv.at[y_slot(k, q)], y_peer
        )

    def z_copy(k, h, m):
        spot = weights.at[k, rep, fs if h == 0 else 2 * z + 1 - y]
        src = shard_block(k, y, rep) if h == 0 else spot
        return remote(src, spot, z_send.at[0], z_recv.at[k, h, m - 1], z_peer(m))

    def z_relay(k, h):
        spot = weights.at[k, rep, 2 * plane(2) + (y if h == 0 else 1 - y)]
        return remote(spot, spot, z_send.at[0], z_recv.at[k, h, 2], z_peer(1))

    def x_copy(k, h, m):
        spot = weights.at[k, rep, 2 * plane(m) + (y if h == 0 else 1 - y)]
        return remote(spot, spot, x_send.at[0], x_recv.at[x_slot(k, h, m)], x_peer)

    every = (2, 1, 3)
    up = 6
    events = [(k, h, every) for k, h in ((0, 0), (1, 0), (0, 1), (1, 1), (2, 0), (2, 1))]
    events += [(k, h, every) for h in range(2) for k in range(3, last_raise)]
    events += [(k, 0, every) for k in lowers]
    events += [(k, 1, (2, 3)) for k in lowers] + [(k, 1, (1,)) for k in lowers]

    def start_after(index):
        def reach_of(place):
            return place + AHEAD[min(place, len(AHEAD) - 1)] if place >= 0 else 0

        for later in range(reach_of(index - 1) + 1, reach_of(index) + 1):
            if later == STEADY + 1:

                @pl.when(is_mid)
                def _():
                    start(STEADY + 1)

            else:
                start(later)

    def start(index):
        if index >= len(events):
            return
        k, h, sources = events[index]
        if h == 1 and 2 in sources:
            y_copy(k, 0).wait_recv()
        for m in sources:
            if m == 1 and index >= 1:

                @pl.when(is_end)
                def _():
                    z_copy(k, h, 1).start()

            elif m < 3:
                z_copy(k, h, m).start()
            else:

                @pl.when(is_mid)
                def _():
                    z_copy(k, h, 3).start()

    def relay(index, m):
        k, h, _ = events[index]
        z_copy(k, h, m).wait_recv()
        x_copy(k, h, m).start()

        @pl.when(jnp.logical_and(is_mid, m == 2))
        def _():
            z_relay(k, h).start()
            lead = index + (1 if index < STEADY else LEAD)
            for place in (lead,) if index != STEADY else (lead - 1, lead):
                next_k, next_h, next_sources = events[min(place, len(events) - 1)]
                if next_sources == every:
                    z_copy(next_k, next_h, 1).start()
            far_step = index - up - 3 * raises
            if far_step == raises - 2:
                z_copy(last_raise, 1, 1).start()
            if far_step == raises - 1:
                for later_k in range(last_raise + 1, chunks):
                    z_copy(later_k, 1, 1).start()

    def advance(index):
        for place, m in enumerate(sorted(events[index][2])):
            relay(index, m)
            if place == 0:
                start_after(index)

    def skewed(index):
        relay(index, 1)
        start_after(index)
        relay(index, 2)
        if index > up:
            relay(index - 1, 3)

    def advance_both(index):
        @pl.when(is_mid)
        def _():
            skewed(index)

        @pl.when(is_end)
        def _():
            advance(index)

    def advance_for(role, index):
        @pl.when(role)
        def _():
            advance(index)

    def advance_at(step, role, index, first=1, last=3):
        @pl.when(jnp.logical_and(role, jnp.logical_and(step + 1 >= first, step + 1 <= last)))
        def _():
            relay(index, step + 1)

        if first == 1:

            @pl.when(jnp.logical_and(role, step == 0))
            def _():
                start_after(index)

    def wait_y(first, last):
        count_wait(weights.at[first:last, 0, 0], y_recv.at[y_slot(first, 1)])

    def wait_x(first, last, h, sources):
        parts = 1 if h is not None else 2
        sample = weights.at[first:last, 0:parts, 0 : len(sources)]
        count_wait(sample, x_recv.at[x_slot(first, h, sources[0])])

    def tp_copy(src, dst, slot):
        return remote(src, dst, act_send.at[slot], act_recv.at[slot], t_peer)

    def y_act(src, dst, slot):
        return remote(src, dst, act_send.at[slot], act_recv.at[slot], y_peer)

    def y_start(places, parts=(0, 1)):
        for q in parts:
            for k in places:
                y_copy(k, q).start()

    y_start((0,), (0,))
    start(0)
    y_start((1,), (0,))
    y_start((0, 1), (1,))
    for k in range(chunks):
        for q in range(2):
            local_copy(k, q).start()

    own_columns = pl.ds(pl.multiple_of(tp * half_width, half_width), half_width)

    def squares(source, phase):
        def body(step, _):
            rows = pl.ds(pl.multiple_of(step * CHUNK_ROWS, CHUNK_ROWS), CHUNK_ROWS)
            total = None
            for tile in range(lane_tiles):
                value = source[rows, tile * LANES : (tile + 1) * LANES].astype(jnp.float32)
                total = value * value if total is None else total + value * value
            square_own[phase, rows, :] = total
            return 0

        lax.fori_loop(0, tokens // CHUNK_ROWS, body, 0)

    def square_copy(phase):
        return tp_copy(square_own.at[phase], square_got.at[phase], 9 + phase)

    def norm(source, phase, gain_ref, target):
        def body(step, _):
            rows = pl.ds(pl.multiple_of(step * CHUNK_ROWS, CHUNK_ROWS), CHUNK_ROWS)
            total = jnp.sum(square_own[phase, rows, :] + square_got[phase, rows, :], axis=1, keepdims=True)
            inverse = lax.rsqrt(total * (1.0 / width) + EPSILON)
            for tile in range(lane_tiles):
                value = source[rows, tile * LANES : (tile + 1) * LANES].astype(jnp.float32)
                gain = gain_ref[pl.ds(tp * lane_tiles + tile, 1), :]
                lanes = pl.ds(pl.multiple_of(tp * half_width + tile * LANES, LANES), LANES)
                target[y, rows, lanes] = (value * inverse * gain).astype(jnp.bfloat16)
            return 0

        lax.fori_loop(0, tokens // CHUNK_ROWS, body, 0)

    def block_copies(target, base):
        own = target.at[y, :, own_columns]
        theirs = target.at[1 - y, :, own_columns]
        return (
            tp_copy(own, own, base),
            y_act(own, own, base + 1),
            tp_copy(theirs, theirs, base + 2),
        )

    loads[0].wait()
    loads[1].wait()
    squares(stream_ref, 0)
    square_copy(0).start()
    for load in loads[2:]:
        load.wait()
    mine = pl.ds(pl.multiple_of(y * quarter, quarter), quarter)
    peers = pl.ds(pl.multiple_of((1 - y) * quarter, quarter), quarter)
    offset_send[...] = offset_ref[:, peers].astype(jnp.bfloat16)
    offsets[0] = offset_ref[:, mine].astype(jnp.bfloat16)
    square_copy(0).wait_recv()
    norm(stream_ref, 0, first_gain_ref, normed)
    first_tp, first_y, first_pass = block_copies(normed, 0)
    first_tp.start()
    offset_copy = y_act(offset_send, offsets.at[1], 3)

    y_start((2,))
    wide = jnp.exp(-jnp.abs(param_ref[...]))
    ratio = wide / (2.0 + wide)
    ratio_square = ratio * ratio
    log_sum = jnp.ones_like(ratio) * (1.0 / 17.0)
    for odd in (15.0, 13.0, 11.0, 9.0, 7.0, 5.0, 3.0, 1.0):
        log_sum = log_sum * ratio_square + 1.0 / odd
    rate_ref[...] = -DECAY_MULTIPLIER * (jnp.maximum(-param_ref[...], 0.0) + 2.0 * ratio * log_sum)

    size = decay_maps_ref.shape[1]
    per = LANES // size
    tiles = quarter // LANES
    maps[...] = jnp.zeros_like(maps)
    for tile in range(tiles):
        for index in range(per):
            place = y * (tiles * per) + tile * per + index
            span = slice(index * size, (index + 1) * size)
            maps[tile, span, index * size : (index + 1) * size] = decay_maps_ref[place]
            maps[tile, span, LANES + index * size : LANES + (index + 1) * size] = input_maps_ref[place]

    @pl.when(is_mid)
    def _():
        advance(0)
        first_y.start()
        advance(1)
        offset_copy.start()
        advance(2)
        y_start(range(3, last_raise))
        advance(3)

    @pl.when(is_end)
    def _():
        for place, (index, m) in enumerate(END_ORDER):
            relay(index, m)
            if place % 3 == 0:
                start_after(index)
            if place == 1:
                first_y.start()
            if place == 4:
                offset_copy.start()
            if place == 7:
                y_start(range(3, last_raise))
        start(STEADY + 1)

    first_y.wait_recv()
    first_pass.start()

    count_wait(weights.at[:, :, 0], local_sem.at[0])
    wait_y(0, 2)
    advance_for(is_mid, 4)
    wait_x(0, 2, None, every)
    first_tp.wait_recv()

    def project(which, token_block, *relays):
        def body(step, _):
            for role, *steps in relays:
                advance_at(step, role, *steps)
            matrix = weights[step // 2, step % 2].reshape(width, block)
            projected[which, step] = jnp.dot(
                normed[token_block], matrix, preferred_element_type=jnp.float32
            ).astype(jnp.bfloat16)
            return 0

        lax.fori_loop(0, 4, body, 0)

    reach = taps_ref.shape[0]

    def recur(which, *relays):
        def body(step, _):
            for role, *steps in relays:
                advance_at(step, role, *steps)
            rows = pl.ds(pl.multiple_of(step * SEQ_LEN, SEQ_LEN), SEQ_LEN)
            for tile in range(tiles):
                part, lane = tile * LANES // block, tile * LANES % block
                lanes = slice(lane, lane + LANES)
                taps = taps_ref[
                    :, pl.ds(pl.multiple_of(y * quarter + tile * LANES, LANES), LANES)
                ].astype(jnp.float32)
                values = projected[which, part, rows, lanes].astype(jnp.float32)
                filtered = taps[reach - 1 : reach] * values
                for back in range(1, reach):
                    tap = taps[reach - 1 - back : reach - back]
                    filtered = filtered + tap * shift_down(values, back, 0.0)
                conved = filtered.astype(jnp.bfloat16)
                logits = jnp.dot(conved, maps[tile], preferred_element_type=jnp.float32)
                offset = offsets[which, rows, tile * LANES : (tile + 1) * LANES].astype(jnp.float32)
                steps = 1.0 / (1.0 + jnp.exp(-logits))
                rate = rate_ref[pl.ds(y * tiles + tile, 1), :]
                log_decay = steps[:, :LANES] * rate + offset
                decay = jnp.exp(log_decay)
                twice = -2.0 * log_decay
                series = 1.0 + twice * (
                    -1 / 2
                    + twice
                    * (1 / 6 + twice * (-1 / 24 + twice * (1 / 120 + twice * (-1 / 720 + twice * (1 / 5040)))))
                )
                lost = jnp.where(twice < 0.35, twice * series, 1.0 - decay * decay)
                state = jnp.sqrt(lost) * steps[:, LANES:] * conved.astype(jnp.float32)
                span = 1
                while span < SEQ_LEN:
                    state = state + decay * shift_down(state, span, 0.0)
                    if span * 2 < SEQ_LEN:
                        decay = decay * shift_down(decay, span, 1.0)
                    span *= 2
                gate = projected[which, 2 + part, rows, lanes].astype(jnp.float32)
                gelu = 0.5 * gate * (1.0 + lax.erf(gate * 0.7071067811865476))
                mixed[which, rows, tile * LANES : (tile + 1) * LANES] = (state * gelu).astype(jnp.bfloat16)
            return 0

        lax.fori_loop(0, tokens // SEQ_LEN, body, 0)

    project(0, y, (is_end, 4))
    recur(0, (is_mid, 5, 1, 2))
    first_pass.wait_recv()
    project(1, 1 - y, (is_mid, 5, 3, 3))
    offset_copy.wait_recv()
    recur(1, (is_end, 5))


    @pl.when(is_mid)
    def _():
        skewed(up)

    wait_y(2, 3)
    wait_x(2, 3, None, every)

    def mix_out(which, *relays):
        def body(step, _):
            for role, *steps in relays:
                advance_at(step, role, *steps)

            def term(place):
                matrix = weights[2, :, place].reshape(quarter, block)
                return jnp.dot(mixed[which], matrix, preferred_element_type=jnp.float32).astype(jnp.bfloat16)

            lanes = pl.ds(pl.multiple_of(step * block, block), block)
            per_half = n_fs // 2
            passed[which, :, lanes] = term(per_half * (1 - tp) + step)
            kept[which, :, lanes] = term(per_half * tp + step)
            return 0

        lax.fori_loop(0, n_fs // 2, body, 0)

    def mix_copy(which):
        return tp_copy(passed.at[which], got.at[which], 4 + which)

    mix_out(1, (is_end, 6))
    mix_copy(1).start()
    mix_out(0)
    mix_copy(0).start()

    def add_peer(step, _):
        rows = pl.ds(pl.multiple_of(step * CHUNK_ROWS, CHUNK_ROWS), CHUNK_ROWS)
        mid_send[rows, :] = (
            kept[1, rows, :].astype(jnp.float32) + got[1, rows, :].astype(jnp.float32)
        ).astype(jnp.bfloat16)
        return 0

    mix_copy(1).wait_recv()
    lax.fori_loop(0, tokens // CHUNK_ROWS, add_peer, 0)
    mid_copy = y_act(mid_send, mid_got, 6)
    mid_copy.start()
    y_start(lowers, (0,))

    for index in range(1, raises + 1):
        advance_both(up + index)
    mix_copy(0).wait_recv()
    relay(up + raises + 1, 1)
    start_after(up + raises + 1)
    relay(up + raises + 1, 2)

    @pl.when(is_mid)
    def _():
        relay(up + raises, 3)

    mid_copy.wait_recv()

    def add_own(step, _):
        rows = pl.ds(pl.multiple_of(step * CHUNK_ROWS, CHUNK_ROWS), CHUNK_ROWS)
        total = None
        for tile in range(lane_tiles):
            lanes = slice(tile * LANES, (tile + 1) * LANES)
            update = kept[0, rows, lanes].astype(jnp.float32) + got[0, rows, lanes].astype(jnp.float32)
            update = update + mid_got[rows, lanes].astype(jnp.float32)
            value = (stream_ref[rows, lanes].astype(jnp.float32) + update).astype(jnp.bfloat16)
            middle[rows, lanes] = value
            value = value.astype(jnp.float32)
            total = value * value if total is None else total + value * value
        square_own[1, rows, :] = total
        return 0

    lax.fori_loop(0, tokens // CHUNK_ROWS, add_own, 0)
    square_copy(1).start()
    square_copy(1).wait_recv()
    norm(middle, 1, second_gain_ref, normed_mid)
    second_tp, second_y, second_pass = block_copies(normed_mid, 11)
    second_y.start()
    second_tp.start()

    @pl.when(is_end)
    def _():
        relay(up + raises + 1, 3)

    for index in range(2, raises):
        advance_both(up + raises + index)
    down = up + 2 * raises
    wait_y(3, last_raise)
    for k in range(3, last_raise):
        if k == last_raise - 1:
            advance_both(down)

            @pl.when(is_mid)
            def _():
                skewed(down + 1)

        wait_x(k, k + 1, None, every)

    def lift(which, token_block, *relays):
        def body(step, _):
            for role, *steps in relays:
                advance_at(step, role, *steps)
            matrix = weights[3 + step // 2, step % 2].reshape(width, block)
            total = jnp.dot(normed_mid[token_block], matrix, preferred_element_type=jnp.float32)
            lanes = pl.ds(pl.multiple_of(step * block, block), block)
            activity[which, :, lanes] = jnp.square(jnp.maximum(total, 0.0)).astype(jnp.bfloat16)
            return 0

        lax.fori_loop(0, 2 * raises, body, 0)

    second_tp.wait_recv()
    lift(0, y)

    @pl.when(is_mid)
    def _():
        skewed(down + 2)

    advance_for(is_end, down + 1)

    second_y.wait_recv()
    y_start(lowers, (1,))
    second_pass.start()
    second_pass.wait_recv()
    lift(1, 1 - y, (is_end, down + 2))

    for index in range(3, raises):
        advance(down + index)

    depth = raises * quarter

    def lower(h, m):
        place = 2 * plane(m) + (y if h == 0 else 1 - y)

        def body(which, _):
            matrix = weights[last_raise:chunks, :, place].reshape(depth, block)
            partial[m, h, which] = jnp.dot(
                activity[which], matrix, preferred_element_type=jnp.float32
            ).astype(jnp.bfloat16)
            return 0

        lax.fori_loop(0, 2, body, 0)

    def is_owner(m):
        return low if m < 2 else jnp.logical_not(low)

    def owner_copy(h, m):
        slot = 14 + 2 * (m % 2) + h
        return tp_copy(partial.at[m, h], partial_got.at[m % 2, h], slot)

    def last_copy(h, m):
        slot = 18 + 2 * (m % 2)
        return remote(
            last_send.at[m % 2, h],
            last_got.at[m % 2, 1 - h],
            act_send.at[slot + h],
            act_recv.at[slot + 1 - h],
            y_peer,
        )

    def pass_on(h, m):
        @pl.when(jnp.logical_not(is_owner(m)))
        def _():
            owner_copy(h, m).start()

    def finish(h, m):
        @pl.when(is_owner(m))
        def _():
            (last_part(1) if (h, m) == (1, 1) else owner_copy(h, m)).wait_recv()

            def body(step, _):
                rows = pl.ds(pl.multiple_of(step * CHUNK_ROWS, CHUNK_ROWS), CHUNK_ROWS)
                last_send[m % 2, h, rows, :] = (
                    partial[m, h, 1, rows, :].astype(jnp.float32)
                    + partial_got[m % 2, h, 1, rows, :].astype(jnp.float32)
                ).astype(jnp.bfloat16)
                return 0

            lax.fori_loop(0, tokens // CHUNK_ROWS, body, 0)
            last_copy(h, m).start()

    def last_part(which):
        return tp_copy(partial.at[1, 1, which], partial_got.at[1, 1, which], 17 if which else 22)

    def lower_last():
        place = 2 * plane(1) + 1 - y
        split = (raises - 1) * quarter
        for k in range(last_raise, chunks - 1):
            wait_x(k, k + 1, 1, (1,))

        def early(which, _):
            matrix = weights[last_raise : chunks - 1, :, place].reshape(split, block)
            total[which] = jnp.dot(activity[which, :, :split], matrix, preferred_element_type=jnp.float32)
            return 0

        lax.fori_loop(0, 2, early, 0)
        wait_x(chunks - 1, chunks, 1, (1,))
        for which in (1, 0):
            matrix = weights[chunks - 1, :, place].reshape(quarter, block)
            term = jnp.dot(activity[which, :, split:], matrix, preferred_element_type=jnp.float32)
            partial[1, 1, which] = (total[which] + term).astype(jnp.bfloat16)

            @pl.when(jnp.logical_not(low))
            def _():
                last_part(which).start()

    def close(h, mm):
        owned = mm + 2 * (1 - low.astype(jnp.int32))
        last_copy(1 - h, mm).wait_recv()
        place = 2 * ((z % 2 + mm) % 2) + (y if h == 0 else 1 - y)
        lanes = pl.ds(pl.multiple_of(place * block, block), block)

        def body(step, _):
            rows = pl.ds(pl.multiple_of(step * CHUNK_ROWS, CHUNK_ROWS), CHUNK_ROWS)
            update = (
                partial[owned, h, 0, rows, :].astype(jnp.float32)
                + partial_got[mm, h, 0, rows, :].astype(jnp.float32)
                + last_got[mm, h, rows, :].astype(jnp.float32)
            )
            out_ref[rows, lanes] = (middle[rows, lanes].astype(jnp.float32) + update).astype(jnp.bfloat16)
            return 0

        lax.fori_loop(0, tokens // CHUNK_ROWS, body, 0)

    order = [(0, m) for m in range(4)] + [(1, m) for m in (0, 2, 3, 1)]
    far, near = down + raises, down + 2 * raises

    def first_far(index):
        relay(index, 2)
        start_after(index)

    @pl.when(is_mid)
    def _():
        first_far(far)
        relay(far - 1, 3)
        first_far(far + 1)
        relay(far, 3)

    advance_for(is_end, far)
    wait_y(last_raise, chunks)
    wait_x(last_raise, chunks, 0, every)
    for index, (h, m) in enumerate(order):
        if index == 2:

            @pl.when(is_mid)
            def _():
                first_far(far + 2)
                relay(far + 1, 3)

        if index == 4:

            @pl.when(is_mid)
            def _():
                relay(far + 2, 3)

        if index in (2, 4):
            advance_for(is_end, far + index // 2)
        if index >= 5:
            advance(near + index - 5)
        if (h, m) == (1, 1):
            lower_last()
            finish(1, 1)
            continue
        if h == 1 and m:
            wait_x(last_raise, chunks, 1, (m,))
        lower(h, m)
        pass_on(h, m)
        if index and index < 5:
            finish(*order[index - 1])
        if index >= 4:
            finish(h, m)
    close(1, 0)
    close(0, 0)

    @pl.when(low)
    def _():
        last_part(0).wait_recv()

    close(1, 1)
    close(0, 1)

    count_wait(weights.at[:, :, 0], y_send.at[0])
    count_wait(weights.at[:, 0, 0:6], x_send.at[0])
    count_wait(weights.at[:, 0, 0:4], z_send.at[0])

    @pl.when(is_mid)
    def _():
        count_wait(weights.at[:, 0, 0:4], z_send.at[0])

    for copy in (first_tp, first_y, first_pass, second_tp, second_y, second_pass, offset_copy, mid_copy):
        copy.wait_send()
    for phase in range(2):
        square_copy(phase).wait_send()
        mix_copy(phase).wait_send()
    for h, m in order:

        @pl.when(is_owner(m))
        def _():
            last_copy(h, m).wait_send()

        @pl.when(jnp.logical_not(is_owner(m)))
        def _():
            if (h, m) == (1, 1):
                last_part(0).wait_send()
                last_part(1).wait_send()
            else:
                owner_copy(h, m).wait_send()


def whole_layer(
    stream,
    recurrent_norm_gain,
    feedforward_norm_gain,
    recurrent_input_weight,
    output_gate_weight,
    causal_filter_weight,
    decay_gate_matrix,
    input_gate_matrix,
    channel_decay_param,
    token_decay_offset,
    recurrent_output_weight,
    up_projection_weight,
    down_projection_weight,
):
    tokens, half_width = stream.shape
    width = 2 * half_width
    quarter = half_width // 2
    block, n_fs = quarter // 2, 8
    raises = up_projection_weight.shape[1] // half_width
    chunks = 3 + 2 * raises
    depth = raises * quarter
    tiles = quarter // LANES
    half_type, full_type = jnp.bfloat16, jnp.float32
    vmem = pl.BlockSpec(memory_space=pltpu.VMEM)
    anywhere = pl.BlockSpec(memory_space=pl.ANY)
    dma = pltpu.SemaphoreType.DMA
    return pl.pallas_call(
        whole_kernel,
        out_shape=jax.ShapeDtypeStruct((tokens, half_width), half_type),
        in_specs=[anywhere] * 13,
        out_specs=vmem,
        scratch_shapes=[
            pltpu.VMEM((tokens, half_width), half_type),
            pltpu.VMEM((tokens, half_width), full_type),
            pltpu.VMEM((width // LANES, LANES), full_type),
            pltpu.VMEM((width // LANES, LANES), full_type),
            pltpu.VMEM(causal_filter_weight.shape, half_type),
            pltpu.VMEM(decay_gate_matrix.shape, half_type),
            pltpu.VMEM(input_gate_matrix.shape, half_type),
            pltpu.VMEM((half_width // LANES, LANES), full_type),
            pltpu.VMEM((half_width // LANES, LANES), full_type),
            pltpu.VMEM((chunks, 2, n_fs, block, block), half_type),
            pltpu.VMEM((2, tokens, width), half_type),
            pltpu.VMEM((2, tokens, width), half_type),
            pltpu.VMEM((2, tokens, LANES), full_type),
            pltpu.VMEM((2, tokens, LANES), full_type),
            pltpu.VMEM((2, 4, tokens, block), half_type),
            pltpu.VMEM((2, tokens, quarter), half_type),
            pltpu.VMEM((2, tokens, quarter), half_type),
            pltpu.VMEM((tokens, quarter), half_type),
            pltpu.VMEM((tiles, LANES, 2 * LANES), half_type),
            pltpu.VMEM((2, tokens, half_width), half_type),
            pltpu.VMEM((2, tokens, half_width), half_type),
            pltpu.VMEM((2, tokens, half_width), half_type),
            pltpu.VMEM((tokens, half_width), half_type),
            pltpu.VMEM((tokens, half_width), half_type),
            pltpu.VMEM((tokens, half_width), half_type),
            pltpu.VMEM((2, tokens, depth), half_type),
            pltpu.VMEM((4, 2, 2, tokens, block), half_type),
            pltpu.VMEM((2, 2, 2, tokens, block), half_type),
            pltpu.VMEM((2, tokens, block), full_type),
            pltpu.VMEM((2, 2, tokens, block), half_type),
            pltpu.VMEM((2, 2, tokens, block), half_type),
            dma((1,)),
            dma((1,)),
            dma((chunks + 4,)),
            dma((1,)),
            dma((chunks, 2, 3)),
            dma((1,)),
            dma((2 * raises + 5,)),
            dma((23,)),
            dma((23,)),
            dma((8,)),
        ],
        compiler_params=pltpu.CompilerParams(
            collective_id=0, has_side_effects=True, vmem_limit_bytes=67043328
        ),
        name="whole_layer",
    )(
        stream,
        token_decay_offset,
        recurrent_norm_gain.reshape(-1, LANES),
        feedforward_norm_gain.reshape(-1, LANES),
        causal_filter_weight,
        decay_gate_matrix,
        input_gate_matrix,
        channel_decay_param.reshape(-1, LANES),
        recurrent_input_weight,
        output_gate_weight,
        recurrent_output_weight,
        up_projection_weight,
        down_projection_weight,
    )


def fits_whole(sizes, stream, up_projection_weight, decay_gate_matrix):
    tokens, half_width = stream.shape
    return (
        sizes == (2, 8, 2)
        and half_width % (8 * LANES) == 0
        and tokens % (4 * SEQ_LEN) == 0
        and up_projection_weight.shape[1] % half_width == 0
        and up_projection_weight.shape[1] // half_width >= 3
        and LANES % decay_gate_matrix.shape[1] == 0
    )


def solution(mesh):
    in_specs = (
        P(("rep", "fs"), "tp"),
        P(),
        P(),
        P("fs", "tp"),
        P("fs", "tp"),
        P(None, "tp"),
        P("tp", None, None),
        P("tp", None, None),
        P("tp"),
        P(("rep", "fs"), "tp"),
        P("tp", "fs"),
        P("fs", "tp"),
        P("tp", "fs"),
    )
    out_specs = P(("rep", "fs"), "tp")
    sizes = tuple(mesh.shape[axis] for axis in ("rep", "fs", "tp"))

    def body(*args):
        if fits_whole(sizes, args[0], args[11], args[6]):
            return whole_layer(*args)
        return shards(sizes, *args)

    return jax.shard_map(
        body, mesh=mesh, in_specs=in_specs, out_specs=out_specs, check_vma=False
    )
```

```python
import functools

import jax
import jax.numpy as jnp
from jax import lax
from jax.experimental import pallas as pl
from jax.experimental.pallas import tpu as pltpu
from jax.sharding import PartitionSpec as P


SEQ_LEN = 128
EPSILON = 1e-06
DECAY_MULTIPLIER = 8.0
LANES = 128


def half(values, which, axis):
    first, second = jnp.split(values, 2, axis)
    return jnp.where(which == 0, first, second)


def gather_shard(shard, ids, sizes):
    rep, fs, _ = ids
    _, n_fs, _ = sizes
    own, for_peer = shard
    hops = n_fs // 2
    place, side = fs // 2, fs % 2
    from_peer = lax.ppermute(for_peer, "fs", [(i, i ^ 1) for i in range(n_fs)])
    start = jnp.where(side == rep, own, from_peer)
    up = [(i, (i + 2) % n_fs) for i in range(n_fs)]
    down = [(i, (i + n_fs - 2) % n_fs) for i in range(n_fs)]
    pieces, places = [own, from_peer], [fs, fs ^ 1]
    below = above = start
    for step in range(1, hops):
        if step % 2:
            below = mine = lax.ppermute(below, "fs", up)
            base = 2 * ((place + hops - (step + 1) // 2) % hops)
        else:
            above = mine = lax.ppermute(above, "fs", down)
            base = 2 * ((place + step // 2) % hops)
        pieces += [mine, lax.ppermute(mine, "rep", [(0, 1), (1, 0)])]
        places += [base + rep, base + 1 - rep]
    return pieces, jnp.stack(places).astype(jnp.int32)


def gather_features(values, tp, n_tp):
    if n_tp != 2:
        return lax.all_gather(values, "tp", axis=1, tiled=True)
    other = lax.ppermute(values, "tp", [(0, 1), (1, 0)])
    return jnp.where(
        tp == 0, jnp.concatenate([values, other], 1), jnp.concatenate([other, values], 1)
    )


def sum_features(parts, tp, n_tp):
    total = lax.dynamic_index_in_dim(parts, tp, 0, False).astype(jnp.float32)
    for shift in range(1, n_tp):
        piece = lax.dynamic_index_in_dim(parts, (tp + shift) % n_tp, 0, False)
        got = lax.ppermute(piece, "tp", [(i, (i + shift) % n_tp) for i in range(n_tp)])
        total = total + got.astype(jnp.float32)
    return total.astype(jnp.bfloat16)


def norm_rows(values, gain):
    widened = values.astype(jnp.float32)
    inverse = lax.rsqrt(jnp.mean(widened * widened, axis=-1, keepdims=True) + EPSILON)
    return (widened * inverse * gain).astype(jnp.bfloat16)


ROWS = 256
CHUNK = 512


def depth_kernel(squared, places_ref, x_ref, *refs):
    *pieces, out_ref = refs
    depth, width = pieces[0].shape
    chunk = min(CHUNK, width)
    for lower in range(0, width, chunk):
        cols = slice(lower, lower + chunk)
        total = None
        for index, piece in enumerate(pieces):
            place = pl.multiple_of(places_ref[index] * depth, depth)
            term = jnp.dot(
                x_ref[:, pl.ds(place, depth)], piece[:, cols], preferred_element_type=jnp.float32
            )
            total = term if total is None else total + term
        if squared:
            total = jnp.square(jnp.maximum(total, 0.0))
        out_ref[:, cols] = total.astype(jnp.bfloat16)


def depth_matmul(x, gathered, squared=False):
    pieces, places = gathered
    tokens, width = x.shape
    shape = pieces[0].shape
    return pl.pallas_call(
        functools.partial(depth_kernel, squared),
        grid_spec=pltpu.PrefetchScalarGridSpec(
            num_scalar_prefetch=1,
            grid=(tokens // ROWS,),
            in_specs=[pl.BlockSpec((ROWS, width), lambda m, _: (m, 0))]
            + [pl.BlockSpec(shape, lambda m, _: (0, 0))] * len(pieces),
            out_specs=pl.BlockSpec((ROWS, shape[1]), lambda m, _: (m, 0)),
        ),
        out_shape=jax.ShapeDtypeStruct((tokens, shape[1]), jnp.bfloat16),
        cost_estimate=pl.CostEstimate(
            flops=2 * tokens * width * shape[1],
            bytes_accessed=2 * (tokens * width + (tokens + width) * shape[1]),
            transcendentals=0,
        ),
        name="depth_matmul",
    )(places, x, *pieces)


def columns_kernel(per, places_ref, x_ref, *refs):
    *pieces, out_ref = refs
    cols = pieces[0].shape[1]
    for index, piece in enumerate(pieces):
        place = places_ref[index]
        lower = pl.multiple_of((place % per) * cols, cols)
        out_ref[place // per, :, pl.ds(lower, cols)] = jnp.dot(
            x_ref[...], piece[...], preferred_element_type=jnp.float32
        ).astype(jnp.bfloat16)


def columns_matmul(x, gathered, n_tp, first, tokens):
    pieces, places = gathered
    depth, cols = pieces[0].shape
    per = len(pieces) // n_tp
    skip = first // ROWS
    return pl.pallas_call(
        functools.partial(columns_kernel, per),
        grid_spec=pltpu.PrefetchScalarGridSpec(
            num_scalar_prefetch=1,
            grid=(tokens // ROWS,),
            in_specs=[pl.BlockSpec((ROWS, depth), lambda m, _: (m + skip, 0))]
            + [pl.BlockSpec((depth, cols), lambda m, _: (0, 0))] * len(pieces),
            out_specs=pl.BlockSpec((n_tp, ROWS, per * cols), lambda m, _: (0, m, 0)),
        ),
        out_shape=jax.ShapeDtypeStruct((n_tp, tokens, per * cols), jnp.bfloat16),
        cost_estimate=pl.CostEstimate(
            flops=2 * tokens * depth * cols * len(pieces),
            bytes_accessed=2 * (tokens * depth + len(pieces) * cols * (depth + tokens)),
            transcendentals=0,
        ),
        name="columns_matmul",
    )(places, x, *pieces)


def shift_down(values, amount, fill):
    index = lax.broadcasted_iota(jnp.int32, values.shape, 0)
    return jnp.where(index < amount, fill, pltpu.roll(values, amount, 0))


def recurrence_kernel(
    side_ref, value_ref, gate_ref, own_ref, peer_ref, taps_ref, maps_ref, rate_ref, out_ref
):
    rows, channels = value_ref.shape
    reach = taps_ref.shape[0]
    per = LANES // maps_ref.shape[1]
    is_own = pl.program_id(0) < pl.num_programs(0) // 2
    for tile in range(channels // LANES):
        cols = slice(tile * LANES, (tile + 1) * LANES)
        values = value_ref[:, cols].astype(jnp.float32)
        filtered = taps_ref[reach - 1 : reach, cols] * values
        for back in range(1, reach):
            tap = taps_ref[reach - 1 - back : reach - back, cols]
            filtered = filtered + tap * shift_down(values, back, 0.0)
        conved = filtered.astype(jnp.bfloat16)
        maps = maps_ref[tile * per : (tile + 1) * per].reshape(LANES, 2 * LANES)
        logits = jnp.dot(conved, maps, preferred_element_type=jnp.float32)
        offset = jnp.where(is_own, own_ref[:, cols], peer_ref[:, cols].astype(jnp.float32))
        steps = 1.0 / (1.0 + jnp.exp(-logits))
        log_decay = steps[:, :LANES] * rate_ref[:, cols] + offset
        decay = jnp.exp(log_decay)
        y = -2.0 * log_decay
        series = 1.0 + y * (
            -1 / 2 + y * (1 / 6 + y * (-1 / 24 + y * (1 / 120 + y * (-1 / 720 + y * (1 / 5040)))))
        )
        lost = jnp.where(y < 0.35, y * series, 1.0 - decay * decay)
        state = jnp.sqrt(lost) * steps[:, LANES:] * conved.astype(jnp.float32)
        span = 1
        while span < rows:
            state = state + decay * shift_down(state, span, 0.0)
            if span * 2 < rows:
                decay = decay * shift_down(decay, span, 1.0)
            span *= 2
        gate = gate_ref[:, cols].astype(jnp.float32)
        gelu = 0.5 * gate * (1.0 + lax.erf(gate * 0.7071067811865476))
        out_ref[:, cols] = (state * gelu).astype(jnp.bfloat16)


def recurrence(projected, offset_own, offset_peer, taps, decay_maps, input_maps, rate, side):
    tokens = projected.shape[0]
    channels = offset_peer.shape[1]
    blocks, size, _ = decay_maps.shape
    per = LANES // size
    block = jnp.arange(blocks)[:, None, None] % per
    group = jnp.arange(LANES)[None, None, :] // size

    def diagonal(maps):
        return jnp.where(block == group, jnp.tile(maps, (1, 1, per)), 0)

    maps = jnp.concatenate([diagonal(decay_maps), diagonal(input_maps)], 2)
    sequences = tokens // SEQ_LEN
    own = sequences // 2
    return pl.pallas_call(
        recurrence_kernel,
        grid_spec=pltpu.PrefetchScalarGridSpec(
            num_scalar_prefetch=1,
            grid=(sequences,),
            in_specs=[
                pl.BlockSpec((SEQ_LEN, channels), lambda s, side: (s, 0)),
                pl.BlockSpec((SEQ_LEN, channels), lambda s, side: (s, 1)),
                pl.BlockSpec(
                    (SEQ_LEN, channels), lambda s, side: (jnp.minimum(s, own - 1), side[0])
                ),
                pl.BlockSpec((SEQ_LEN, channels), lambda s, side: (jnp.maximum(s - own, 0), 0)),
                pl.BlockSpec((taps.shape[0], channels), lambda s, side: (0, side[0])),
                pl.BlockSpec((blocks // 2, size, 2 * LANES), lambda s, side: (side[0], 0, 0)),
                pl.BlockSpec((1, channels), lambda s, side: (0, side[0])),
            ],
            out_specs=pl.BlockSpec((SEQ_LEN, channels), lambda s, side: (s, 0)),
        ),
        out_shape=jax.ShapeDtypeStruct((tokens, channels), jnp.bfloat16),
        cost_estimate=pl.CostEstimate(
            flops=tokens * channels * 700,
            bytes_accessed=tokens * channels * 10,
            transcendentals=tokens * channels * 6,
        ),
        name="recurrence",
    )(
        side.astype(jnp.int32)[None],
        projected,
        projected,
        offset_own,
        offset_peer,
        taps.astype(jnp.float32),
        maps,
        rate[None, :],
    )


def shards(
    sizes,
    stream,
    recurrent_norm_gain,
    feedforward_norm_gain,
    recurrent_input_weight,
    output_gate_weight,
    causal_filter_weight,
    decay_gate_matrix,
    input_gate_matrix,
    channel_decay_param,
    token_decay_offset,
    recurrent_output_weight,
    up_projection_weight,
    down_projection_weight,
):
    _, n_fs, n_tp = sizes
    ids = lax.axis_index("rep"), lax.axis_index("fs"), lax.axis_index("tp")
    _, fs, tp = ids
    side = fs % 2
    pairs = [(i, i ^ 1) for i in range(n_fs)]
    tokens = stream.shape[0]

    def halves(weight, axis):
        return half(weight, side, axis), half(weight, 1 - side, axis)

    def to_peer(values):
        return lax.ppermute(values, "fs", pairs)

    value_own, value_peer = halves(recurrent_input_weight, 1)
    gate_own, gate_peer = halves(output_gate_weight, 1)
    entry = (
        jnp.concatenate([value_own, gate_own], 1),
        jnp.concatenate([value_peer, gate_peer], 1),
    )
    entry_full = gather_shard(entry, ids, sizes)
    stream_peer = to_peer(stream)
    offset_peer = to_peer(half(token_decay_offset, 1 - side, 1).astype(jnp.bfloat16))
    output_full = gather_shard(halves(recurrent_output_weight, 0), ids, sizes)
    expand_full = gather_shard(halves(up_projection_weight, 1), ids, sizes)
    contract_full = gather_shard(halves(down_projection_weight, 0), ids, sizes)

    own_pair = jnp.concatenate([stream, stream_peer], 0)
    whole = gather_features(own_pair, tp, n_tp)
    normed = norm_rows(whole, recurrent_norm_gain)
    projected = depth_matmul(normed, entry_full)
    mixed = recurrence(
        projected,
        token_decay_offset,
        offset_peer,
        causal_filter_weight,
        decay_gate_matrix,
        input_gate_matrix,
        -DECAY_MULTIPLIER * jax.nn.softplus(-channel_decay_param),
        side,
    )
    mixer_terms = columns_matmul(mixed, output_full, n_tp, 0, 2 * tokens)
    mixer_chip = sum_features(mixer_terms, tp, n_tp)
    got_own = to_peer(mixer_chip[tokens:])
    got_peer = to_peer(mixer_chip[:tokens])
    update = mixer_chip.astype(jnp.float32) + jnp.concatenate([got_own, got_peer], 0).astype(
        jnp.float32
    )
    middle = (own_pair.astype(jnp.float32) + update).astype(jnp.bfloat16)
    normed_mid = norm_rows(gather_features(middle, tp, n_tp), feedforward_norm_gain)
    activity = depth_matmul(normed_mid, expand_full, squared=True)
    peer_terms = columns_matmul(activity, contract_full, n_tp, tokens, tokens)
    got = to_peer(sum_features(peer_terms, tp, n_tp))
    own_terms = columns_matmul(activity, contract_full, n_tp, 0, tokens)
    own_chip = sum_features(own_terms, tp, n_tp)
    channel_sum = own_chip.astype(jnp.float32) + got.astype(jnp.float32)
    return (middle[:tokens].astype(jnp.float32) + channel_sum).astype(jnp.bfloat16)


MESH = pl.DeviceIdType.MESH
CHUNK_ROWS = 128
AHEAD = (1, 1, 1, 1, 2, 3)
STEADY = 4
LEAD = 1
END_ORDER = (
    (0, 1), (0, 2), (0, 3), (1, 2), (1, 1), (1, 3), (2, 2), (2, 1), (2, 3), (3, 2), (3, 1), (3, 3),
)


def whole_kernel(
    stream_hbm,
    offset_hbm,
    first_gain_hbm,
    second_gain_hbm,
    taps_hbm,
    decay_maps_hbm,
    input_maps_hbm,
    param_hbm,
    value_hbm,
    gate_hbm,
    output_hbm,
    raise_hbm,
    lower_hbm,
    out_ref,
    stream_ref,
    offset_ref,
    first_gain_ref,
    second_gain_ref,
    taps_ref,
    decay_maps_ref,
    input_maps_ref,
    param_ref,
    rate_ref,
    weights,
    normed,
    normed_mid,
    square_own,
    square_got,
    projected,
    mixed,
    offsets,
    offset_send,
    maps,
    kept,
    passed,
    got,
    mid_send,
    mid_got,
    middle,
    activity,
    partial,
    partial_got,
    total,
    last_send,
    last_got,
    local_sem,
    y_send,
    y_recv,
    z_send,
    z_recv,
    x_send,
    x_recv,
    act_send,
    act_recv,
    load_sem,
):
    rep, fs, tp = lax.axis_index("rep"), lax.axis_index("fs"), lax.axis_index("tp")
    z, y = fs // 2, fs % 2
    tokens, half_width = stream_ref.shape
    width = 2 * half_width
    chunks, _, n_fs, block, _ = weights.shape
    quarter = half_width // 2
    lane_tiles = half_width // LANES
    raises = (chunks - 3) // 2
    last_raise = 3 + raises
    lowers = range(last_raise, chunks)
    is_mid = jnp.logical_or(z == 1, z == 2)
    is_end = jnp.logical_not(is_mid)
    low = (z // 2) == tp

    def plane(m):
        return 2 * ((z // 2 + m // 2) % 2) + (z % 2 + m % 2) % 2

    x_peer = (1 - rep, fs, tp)
    y_peer = (rep, 2 * z + 1 - y, tp)
    t_peer = (rep, fs, 1 - tp)

    def z_peer(m):
        return (rep, 2 * plane(m) + y, tp)

    places = (
        (stream_hbm, stream_ref),
        (first_gain_hbm, first_gain_ref),
        (offset_hbm, offset_ref),
        (second_gain_hbm, second_gain_ref),
        (taps_hbm, taps_ref),
        (decay_maps_hbm, decay_maps_ref),
        (input_maps_hbm, input_maps_ref),
        (param_hbm, param_ref),
    )
    loads = [
        pltpu.make_async_copy(source, target, load_sem.at[index])
        for index, (source, target) in enumerate(places)
    ]
    for load in loads:
        load.start()

    barrier = pltpu.get_barrier_semaphore()
    for peer in (x_peer, y_peer, t_peer, z_peer(1), z_peer(2), z_peer(3)):
        pl.semaphore_signal(barrier, inc=1, device_id=peer, device_id_type=MESH)
    pl.semaphore_wait(barrier, 6)

    def remote(src, dst, send, recv, peer):
        return pltpu.make_async_remote_copy(
            src_ref=src, dst_ref=dst, send_sem=send, recv_sem=recv, device_id=peer, device_id_type=MESH
        )

    def shard_block(k, side, part):
        if k < 2 or 3 <= k < 3 + raises:
            ref = (value_hbm, gate_hbm)[k] if k < 2 else raise_hbm
            first = 0 if k < 2 else (k - 3) * quarter
            span = ref.shape[1] // 2
            start = pl.multiple_of(side * span + first + part * block, block)
            return ref.at[:, pl.ds(start, block)]
        ref = output_hbm if k == 2 else lower_hbm
        first = 0 if k == 2 else (k - 3 - raises) * quarter
        span = ref.shape[0] // 2
        start = pl.multiple_of(side * span + first + part * block, block)
        return ref.at[pl.ds(start, block), :]

    def part_of(q):
        return rep if q == 0 else 1 - rep

    def local_copy(k, q):
        part = part_of(q)
        return pltpu.make_async_copy(
            shard_block(k, y, part), weights.at[k, part, fs], local_sem.at[0]
        )

    def group_of(k):
        return 0 if k < 2 else 1 if k == 2 else 2 if k < last_raise else 3

    def y_slot(k, q):
        return k if q == 0 else chunks + group_of(k)

    def x_slot(k, h, m, half=None):
        if k < last_raise:
            return group_of(k) if k < 3 else k - 1
        if half is not None:
            return 5 + raises + (0 if half == 0 else 1 if k < chunks - 1 else 2)
        return 2 + raises + (0 if h == 0 else m - 1)

    def count_wait(ref, sem):
        pltpu.make_async_copy(ref, ref, sem).wait()

    def y_copy(k, q):
        part = part_of(q)
        return remote(
            shard_block(k, 1 - y, part), weights.at[k, part, fs], y_send.at[0], y_recv.at[y_slot(k, q)], y_peer
        )

    def cut(place, k, half):
        if half is None:
            return weights.at[k, rep, place]
        return weights.at[k, rep, place, :, half * (block // 2) : (half + 1) * (block // 2)]

    def z_copy(k, h, m, half=None):
        spot = cut(fs if h == 0 else 2 * z + 1 - y, k, half)
        src = shard_block(k, y, rep) if h == 0 else spot
        slot = 3 if half else m - 1
        return remote(src, spot, z_send.at[0], z_recv.at[k, h, slot], z_peer(m))

    def z_relay(k, h):
        spot = weights.at[k, rep, 2 * plane(2) + (y if h == 0 else 1 - y)]
        return remote(spot, spot, z_send.at[0], z_recv.at[k, h, 2], z_peer(1))

    def x_copy(k, h, m, half=None):
        spot = cut(2 * plane(m) + (y if h == 0 else 1 - y), k, half)
        return remote(spot, spot, x_send.at[0], x_recv.at[x_slot(k, h, m, half)], x_peer)

    every = (2, 1, 3)
    up = 6
    events = [(k, h, every, None) for k, h in ((0, 0), (1, 0), (0, 1), (1, 1), (2, 0), (2, 1))]
    events += [(k, h, every, None) for h in range(2) for k in range(3, last_raise)]
    events += [(k, 0, every, None) for k in lowers]
    events += [(k, 1, (2, 3), None) for k in lowers]
    events += [(k, 1, (1,), half) for half in range(2) for k in lowers]

    def start_after(index):
        def reach_of(place):
            return place + AHEAD[min(place, len(AHEAD) - 1)] if place >= 0 else 0

        for later in range(reach_of(index - 1) + 1, reach_of(index) + 1):
            if later == STEADY + 1:

                @pl.when(is_mid)
                def _():
                    start(STEADY + 1)

            else:
                start(later)

    def start(index):
        if index >= len(events):
            return
        k, h, sources, half = events[index]
        if h == 1 and 2 in sources:
            y_copy(k, 0).wait_recv()
        for m in sources:
            if m == 1 and index >= 1:

                @pl.when(is_end)
                def _():
                    z_copy(k, h, 1, half).start()

            elif m < 3:
                z_copy(k, h, m).start()
            else:

                @pl.when(is_mid)
                def _():
                    z_copy(k, h, 3).start()

    def relay(index, m):
        k, h, _, half = events[index]
        z_copy(k, h, m, half).wait_recv()
        x_copy(k, h, m, half).start()

        @pl.when(jnp.logical_and(is_mid, m == 2))
        def _():
            z_relay(k, h).start()
            lead = index + (1 if index < STEADY else LEAD)
            for place in (lead,):
                next_k, next_h, next_sources, _ = events[min(place, len(events) - 1)]
                if next_sources == every:
                    z_copy(next_k, next_h, 1).start()
            far_step = index - up - 3 * raises
            if far_step == raises - 2:
                z_copy(last_raise, 1, 1, 0).start()
            if far_step == raises - 1:
                for later_k in range(last_raise + 1, chunks):
                    z_copy(later_k, 1, 1, 0).start()
                for later_k in lowers:
                    z_copy(later_k, 1, 1, 1).start()

    def advance(index):
        for place, m in enumerate(sorted(events[index][2])):
            relay(index, m)
            if place == 0:
                start_after(index)

    def skewed(index):
        relay(index, 1)
        start_after(index)
        relay(index, 2)
        if index > up:
            relay(index - 1, 3)

    def advance_both(index):
        @pl.when(is_mid)
        def _():
            skewed(index)

        @pl.when(is_end)
        def _():
            advance(index)

    def advance_for(role, index):
        @pl.when(role)
        def _():
            advance(index)

    def advance_at(step, role, index, first=1, last=3):
        @pl.when(jnp.logical_and(role, jnp.logical_and(step + 1 >= first, step + 1 <= last)))
        def _():
            relay(index, step + 1)

        if first == 1:

            @pl.when(jnp.logical_and(role, step == 0))
            def _():
                start_after(index)

    def wait_y(first, last):
        count_wait(weights.at[first:last, 0, 0], y_recv.at[y_slot(first, 1)])

    def wait_x(first, last, h, sources):
        parts = 1 if h is not None else 2
        sample = weights.at[first:last, 0:parts, 0 : len(sources)]
        count_wait(sample, x_recv.at[x_slot(first, h, sources[0])])

    def tp_copy(src, dst, slot):
        return remote(src, dst, act_send.at[slot], act_recv.at[slot], t_peer)

    def y_act(src, dst, slot):
        return remote(src, dst, act_send.at[slot], act_recv.at[slot], y_peer)

    def y_start(places, parts=(0, 1)):
        for q in parts:
            for k in places:
                y_copy(k, q).start()

    y_start((0,), (0,))
    start(0)
    y_start((1,), (0,))
    y_start((0, 1), (1,))
    for k in range(chunks):
        for q in range(2):
            local_copy(k, q).start()

    own_columns = pl.ds(pl.multiple_of(tp * half_width, half_width), half_width)

    def squares(source, phase):
        def body(step, _):
            rows = pl.ds(pl.multiple_of(step * CHUNK_ROWS, CHUNK_ROWS), CHUNK_ROWS)
            total = None
            for tile in range(lane_tiles):
                value = source[rows, tile * LANES : (tile + 1) * LANES].astype(jnp.float32)
                total = value * value if total is None else total + value * value
            square_own[phase, rows, :] = total
            return 0

        lax.fori_loop(0, tokens // CHUNK_ROWS, body, 0)

    def square_copy(phase):
        return tp_copy(square_own.at[phase], square_got.at[phase], 9 + phase)

    def norm(source, phase, gain_ref, target):
        def body(step, _):
            rows = pl.ds(pl.multiple_of(step * CHUNK_ROWS, CHUNK_ROWS), CHUNK_ROWS)
            total = jnp.sum(square_own[phase, rows, :] + square_got[phase, rows, :], axis=1, keepdims=True)
            inverse = lax.rsqrt(total * (1.0 / width) + EPSILON)
            for tile in range(lane_tiles):
                value = source[rows, tile * LANES : (tile + 1) * LANES].astype(jnp.float32)
                gain = gain_ref[pl.ds(tp * lane_tiles + tile, 1), :]
                lanes = pl.ds(pl.multiple_of(tp * half_width + tile * LANES, LANES), LANES)
                target[y, rows, lanes] = (value * inverse * gain).astype(jnp.bfloat16)
            return 0

        lax.fori_loop(0, tokens // CHUNK_ROWS, body, 0)

    def block_copies(target, base):
        own = target.at[y, :, own_columns]
        theirs = target.at[1 - y, :, own_columns]
        return (
            tp_copy(own, own, base),
            y_act(own, own, base + 1),
            tp_copy(theirs, theirs, base + 2),
        )

    loads[0].wait()
    loads[1].wait()
    squares(stream_ref, 0)
    square_copy(0).start()
    for load in loads[2:]:
        load.wait()
    mine = pl.ds(pl.multiple_of(y * quarter, quarter), quarter)
    peers = pl.ds(pl.multiple_of((1 - y) * quarter, quarter), quarter)
    offset_send[...] = offset_ref[:, peers].astype(jnp.bfloat16)
    offsets[0] = offset_ref[:, mine].astype(jnp.bfloat16)
    square_copy(0).wait_recv()
    norm(stream_ref, 0, first_gain_ref, normed)
    first_tp, first_y, first_pass = block_copies(normed, 0)
    first_tp.start()
    offset_copy = y_act(offset_send, offsets.at[1], 3)

    y_start((2,))
    wide = jnp.exp(-jnp.abs(param_ref[...]))
    ratio = wide / (2.0 + wide)
    ratio_square = ratio * ratio
    log_sum = jnp.ones_like(ratio) * (1.0 / 17.0)
    for odd in (15.0, 13.0, 11.0, 9.0, 7.0, 5.0, 3.0, 1.0):
        log_sum = log_sum * ratio_square + 1.0 / odd
    rate_ref[...] = -DECAY_MULTIPLIER * (jnp.maximum(-param_ref[...], 0.0) + 2.0 * ratio * log_sum)

    size = decay_maps_ref.shape[1]
    per = LANES // size
    tiles = quarter // LANES
    maps[...] = jnp.zeros_like(maps)
    for tile in range(tiles):
        for index in range(per):
            place = y * (tiles * per) + tile * per + index
            span = slice(index * size, (index + 1) * size)
            maps[tile, span, index * size : (index + 1) * size] = decay_maps_ref[place]
            maps[tile, span, LANES + index * size : LANES + (index + 1) * size] = input_maps_ref[place]

    @pl.when(is_mid)
    def _():
        advance(0)
        first_y.start()
        advance(1)
        offset_copy.start()
        advance(2)
        y_start(range(3, last_raise))
        advance(3)

    @pl.when(is_end)
    def _():
        for place, (index, m) in enumerate(END_ORDER):
            relay(index, m)
            if place % 3 == 0:
                start_after(index)
            if place == 1:
                first_y.start()
            if place == 4:
                offset_copy.start()
            if place == 7:
                y_start(range(3, last_raise))
        start(STEADY + 1)

    first_y.wait_recv()
    first_pass.start()

    count_wait(weights.at[:, :, 0], local_sem.at[0])
    wait_y(0, 2)
    advance_for(is_mid, 4)
    wait_x(0, 2, None, every)
    first_tp.wait_recv()

    def project(which, token_block, *relays):
        def body(step, _):
            for role, *steps in relays:
                advance_at(step, role, *steps)
            matrix = weights[step // 2, step % 2].reshape(width, block)
            projected[which, step] = jnp.dot(
                normed[token_block], matrix, preferred_element_type=jnp.float32
            ).astype(jnp.bfloat16)
            return 0

        lax.fori_loop(0, 4, body, 0)

    reach = taps_ref.shape[0]

    def recur(which, *relays):
        def body(step, _):
            for role, *steps in relays:
                advance_at(step, role, *steps)
            rows = pl.ds(pl.multiple_of(step * SEQ_LEN, SEQ_LEN), SEQ_LEN)
            for tile in range(tiles):
                part, lane = tile * LANES // block, tile * LANES % block
                lanes = slice(lane, lane + LANES)
                taps = taps_ref[
                    :, pl.ds(pl.multiple_of(y * quarter + tile * LANES, LANES), LANES)
                ].astype(jnp.float32)
                values = projected[which, part, rows, lanes].astype(jnp.float32)
                filtered = taps[reach - 1 : reach] * values
                for back in range(1, reach):
                    tap = taps[reach - 1 - back : reach - back]
                    filtered = filtered + tap * shift_down(values, back, 0.0)
                conved = filtered.astype(jnp.bfloat16)
                logits = jnp.dot(conved, maps[tile], preferred_element_type=jnp.float32)
                offset = offsets[which, rows, tile * LANES : (tile + 1) * LANES].astype(jnp.float32)
                steps = 1.0 / (1.0 + jnp.exp(-logits))
                rate = rate_ref[pl.ds(y * tiles + tile, 1), :]
                log_decay = steps[:, :LANES] * rate + offset
                decay = jnp.exp(log_decay)
                twice = -2.0 * log_decay
                series = 1.0 + twice * (
                    -1 / 2
                    + twice
                    * (1 / 6 + twice * (-1 / 24 + twice * (1 / 120 + twice * (-1 / 720 + twice * (1 / 5040)))))
                )
                lost = jnp.where(twice < 0.35, twice * series, 1.0 - decay * decay)
                state = jnp.sqrt(lost) * steps[:, LANES:] * conved.astype(jnp.float32)
                span = 1
                while span < SEQ_LEN:
                    state = state + decay * shift_down(state, span, 0.0)
                    if span * 2 < SEQ_LEN:
                        decay = decay * shift_down(decay, span, 1.0)
                    span *= 2
                gate = projected[which, 2 + part, rows, lanes].astype(jnp.float32)
                gelu = 0.5 * gate * (1.0 + lax.erf(gate * 0.7071067811865476))
                mixed[which, rows, tile * LANES : (tile + 1) * LANES] = (state * gelu).astype(jnp.bfloat16)
            return 0

        lax.fori_loop(0, tokens // SEQ_LEN, body, 0)

    project(0, y, (is_end, 4))
    recur(0, (is_mid, 5, 1, 2))
    first_pass.wait_recv()
    project(1, 1 - y, (is_mid, 5, 3, 3))
    offset_copy.wait_recv()
    recur(1, (is_end, 5))


    @pl.when(is_mid)
    def _():
        skewed(up)

    wait_y(2, 3)
    wait_x(2, 3, None, every)

    def mix_out(which, *relays):
        def body(step, _):
            for role, *steps in relays:
                advance_at(step, role, *steps)

            def term(place):
                matrix = weights[2, :, place].reshape(quarter, block)
                return jnp.dot(mixed[which], matrix, preferred_element_type=jnp.float32).astype(jnp.bfloat16)

            lanes = pl.ds(pl.multiple_of(step * block, block), block)
            per_half = n_fs // 2
            passed[which, :, lanes] = term(per_half * (1 - tp) + step)
            kept[which, :, lanes] = term(per_half * tp + step)
            return 0

        lax.fori_loop(0, n_fs // 2, body, 0)

    def mix_copy(which):
        return tp_copy(passed.at[which], got.at[which], 4 + which)

    mix_out(1, (is_end, 6))
    mix_copy(1).start()
    mix_out(0)
    mix_copy(0).start()

    def add_peer(step, _):
        rows = pl.ds(pl.multiple_of(step * CHUNK_ROWS, CHUNK_ROWS), CHUNK_ROWS)
        mid_send[rows, :] = (
            kept[1, rows, :].astype(jnp.float32) + got[1, rows, :].astype(jnp.float32)
        ).astype(jnp.bfloat16)
        return 0

    mix_copy(1).wait_recv()
    lax.fori_loop(0, tokens // CHUNK_ROWS, add_peer, 0)
    mid_copy = y_act(mid_send, mid_got, 6)
    mid_copy.start()
    y_start(lowers, (0,))

    for index in range(1, raises + 1):
        advance_both(up + index)
    mix_copy(0).wait_recv()
    relay(up + raises + 1, 1)
    start_after(up + raises + 1)
    relay(up + raises + 1, 2)

    @pl.when(is_mid)
    def _():
        relay(up + raises, 3)

    mid_copy.wait_recv()

    def add_own(step, _):
        rows = pl.ds(pl.multiple_of(step * CHUNK_ROWS, CHUNK_ROWS), CHUNK_ROWS)
        total = None
        for tile in range(lane_tiles):
            lanes = slice(tile * LANES, (tile + 1) * LANES)
            update = kept[0, rows, lanes].astype(jnp.float32) + got[0, rows, lanes].astype(jnp.float32)
            update = update + mid_got[rows, lanes].astype(jnp.float32)
            value = (stream_ref[rows, lanes].astype(jnp.float32) + update).astype(jnp.bfloat16)
            middle[rows, lanes] = value
            value = value.astype(jnp.float32)
            total = value * value if total is None else total + value * value
        square_own[1, rows, :] = total
        return 0

    lax.fori_loop(0, tokens // CHUNK_ROWS, add_own, 0)
    square_copy(1).start()
    square_copy(1).wait_recv()
    norm(middle, 1, second_gain_ref, normed_mid)
    second_tp, second_y, second_pass = block_copies(normed_mid, 11)
    second_y.start()
    second_tp.start()

    @pl.when(is_end)
    def _():
        relay(up + raises + 1, 3)

    for index in range(2, raises):
        advance_both(up + raises + index)
    down = up + 2 * raises
    wait_y(3, last_raise)
    for k in range(3, last_raise):
        if k == last_raise - 1:
            advance_both(down)

            @pl.when(is_mid)
            def _():
                skewed(down + 1)

        wait_x(k, k + 1, None, every)

    def lift(which, token_block, *relays):
        def body(step, _):
            for role, *steps in relays:
                advance_at(step, role, *steps)
            matrix = weights[3 + step // 2, step % 2].reshape(width, block)
            total = jnp.dot(normed_mid[token_block], matrix, preferred_element_type=jnp.float32)
            lanes = pl.ds(pl.multiple_of(step * block, block), block)
            activity[which, :, lanes] = jnp.square(jnp.maximum(total, 0.0)).astype(jnp.bfloat16)
            return 0

        lax.fori_loop(0, 2 * raises, body, 0)

    second_tp.wait_recv()
    lift(0, y)

    @pl.when(is_mid)
    def _():
        skewed(down + 2)

    advance_for(is_end, down + 1)

    second_y.wait_recv()
    y_start(lowers, (1,))
    second_pass.start()
    second_pass.wait_recv()
    lift(1, 1 - y, (is_end, down + 2))

    for index in range(3, raises):
        advance(down + index)

    depth = raises * quarter

    def lower(h, m):
        place = 2 * plane(m) + (y if h == 0 else 1 - y)

        def body(which, _):
            matrix = weights[last_raise:chunks, :, place].reshape(depth, block)
            partial[m, h, which] = jnp.dot(
                activity[which], matrix, preferred_element_type=jnp.float32
            ).astype(jnp.bfloat16)
            return 0

        lax.fori_loop(0, 2, body, 0)

    def is_owner(m):
        return low if m < 2 else jnp.logical_not(low)

    def owner_copy(h, m):
        slot = 14 + 2 * (m % 2) + h
        return tp_copy(partial.at[m, h], partial_got.at[m % 2, h], slot)

    def last_copy(h, m):
        slot = 18 + 2 * (m % 2)
        return remote(
            last_send.at[m % 2, h],
            last_got.at[m % 2, 1 - h],
            act_send.at[slot + h],
            act_recv.at[slot + 1 - h],
            y_peer,
        )

    def pass_on(h, m):
        @pl.when(jnp.logical_not(is_owner(m)))
        def _():
            owner_copy(h, m).start()

    def finish(h, m):
        @pl.when(is_owner(m))
        def _():
            owner_copy(h, m).wait_recv()

            def body(step, _):
                rows = pl.ds(pl.multiple_of(step * CHUNK_ROWS, CHUNK_ROWS), CHUNK_ROWS)
                last_send[m % 2, h, rows, :] = (
                    partial[m, h, 1, rows, :].astype(jnp.float32)
                    + partial_got[m % 2, h, 1, rows, :].astype(jnp.float32)
                ).astype(jnp.bfloat16)
                return 0

            lax.fori_loop(0, tokens // CHUNK_ROWS, body, 0)
            last_copy(h, m).start()

    def lanes_of(half):
        return slice(half * (block // 2), (half + 1) * (block // 2))

    def last_part(half, which):
        lanes = lanes_of(half)
        return tp_copy(
            partial.at[1, 1, which, :, lanes],
            partial_got.at[1, 1, which, :, lanes],
            (17, 22, 23, 24)[2 * half + which],
        )

    def last_half(half):
        lanes = lanes_of(half)
        return remote(
            last_send.at[1, 1, :, lanes],
            last_got.at[1, 0, :, lanes],
            act_send.at[(21, 25)[half]],
            act_recv.at[(20, 25)[half]],
            y_peer,
        )

    def half_wait(first, last, half):
        sample = weights.at[first:last, 0, 0, :, lanes_of(0)]
        count_wait(sample, x_recv.at[x_slot(first, 1, 1, half)])

    def send_half(half):
        lanes = lanes_of(half)

        @pl.when(low)
        def _():
            last_part(half, 1).wait_recv()

            def body(step, _):
                rows = pl.ds(pl.multiple_of(step * CHUNK_ROWS, CHUNK_ROWS), CHUNK_ROWS)
                last_send[1, 1, rows, lanes] = (
                    partial[1, 1, 1, rows, lanes].astype(jnp.float32)
                    + partial_got[1, 1, 1, rows, lanes].astype(jnp.float32)
                ).astype(jnp.bfloat16)
                return 0

            lax.fori_loop(0, tokens // CHUNK_ROWS, body, 0)
            last_half(half).start()

    def store_half(half, which, value):
        partial[1, 1, which, :, lanes_of(half)] = value.astype(jnp.bfloat16)

        @pl.when(jnp.logical_not(low))
        def _():
            last_part(half, which).start()

    def lower_last():
        place = 2 * plane(1) + 1 - y
        split = (raises - 1) * quarter
        advance(near + 2 * raises - 1)
        half_wait(last_raise, chunks, 0)
        for which in (1, 0):
            matrix = weights[last_raise:chunks, :, place, :, lanes_of(0)].reshape(depth, block // 2)
            store_half(0, which, jnp.dot(activity[which], matrix, preferred_element_type=jnp.float32))
        send_half(0)
        half_wait(last_raise, chunks - 1, 1)

        def early(which, _):
            matrix = weights[last_raise : chunks - 1, :, place, :, lanes_of(1)].reshape(split, block // 2)
            total[which] = jnp.dot(activity[which, :, :split], matrix, preferred_element_type=jnp.float32)
            return 0

        lax.fori_loop(0, 2, early, 0)
        half_wait(chunks - 1, chunks, 1)
        for which in (1, 0):
            matrix = weights[chunks - 1, :, place, :, lanes_of(1)].reshape(quarter, block // 2)
            term = jnp.dot(activity[which, :, split:], matrix, preferred_element_type=jnp.float32)
            store_half(1, which, total[which] + term)
        send_half(1)

    def close(h, mm):
        owned = mm + 2 * (1 - low.astype(jnp.int32))
        if (h, mm) == (0, 1):

            @pl.when(low)
            def _():
                last_half(0).wait_recv()
                last_half(1).wait_recv()

            @pl.when(jnp.logical_not(low))
            def _():
                last_copy(1, 3).wait_recv()

        else:
            last_copy(1 - h, mm).wait_recv()
        place = 2 * ((z % 2 + mm) % 2) + (y if h == 0 else 1 - y)
        lanes = pl.ds(pl.multiple_of(place * block, block), block)

        def body(step, _):
            rows = pl.ds(pl.multiple_of(step * CHUNK_ROWS, CHUNK_ROWS), CHUNK_ROWS)
            update = (
                partial[owned, h, 0, rows, :].astype(jnp.float32)
                + partial_got[mm, h, 0, rows, :].astype(jnp.float32)
                + last_got[mm, h, rows, :].astype(jnp.float32)
            )
            out_ref[rows, lanes] = (middle[rows, lanes].astype(jnp.float32) + update).astype(jnp.bfloat16)
            return 0

        lax.fori_loop(0, tokens // CHUNK_ROWS, body, 0)

    order = [(0, m) for m in range(4)] + [(1, m) for m in (0, 2, 3, 1)]
    far, near = down + raises, down + 2 * raises

    def first_far(index):
        relay(index, 2)
        start_after(index)

    @pl.when(is_mid)
    def _():
        first_far(far)
        relay(far - 1, 3)
        first_far(far + 1)
        relay(far, 3)

    advance_for(is_end, far)
    wait_y(last_raise, chunks)
    wait_x(last_raise, chunks, 0, every)
    for index, (h, m) in enumerate(order):
        if index == 2:

            @pl.when(is_mid)
            def _():
                first_far(far + 2)
                relay(far + 1, 3)

        if index == 4:

            @pl.when(is_mid)
            def _():
                relay(far + 2, 3)

        if index in (2, 4):
            advance_for(is_end, far + index // 2)
        if (h, m) == (1, 1):
            lower_last()
            continue
        if index >= 5:
            for step in range(raises) if index == 5 else range(raises, 2 * raises - 1):
                advance(near + step)
        if h == 1 and m:
            wait_x(last_raise, chunks, 1, (m,))
        lower(h, m)
        pass_on(h, m)
        if index and index < 5:
            finish(*order[index - 1])
        if index >= 4:
            finish(h, m)
    close(1, 0)
    close(0, 0)

    @pl.when(low)
    def _():
        last_part(0, 0).wait_recv()
        last_part(1, 0).wait_recv()

    close(1, 1)
    close(0, 1)

    count_wait(weights.at[:, :, 0], y_send.at[0])
    count_wait(weights.at[:, 0, 0:6], x_send.at[0])
    count_wait(weights.at[:, 0, 0:4], z_send.at[0])

    @pl.when(is_mid)
    def _():
        count_wait(weights.at[:, 0, 0:4], z_send.at[0])

    for copy in (first_tp, first_y, first_pass, second_tp, second_y, second_pass, offset_copy, mid_copy):
        copy.wait_send()
    for phase in range(2):
        square_copy(phase).wait_send()
        mix_copy(phase).wait_send()
    for h, m in order[:-1]:

        @pl.when(is_owner(m))
        def _():
            last_copy(h, m).wait_send()

        @pl.when(jnp.logical_not(is_owner(m)))
        def _():
            owner_copy(h, m).wait_send()

    @pl.when(low)
    def _():
        for half in range(2):
            last_half(half).wait_send()

    @pl.when(jnp.logical_not(low))
    def _():
        for half in range(2):
            for which in range(2):
                last_part(half, which).wait_send()


def whole_layer(
    stream,
    recurrent_norm_gain,
    feedforward_norm_gain,
    recurrent_input_weight,
    output_gate_weight,
    causal_filter_weight,
    decay_gate_matrix,
    input_gate_matrix,
    channel_decay_param,
    token_decay_offset,
    recurrent_output_weight,
    up_projection_weight,
    down_projection_weight,
):
    tokens, half_width = stream.shape
    width = 2 * half_width
    quarter = half_width // 2
    block, n_fs = quarter // 2, 8
    raises = up_projection_weight.shape[1] // half_width
    chunks = 3 + 2 * raises
    depth = raises * quarter
    tiles = quarter // LANES
    half_type, full_type = jnp.bfloat16, jnp.float32
    vmem = pl.BlockSpec(memory_space=pltpu.VMEM)
    anywhere = pl.BlockSpec(memory_space=pl.ANY)
    dma = pltpu.SemaphoreType.DMA
    return pl.pallas_call(
        whole_kernel,
        out_shape=jax.ShapeDtypeStruct((tokens, half_width), half_type),
        in_specs=[anywhere] * 13,
        out_specs=vmem,
        scratch_shapes=[
            pltpu.VMEM((tokens, half_width), half_type),
            pltpu.VMEM((tokens, half_width), full_type),
            pltpu.VMEM((width // LANES, LANES), full_type),
            pltpu.VMEM((width // LANES, LANES), full_type),
            pltpu.VMEM(causal_filter_weight.shape, half_type),
            pltpu.VMEM(decay_gate_matrix.shape, half_type),
            pltpu.VMEM(input_gate_matrix.shape, half_type),
            pltpu.VMEM((half_width // LANES, LANES), full_type),
            pltpu.VMEM((half_width // LANES, LANES), full_type),
            pltpu.VMEM((chunks, 2, n_fs, block, block), half_type),
            pltpu.VMEM((2, tokens, width), half_type),
            pltpu.VMEM((2, tokens, width), half_type),
            pltpu.VMEM((2, tokens, LANES), full_type),
            pltpu.VMEM((2, tokens, LANES), full_type),
            pltpu.VMEM((2, 4, tokens, block), half_type),
            pltpu.VMEM((2, tokens, quarter), half_type),
            pltpu.VMEM((2, tokens, quarter), half_type),
            pltpu.VMEM((tokens, quarter), half_type),
            pltpu.VMEM((tiles, LANES, 2 * LANES), half_type),
            pltpu.VMEM((2, tokens, half_width), half_type),
            pltpu.VMEM((2, tokens, half_width), half_type),
            pltpu.VMEM((2, tokens, half_width), half_type),
            pltpu.VMEM((tokens, half_width), half_type),
            pltpu.VMEM((tokens, half_width), half_type),
            pltpu.VMEM((tokens, half_width), half_type),
            pltpu.VMEM((2, tokens, depth), half_type),
            pltpu.VMEM((4, 2, 2, tokens, block), half_type),
            pltpu.VMEM((2, 2, 2, tokens, block), half_type),
            pltpu.VMEM((2, tokens, block // 2), full_type),
            pltpu.VMEM((2, 2, tokens, block), half_type),
            pltpu.VMEM((2, 2, tokens, block), half_type),
            dma((1,)),
            dma((1,)),
            dma((chunks + 4,)),
            dma((1,)),
            dma((chunks, 2, 4)),
            dma((1,)),
            dma((raises + 8,)),
            dma((26,)),
            dma((26,)),
            dma((8,)),
        ],
        compiler_params=pltpu.CompilerParams(
            collective_id=0, has_side_effects=True, vmem_limit_bytes=67043328
        ),
        name="whole_layer",
    )(
        stream,
        token_decay_offset,
        recurrent_norm_gain.reshape(-1, LANES),
        feedforward_norm_gain.reshape(-1, LANES),
        causal_filter_weight,
        decay_gate_matrix,
        input_gate_matrix,
        channel_decay_param.reshape(-1, LANES),
        recurrent_input_weight,
        output_gate_weight,
        recurrent_output_weight,
        up_projection_weight,
        down_projection_weight,
    )


def fits_whole(sizes, stream, up_projection_weight, decay_gate_matrix):
    tokens, half_width = stream.shape
    return (
        sizes == (2, 8, 2)
        and half_width % (8 * LANES) == 0
        and tokens % (4 * SEQ_LEN) == 0
        and up_projection_weight.shape[1] % half_width == 0
        and up_projection_weight.shape[1] // half_width >= 3
        and LANES % decay_gate_matrix.shape[1] == 0
    )


def solution(mesh):
    in_specs = (
        P(("rep", "fs"), "tp"),
        P(),
        P(),
        P("fs", "tp"),
        P("fs", "tp"),
        P(None, "tp"),
        P("tp", None, None),
        P("tp", None, None),
        P("tp"),
        P(("rep", "fs"), "tp"),
        P("tp", "fs"),
        P("fs", "tp"),
        P("tp", "fs"),
    )
    out_specs = P(("rep", "fs"), "tp")
    sizes = tuple(mesh.shape[axis] for axis in ("rep", "fs", "tp"))

    def body(*args):
        if fits_whole(sizes, args[0], args[11], args[6]):
            return whole_layer(*args)
        return shards(sizes, *args)

    return jax.shard_map(
        body, mesh=mesh, in_specs=in_specs, out_specs=out_specs, check_vma=False
    )
```

```python
import functools

import jax
import jax.numpy as jnp
from jax import lax
from jax.experimental import pallas as pl
from jax.experimental.pallas import tpu as pltpu
from jax.sharding import PartitionSpec as P


SEQ_LEN = 128
EPSILON = 1e-06
DECAY_MULTIPLIER = 8.0
LANES = 128


def half(values, which, axis):
    first, second = jnp.split(values, 2, axis)
    return jnp.where(which == 0, first, second)


def gather_shard(shard, ids, sizes):
    rep, fs, _ = ids
    _, n_fs, _ = sizes
    own, for_peer = shard
    hops = n_fs // 2
    place, side = fs // 2, fs % 2
    from_peer = lax.ppermute(for_peer, "fs", [(i, i ^ 1) for i in range(n_fs)])
    start = jnp.where(side == rep, own, from_peer)
    up = [(i, (i + 2) % n_fs) for i in range(n_fs)]
    down = [(i, (i + n_fs - 2) % n_fs) for i in range(n_fs)]
    pieces, places = [own, from_peer], [fs, fs ^ 1]
    below = above = start
    for step in range(1, hops):
        if step % 2:
            below = mine = lax.ppermute(below, "fs", up)
            base = 2 * ((place + hops - (step + 1) // 2) % hops)
        else:
            above = mine = lax.ppermute(above, "fs", down)
            base = 2 * ((place + step // 2) % hops)
        pieces += [mine, lax.ppermute(mine, "rep", [(0, 1), (1, 0)])]
        places += [base + rep, base + 1 - rep]
    return pieces, jnp.stack(places).astype(jnp.int32)


def gather_features(values, tp, n_tp):
    if n_tp != 2:
        return lax.all_gather(values, "tp", axis=1, tiled=True)
    other = lax.ppermute(values, "tp", [(0, 1), (1, 0)])
    return jnp.where(
        tp == 0, jnp.concatenate([values, other], 1), jnp.concatenate([other, values], 1)
    )


def sum_features(parts, tp, n_tp):
    total = lax.dynamic_index_in_dim(parts, tp, 0, False).astype(jnp.float32)
    for shift in range(1, n_tp):
        piece = lax.dynamic_index_in_dim(parts, (tp + shift) % n_tp, 0, False)
        got = lax.ppermute(piece, "tp", [(i, (i + shift) % n_tp) for i in range(n_tp)])
        total = total + got.astype(jnp.float32)
    return total.astype(jnp.bfloat16)


def norm_rows(values, gain):
    widened = values.astype(jnp.float32)
    inverse = lax.rsqrt(jnp.mean(widened * widened, axis=-1, keepdims=True) + EPSILON)
    return (widened * inverse * gain).astype(jnp.bfloat16)


ROWS = 256
CHUNK = 512


def depth_kernel(squared, places_ref, x_ref, *refs):
    *pieces, out_ref = refs
    depth, width = pieces[0].shape
    chunk = min(CHUNK, width)
    for lower in range(0, width, chunk):
        cols = slice(lower, lower + chunk)
        total = None
        for index, piece in enumerate(pieces):
            place = pl.multiple_of(places_ref[index] * depth, depth)
            term = jnp.dot(
                x_ref[:, pl.ds(place, depth)], piece[:, cols], preferred_element_type=jnp.float32
            )
            total = term if total is None else total + term
        if squared:
            total = jnp.square(jnp.maximum(total, 0.0))
        out_ref[:, cols] = total.astype(jnp.bfloat16)


def depth_matmul(x, gathered, squared=False):
    pieces, places = gathered
    tokens, width = x.shape
    shape = pieces[0].shape
    return pl.pallas_call(
        functools.partial(depth_kernel, squared),
        grid_spec=pltpu.PrefetchScalarGridSpec(
            num_scalar_prefetch=1,
            grid=(tokens // ROWS,),
            in_specs=[pl.BlockSpec((ROWS, width), lambda m, _: (m, 0))]
            + [pl.BlockSpec(shape, lambda m, _: (0, 0))] * len(pieces),
            out_specs=pl.BlockSpec((ROWS, shape[1]), lambda m, _: (m, 0)),
        ),
        out_shape=jax.ShapeDtypeStruct((tokens, shape[1]), jnp.bfloat16),
        cost_estimate=pl.CostEstimate(
            flops=2 * tokens * width * shape[1],
            bytes_accessed=2 * (tokens * width + (tokens + width) * shape[1]),
            transcendentals=0,
        ),
        name="depth_matmul",
    )(places, x, *pieces)


def columns_kernel(per, places_ref, x_ref, *refs):
    *pieces, out_ref = refs
    cols = pieces[0].shape[1]
    for index, piece in enumerate(pieces):
        place = places_ref[index]
        lower = pl.multiple_of((place % per) * cols, cols)
        out_ref[place // per, :, pl.ds(lower, cols)] = jnp.dot(
            x_ref[...], piece[...], preferred_element_type=jnp.float32
        ).astype(jnp.bfloat16)


def columns_matmul(x, gathered, n_tp, first, tokens):
    pieces, places = gathered
    depth, cols = pieces[0].shape
    per = len(pieces) // n_tp
    skip = first // ROWS
    return pl.pallas_call(
        functools.partial(columns_kernel, per),
        grid_spec=pltpu.PrefetchScalarGridSpec(
            num_scalar_prefetch=1,
            grid=(tokens // ROWS,),
            in_specs=[pl.BlockSpec((ROWS, depth), lambda m, _: (m + skip, 0))]
            + [pl.BlockSpec((depth, cols), lambda m, _: (0, 0))] * len(pieces),
            out_specs=pl.BlockSpec((n_tp, ROWS, per * cols), lambda m, _: (0, m, 0)),
        ),
        out_shape=jax.ShapeDtypeStruct((n_tp, tokens, per * cols), jnp.bfloat16),
        cost_estimate=pl.CostEstimate(
            flops=2 * tokens * depth * cols * len(pieces),
            bytes_accessed=2 * (tokens * depth + len(pieces) * cols * (depth + tokens)),
            transcendentals=0,
        ),
        name="columns_matmul",
    )(places, x, *pieces)


def shift_down(values, amount, fill):
    index = lax.broadcasted_iota(jnp.int32, values.shape, 0)
    return jnp.where(index < amount, fill, pltpu.roll(values, amount, 0))


def recurrence_kernel(
    side_ref, value_ref, gate_ref, own_ref, peer_ref, taps_ref, maps_ref, rate_ref, out_ref
):
    rows, channels = value_ref.shape
    reach = taps_ref.shape[0]
    per = LANES // maps_ref.shape[1]
    is_own = pl.program_id(0) < pl.num_programs(0) // 2
    for tile in range(channels // LANES):
        cols = slice(tile * LANES, (tile + 1) * LANES)
        values = value_ref[:, cols].astype(jnp.float32)
        filtered = taps_ref[reach - 1 : reach, cols] * values
        for back in range(1, reach):
            tap = taps_ref[reach - 1 - back : reach - back, cols]
            filtered = filtered + tap * shift_down(values, back, 0.0)
        conved = filtered.astype(jnp.bfloat16)
        maps = maps_ref[tile * per : (tile + 1) * per].reshape(LANES, 2 * LANES)
        logits = jnp.dot(conved, maps, preferred_element_type=jnp.float32)
        offset = jnp.where(is_own, own_ref[:, cols], peer_ref[:, cols].astype(jnp.float32))
        steps = 1.0 / (1.0 + jnp.exp(-logits))
        log_decay = steps[:, :LANES] * rate_ref[:, cols] + offset
        decay = jnp.exp(log_decay)
        y = -2.0 * log_decay
        series = 1.0 + y * (
            -1 / 2 + y * (1 / 6 + y * (-1 / 24 + y * (1 / 120 + y * (-1 / 720 + y * (1 / 5040)))))
        )
        lost = jnp.where(y < 0.35, y * series, 1.0 - decay * decay)
        state = jnp.sqrt(lost) * steps[:, LANES:] * conved.astype(jnp.float32)
        span = 1
        while span < rows:
            state = state + decay * shift_down(state, span, 0.0)
            if span * 2 < rows:
                decay = decay * shift_down(decay, span, 1.0)
            span *= 2
        gate = gate_ref[:, cols].astype(jnp.float32)
        gelu = 0.5 * gate * (1.0 + lax.erf(gate * 0.7071067811865476))
        out_ref[:, cols] = (state * gelu).astype(jnp.bfloat16)


def recurrence(projected, offset_own, offset_peer, taps, decay_maps, input_maps, rate, side):
    tokens = projected.shape[0]
    channels = offset_peer.shape[1]
    blocks, size, _ = decay_maps.shape
    per = LANES // size
    block = jnp.arange(blocks)[:, None, None] % per
    group = jnp.arange(LANES)[None, None, :] // size

    def diagonal(maps):
        return jnp.where(block == group, jnp.tile(maps, (1, 1, per)), 0)

    maps = jnp.concatenate([diagonal(decay_maps), diagonal(input_maps)], 2)
    sequences = tokens // SEQ_LEN
    own = sequences // 2
    return pl.pallas_call(
        recurrence_kernel,
        grid_spec=pltpu.PrefetchScalarGridSpec(
            num_scalar_prefetch=1,
            grid=(sequences,),
            in_specs=[
                pl.BlockSpec((SEQ_LEN, channels), lambda s, side: (s, 0)),
                pl.BlockSpec((SEQ_LEN, channels), lambda s, side: (s, 1)),
                pl.BlockSpec(
                    (SEQ_LEN, channels), lambda s, side: (jnp.minimum(s, own - 1), side[0])
                ),
                pl.BlockSpec((SEQ_LEN, channels), lambda s, side: (jnp.maximum(s - own, 0), 0)),
                pl.BlockSpec((taps.shape[0], channels), lambda s, side: (0, side[0])),
                pl.BlockSpec((blocks // 2, size, 2 * LANES), lambda s, side: (side[0], 0, 0)),
                pl.BlockSpec((1, channels), lambda s, side: (0, side[0])),
            ],
            out_specs=pl.BlockSpec((SEQ_LEN, channels), lambda s, side: (s, 0)),
        ),
        out_shape=jax.ShapeDtypeStruct((tokens, channels), jnp.bfloat16),
        cost_estimate=pl.CostEstimate(
            flops=tokens * channels * 700,
            bytes_accessed=tokens * channels * 10,
            transcendentals=tokens * channels * 6,
        ),
        name="recurrence",
    )(
        side.astype(jnp.int32)[None],
        projected,
        projected,
        offset_own,
        offset_peer,
        taps.astype(jnp.float32),
        maps,
        rate[None, :],
    )


def shards(
    sizes,
    stream,
    recurrent_norm_gain,
    feedforward_norm_gain,
    recurrent_input_weight,
    output_gate_weight,
    causal_filter_weight,
    decay_gate_matrix,
    input_gate_matrix,
    channel_decay_param,
    token_decay_offset,
    recurrent_output_weight,
    up_projection_weight,
    down_projection_weight,
):
    _, n_fs, n_tp = sizes
    ids = lax.axis_index("rep"), lax.axis_index("fs"), lax.axis_index("tp")
    _, fs, tp = ids
    side = fs % 2
    pairs = [(i, i ^ 1) for i in range(n_fs)]
    tokens = stream.shape[0]

    def halves(weight, axis):
        return half(weight, side, axis), half(weight, 1 - side, axis)

    def to_peer(values):
        return lax.ppermute(values, "fs", pairs)

    value_own, value_peer = halves(recurrent_input_weight, 1)
    gate_own, gate_peer = halves(output_gate_weight, 1)
    entry = (
        jnp.concatenate([value_own, gate_own], 1),
        jnp.concatenate([value_peer, gate_peer], 1),
    )
    entry_full = gather_shard(entry, ids, sizes)
    stream_peer = to_peer(stream)
    offset_peer = to_peer(half(token_decay_offset, 1 - side, 1).astype(jnp.bfloat16))
    output_full = gather_shard(halves(recurrent_output_weight, 0), ids, sizes)
    expand_full = gather_shard(halves(up_projection_weight, 1), ids, sizes)
    contract_full = gather_shard(halves(down_projection_weight, 0), ids, sizes)

    own_pair = jnp.concatenate([stream, stream_peer], 0)
    whole = gather_features(own_pair, tp, n_tp)
    normed = norm_rows(whole, recurrent_norm_gain)
    projected = depth_matmul(normed, entry_full)
    mixed = recurrence(
        projected,
        token_decay_offset,
        offset_peer,
        causal_filter_weight,
        decay_gate_matrix,
        input_gate_matrix,
        -DECAY_MULTIPLIER * jax.nn.softplus(-channel_decay_param),
        side,
    )
    mixer_terms = columns_matmul(mixed, output_full, n_tp, 0, 2 * tokens)
    mixer_chip = sum_features(mixer_terms, tp, n_tp)
    got_own = to_peer(mixer_chip[tokens:])
    got_peer = to_peer(mixer_chip[:tokens])
    update = mixer_chip.astype(jnp.float32) + jnp.concatenate([got_own, got_peer], 0).astype(
        jnp.float32
    )
    middle = (own_pair.astype(jnp.float32) + update).astype(jnp.bfloat16)
    normed_mid = norm_rows(gather_features(middle, tp, n_tp), feedforward_norm_gain)
    activity = depth_matmul(normed_mid, expand_full, squared=True)
    peer_terms = columns_matmul(activity, contract_full, n_tp, tokens, tokens)
    got = to_peer(sum_features(peer_terms, tp, n_tp))
    own_terms = columns_matmul(activity, contract_full, n_tp, 0, tokens)
    own_chip = sum_features(own_terms, tp, n_tp)
    channel_sum = own_chip.astype(jnp.float32) + got.astype(jnp.float32)
    return (middle[:tokens].astype(jnp.float32) + channel_sum).astype(jnp.bfloat16)


MESH = pl.DeviceIdType.MESH
CHUNK_ROWS = 128
AHEAD = (1, 1, 1, 1, 2, 3)
STEADY = 4
LEAD = 1
END_ORDER = (
    (0, 1), (0, 2), (0, 3), (1, 2), (1, 1), (1, 3), (2, 2), (2, 1), (2, 3), (3, 2), (3, 1), (3, 3),
)


def whole_kernel(
    stream_hbm,
    offset_hbm,
    first_gain_hbm,
    second_gain_hbm,
    taps_hbm,
    decay_maps_hbm,
    input_maps_hbm,
    param_hbm,
    value_hbm,
    gate_hbm,
    output_hbm,
    raise_hbm,
    lower_hbm,
    out_ref,
    stream_ref,
    offset_ref,
    first_gain_ref,
    second_gain_ref,
    taps_ref,
    decay_maps_ref,
    input_maps_ref,
    param_ref,
    rate_ref,
    weights,
    normed,
    normed_mid,
    square_own,
    square_got,
    projected,
    mixed,
    offsets,
    offset_send,
    maps,
    kept,
    passed,
    got,
    mid_send,
    mid_got,
    middle,
    activity,
    partial,
    partial_got,
    total,
    last_send,
    last_got,
    local_sem,
    y_send,
    y_recv,
    z_send,
    z_recv,
    x_send,
    x_recv,
    act_send,
    act_recv,
    load_sem,
):
    rep, fs, tp = lax.axis_index("rep"), lax.axis_index("fs"), lax.axis_index("tp")
    z, y = fs // 2, fs % 2
    tokens, half_width = stream_ref.shape
    width = 2 * half_width
    chunks, _, n_fs, block, _ = weights.shape
    quarter = half_width // 2
    lane_tiles = half_width // LANES
    raises = (chunks - 3) // 2
    last_raise = 3 + raises
    lowers = range(last_raise, chunks)
    is_mid = jnp.logical_or(z == 1, z == 2)
    is_end = jnp.logical_not(is_mid)
    low = (z // 2) == tp

    def plane(m):
        return 2 * ((z // 2 + m // 2) % 2) + (z % 2 + m % 2) % 2

    x_peer = (1 - rep, fs, tp)
    y_peer = (rep, 2 * z + 1 - y, tp)
    t_peer = (rep, fs, 1 - tp)

    def z_peer(m):
        return (rep, 2 * plane(m) + y, tp)

    places = (
        (stream_hbm, stream_ref),
        (first_gain_hbm, first_gain_ref),
        (offset_hbm, offset_ref),
        (second_gain_hbm, second_gain_ref),
        (taps_hbm, taps_ref),
        (decay_maps_hbm, decay_maps_ref),
        (input_maps_hbm, input_maps_ref),
        (param_hbm, param_ref),
    )
    loads = [
        pltpu.make_async_copy(source, target, load_sem.at[index])
        for index, (source, target) in enumerate(places)
    ]
    for load in loads:
        load.start()

    barrier = pltpu.get_barrier_semaphore()
    for peer in (x_peer, y_peer, t_peer, z_peer(1), z_peer(2), z_peer(3)):
        pl.semaphore_signal(barrier, inc=1, device_id=peer, device_id_type=MESH)
    pl.semaphore_wait(barrier, 6)

    def remote(src, dst, send, recv, peer):
        return pltpu.make_async_remote_copy(
            src_ref=src, dst_ref=dst, send_sem=send, recv_sem=recv, device_id=peer, device_id_type=MESH
        )

    def shard_block(k, side, part):
        if k < 2 or 3 <= k < 3 + raises:
            ref = (value_hbm, gate_hbm)[k] if k < 2 else raise_hbm
            first = 0 if k < 2 else (k - 3) * quarter
            span = ref.shape[1] // 2
            start = pl.multiple_of(side * span + first + part * block, block)
            return ref.at[:, pl.ds(start, block)]
        ref = output_hbm if k == 2 else lower_hbm
        first = 0 if k == 2 else (k - 3 - raises) * quarter
        span = ref.shape[0] // 2
        start = pl.multiple_of(side * span + first + part * block, block)
        return ref.at[pl.ds(start, block), :]

    def part_of(q):
        return rep if q == 0 else 1 - rep

    def local_copy(k, q):
        part = part_of(q)
        return pltpu.make_async_copy(
            shard_block(k, y, part), weights.at[k, part, fs], local_sem.at[0]
        )

    def group_of(k):
        return 0 if k < 2 else 1 if k == 2 else 2 if k < last_raise else 3

    def y_slot(k, q):
        return k if q == 0 else chunks + group_of(k)

    def x_slot(k, h, m, half=None):
        if k < last_raise:
            return group_of(k) if k < 3 else k - 1
        if half is not None:
            return 5 + raises + (0 if half == 0 else 1 if k < chunks - 1 else 2)
        return 2 + raises + (0 if h == 0 else m - 1)

    def count_wait(ref, sem):
        pltpu.make_async_copy(ref, ref, sem).wait()

    def y_copy(k, q):
        part = part_of(q)
        return remote(
            shard_block(k, 1 - y, part), weights.at[k, part, fs], y_send.at[0], y_recv.at[y_slot(k, q)], y_peer
        )

    def cut(place, k, half):
        if half is None:
            return weights.at[k, rep, place]
        return weights.at[k, rep, place, :, half * (block // 2) : (half + 1) * (block // 2)]

    def z_copy(k, h, m, half=None):
        spot = cut(fs if h == 0 else 2 * z + 1 - y, k, half)
        src = shard_block(k, y, rep) if h == 0 else spot
        slot = 6 * chunks + k - last_raise if half else 6 * k + 3 * h + m - 1
        return remote(src, spot, z_send.at[0], z_recv.at[slot], z_peer(m))

    def z_relay(k, h):
        spot = weights.at[k, rep, 2 * plane(2) + (y if h == 0 else 1 - y)]
        return remote(spot, spot, z_send.at[0], z_recv.at[6 * k + 3 * h + 2], z_peer(1))

    def x_copy(k, h, m, half=None):
        spot = cut(2 * plane(m) + (y if h == 0 else 1 - y), k, half)
        return remote(spot, spot, x_send.at[0], x_recv.at[x_slot(k, h, m, half)], x_peer)

    every = (2, 3, 1)
    up = 6
    events = [(k, h, every, None) for k, h in ((0, 0), (1, 0), (0, 1), (1, 1), (2, 0), (2, 1))]
    events += [(k, h, every, None) for h in range(2) for k in range(3, last_raise)]
    events += [(k, 0, every, None) for k in lowers]
    events += [(k, 1, (2, 3), None) for k in lowers]
    events += [(k, 1, (1,), half) for half in range(2) for k in lowers]

    def start_after(index):
        def reach_of(place):
            return place + AHEAD[min(place, len(AHEAD) - 1)] if place >= 0 else 0

        for later in range(reach_of(index - 1) + 1, reach_of(index) + 1):
            if later == STEADY + 1:

                @pl.when(is_mid)
                def _():
                    start(STEADY + 1)

            else:
                start(later)

    def start(index):
        if index >= len(events):
            return
        k, h, sources, half = events[index]
        if h == 1 and 2 in sources:
            y_copy(k, 0).wait_recv()
        for m in sources:
            if m == 1 and index >= 1:

                @pl.when(is_end)
                def _():
                    z_copy(k, h, 1, half).start()

            elif m < 3:
                z_copy(k, h, m).start()
            else:

                @pl.when(is_mid)
                def _():
                    z_copy(k, h, 3).start()

    def relay(index, m):
        k, h, _, half = events[index]
        z_copy(k, h, m, half).wait_recv()
        x_copy(k, h, m, half).start()

        @pl.when(jnp.logical_and(is_mid, m == 2))
        def _():
            z_relay(k, h).start()
            lead = index + (1 if index < STEADY else LEAD)
            for place in (lead,):
                next_k, next_h, next_sources, _ = events[min(place, len(events) - 1)]
                if next_sources == every:
                    z_copy(next_k, next_h, 1).start()
            far_step = index - up - 3 * raises
            if far_step == raises - 2:
                z_copy(last_raise, 1, 1, 0).start()
            if far_step == raises - 1:
                for later_k in range(last_raise + 1, chunks):
                    z_copy(later_k, 1, 1, 0).start()
                for later_k in lowers:
                    z_copy(later_k, 1, 1, 1).start()

    def advance(index):
        for place, m in enumerate(sorted(events[index][2])):
            relay(index, m)
            if place == 0:
                start_after(index)

    def skewed(index):
        relay(index, 1)
        start_after(index)
        relay(index, 2)
        if index > up:
            relay(index - 1, 3)

    def advance_both(index):
        @pl.when(is_mid)
        def _():
            skewed(index)

        @pl.when(is_end)
        def _():
            advance(index)

    def advance_for(role, index):
        @pl.when(role)
        def _():
            advance(index)

    def advance_at(step, role, index, first=1, last=3):
        @pl.when(jnp.logical_and(role, jnp.logical_and(step + 1 >= first, step + 1 <= last)))
        def _():
            relay(index, step + 1)

        if first == 1:

            @pl.when(jnp.logical_and(role, step == 0))
            def _():
                start_after(index)

    def wait_y(first, last):
        count_wait(weights.at[first:last, 0, 0], y_recv.at[y_slot(first, 1)])

    def wait_x(first, last, h, sources):
        parts = 1 if h is not None else 2
        sample = weights.at[first:last, 0:parts, 0 : len(sources)]
        count_wait(sample, x_recv.at[x_slot(first, h, sources[0])])

    def tp_copy(src, dst, slot):
        return remote(src, dst, act_send.at[slot], act_recv.at[slot], t_peer)

    def y_act(src, dst, slot):
        return remote(src, dst, act_send.at[slot], act_recv.at[slot], y_peer)

    def y_start(places, parts=(0, 1)):
        for q in parts:
            for k in places:
                y_copy(k, q).start()

    y_start((0,), (0,))
    start(0)
    y_start((1,), (0,))
    y_start((0, 1), (1,))
    for k in range(chunks):
        for q in range(2):
            local_copy(k, q).start()

    own_columns = pl.ds(pl.multiple_of(tp * half_width, half_width), half_width)

    def squares(source, phase):
        def body(step, _):
            rows = pl.ds(pl.multiple_of(step * CHUNK_ROWS, CHUNK_ROWS), CHUNK_ROWS)
            total = None
            for tile in range(lane_tiles):
                value = source[rows, tile * LANES : (tile + 1) * LANES].astype(jnp.float32)
                total = value * value if total is None else total + value * value
            square_own[phase, rows, :] = total
            return 0

        lax.fori_loop(0, tokens // CHUNK_ROWS, body, 0)

    def square_copy(phase):
        return tp_copy(square_own.at[phase], square_got.at[phase], 9 + phase)

    def norm(source, phase, gain_ref, target):
        def body(step, _):
            rows = pl.ds(pl.multiple_of(step * CHUNK_ROWS, CHUNK_ROWS), CHUNK_ROWS)
            total = jnp.sum(square_own[phase, rows, :] + square_got[phase, rows, :], axis=1, keepdims=True)
            inverse = lax.rsqrt(total * (1.0 / width) + EPSILON)
            for tile in range(lane_tiles):
                value = source[rows, tile * LANES : (tile + 1) * LANES].astype(jnp.float32)
                gain = gain_ref[pl.ds(tp * lane_tiles + tile, 1), :]
                lanes = pl.ds(pl.multiple_of(tp * half_width + tile * LANES, LANES), LANES)
                target[y, rows, lanes] = (value * inverse * gain).astype(jnp.bfloat16)
            return 0

        lax.fori_loop(0, tokens // CHUNK_ROWS, body, 0)

    def block_copies(target, base):
        own = target.at[y, :, own_columns]
        theirs = target.at[1 - y, :, own_columns]
        return (
            tp_copy(own, own, base),
            y_act(own, own, base + 1),
            tp_copy(theirs, theirs, base + 2),
        )

    loads[0].wait()
    loads[1].wait()
    squares(stream_ref, 0)
    square_copy(0).start()
    for load in loads[2:]:
        load.wait()
    mine = pl.ds(pl.multiple_of(y * quarter, quarter), quarter)
    peers = pl.ds(pl.multiple_of((1 - y) * quarter, quarter), quarter)
    offset_send[...] = offset_ref[:, peers].astype(jnp.bfloat16)
    offsets[0] = offset_ref[:, mine].astype(jnp.bfloat16)
    square_copy(0).wait_recv()
    norm(stream_ref, 0, first_gain_ref, normed)
    first_tp, first_y, first_pass = block_copies(normed, 0)
    first_tp.start()
    offset_copy = y_act(offset_send, offsets.at[1], 3)

    y_start((2,))
    wide = jnp.exp(-jnp.abs(param_ref[...]))
    ratio = wide / (2.0 + wide)
    ratio_square = ratio * ratio
    log_sum = jnp.ones_like(ratio) * (1.0 / 17.0)
    for odd in (15.0, 13.0, 11.0, 9.0, 7.0, 5.0, 3.0, 1.0):
        log_sum = log_sum * ratio_square + 1.0 / odd
    rate_ref[...] = -DECAY_MULTIPLIER * (jnp.maximum(-param_ref[...], 0.0) + 2.0 * ratio * log_sum)

    size = decay_maps_ref.shape[1]
    per = LANES // size
    tiles = quarter // LANES
    maps[...] = jnp.zeros_like(maps)
    for tile in range(tiles):
        for index in range(per):
            place = y * (tiles * per) + tile * per + index
            span = slice(index * size, (index + 1) * size)
            maps[tile, span, index * size : (index + 1) * size] = decay_maps_ref[place]
            maps[tile, span, LANES + index * size : LANES + (index + 1) * size] = input_maps_ref[place]

    @pl.when(is_mid)
    def _():
        advance(0)
        first_y.start()
        advance(1)
        offset_copy.start()
        advance(2)
        y_start(range(3, last_raise))
        advance(3)

    @pl.when(is_end)
    def _():
        for place, (index, m) in enumerate(END_ORDER):
            relay(index, m)
            if place % 3 == 0:
                start_after(index)
            if place == 1:
                first_y.start()
            if place == 4:
                offset_copy.start()
            if place == 7:
                y_start(range(3, last_raise))
        start(STEADY + 1)

    first_y.wait_recv()
    first_pass.start()

    count_wait(weights.at[:, :, 0], local_sem.at[0])
    wait_y(0, 2)
    advance_for(is_mid, 4)
    wait_x(0, 2, None, every)
    first_tp.wait_recv()

    def project(which, token_block, *relays):
        def body(step, _):
            for role, *steps in relays:
                advance_at(step, role, *steps)
            matrix = weights[step // 2, step % 2].reshape(width, block)
            projected[which, step] = jnp.dot(
                normed[token_block], matrix, preferred_element_type=jnp.float32
            ).astype(jnp.bfloat16)
            return 0

        lax.fori_loop(0, 4, body, 0)

    reach = taps_ref.shape[0]

    def recur(which, *relays):
        def body(step, _):
            for role, *steps in relays:
                advance_at(step, role, *steps)
            rows = pl.ds(pl.multiple_of(step * SEQ_LEN, SEQ_LEN), SEQ_LEN)
            for tile in range(tiles):
                part, lane = tile * LANES // block, tile * LANES % block
                lanes = slice(lane, lane + LANES)
                taps = taps_ref[
                    :, pl.ds(pl.multiple_of(y * quarter + tile * LANES, LANES), LANES)
                ].astype(jnp.float32)
                values = projected[which, part, rows, lanes].astype(jnp.float32)
                filtered = taps[reach - 1 : reach] * values
                for back in range(1, reach):
                    tap = taps[reach - 1 - back : reach - back]
                    filtered = filtered + tap * shift_down(values, back, 0.0)
                conved = filtered.astype(jnp.bfloat16)
                logits = jnp.dot(conved, maps[tile], preferred_element_type=jnp.float32)
                offset = offsets[which, rows, tile * LANES : (tile + 1) * LANES].astype(jnp.float32)
                steps = 1.0 / (1.0 + jnp.exp(-logits))
                rate = rate_ref[pl.ds(y * tiles + tile, 1), :]
                log_decay = steps[:, :LANES] * rate + offset
                decay = jnp.exp(log_decay)
                twice = -2.0 * log_decay
                series = 1.0 + twice * (
                    -1 / 2
                    + twice
                    * (1 / 6 + twice * (-1 / 24 + twice * (1 / 120 + twice * (-1 / 720 + twice * (1 / 5040)))))
                )
                lost = jnp.where(twice < 0.35, twice * series, 1.0 - decay * decay)
                state = jnp.sqrt(lost) * steps[:, LANES:] * conved.astype(jnp.float32)
                span = 1
                while span < SEQ_LEN:
                    state = state + decay * shift_down(state, span, 0.0)
                    if span * 2 < SEQ_LEN:
                        decay = decay * shift_down(decay, span, 1.0)
                    span *= 2
                gate = projected[which, 2 + part, rows, lanes].astype(jnp.float32)
                gelu = 0.5 * gate * (1.0 + lax.erf(gate * 0.7071067811865476))
                mixed[which, rows, tile * LANES : (tile + 1) * LANES] = (state * gelu).astype(jnp.bfloat16)
            return 0

        lax.fori_loop(0, tokens // SEQ_LEN, body, 0)

    project(0, y, (is_end, 4))
    recur(0, (is_mid, 5, 1, 2))
    first_pass.wait_recv()
    project(1, 1 - y, (is_mid, 5, 3, 3))
    offset_copy.wait_recv()
    recur(1, (is_end, 5))


    @pl.when(is_mid)
    def _():
        skewed(up)

    wait_y(2, 3)
    wait_x(2, 3, None, every)

    def mix_out(which, *relays):
        def body(step, _):
            for role, *steps in relays:
                advance_at(step, role, *steps)

            def term(place):
                matrix = weights[2, :, place].reshape(quarter, block)
                return jnp.dot(mixed[which], matrix, preferred_element_type=jnp.float32).astype(jnp.bfloat16)

            lanes = pl.ds(pl.multiple_of(step * block, block), block)
            per_half = n_fs // 2
            passed[which, :, lanes] = term(per_half * (1 - tp) + step)
            kept[which, :, lanes] = term(per_half * tp + step)
            return 0

        lax.fori_loop(0, n_fs // 2, body, 0)

    def mix_copy(which):
        return tp_copy(passed.at[which], got.at[which], 4 + which)

    mix_out(1, (is_end, 6))
    mix_copy(1).start()
    mix_out(0)
    mix_copy(0).start()

    def add_peer(step, _):
        rows = pl.ds(pl.multiple_of(step * CHUNK_ROWS, CHUNK_ROWS), CHUNK_ROWS)
        mid_send[rows, :] = (
            kept[1, rows, :].astype(jnp.float32) + got[1, rows, :].astype(jnp.float32)
        ).astype(jnp.bfloat16)
        return 0

    mix_copy(1).wait_recv()
    lax.fori_loop(0, tokens // CHUNK_ROWS, add_peer, 0)
    mid_copy = y_act(mid_send, mid_got, 6)
    mid_copy.start()
    y_start(lowers, (0,))

    for index in range(1, raises + 1):
        advance_both(up + index)
    mix_copy(0).wait_recv()
    relay(up + raises + 1, 1)
    start_after(up + raises + 1)
    relay(up + raises + 1, 2)

    @pl.when(is_mid)
    def _():
        relay(up + raises, 3)

    mid_copy.wait_recv()

    def add_own(step, _):
        rows = pl.ds(pl.multiple_of(step * CHUNK_ROWS, CHUNK_ROWS), CHUNK_ROWS)
        total = None
        for tile in range(lane_tiles):
            lanes = slice(tile * LANES, (tile + 1) * LANES)
            update = kept[0, rows, lanes].astype(jnp.float32) + got[0, rows, lanes].astype(jnp.float32)
            update = update + mid_got[rows, lanes].astype(jnp.float32)
            value = (stream_ref[rows, lanes].astype(jnp.float32) + update).astype(jnp.bfloat16)
            middle[rows, lanes] = value
            value = value.astype(jnp.float32)
            total = value * value if total is None else total + value * value
        square_own[1, rows, :] = total
        return 0

    lax.fori_loop(0, tokens // CHUNK_ROWS, add_own, 0)
    square_copy(1).start()
    square_copy(1).wait_recv()
    norm(middle, 1, second_gain_ref, normed_mid)
    second_tp, second_y, second_pass = block_copies(normed_mid, 11)
    second_y.start()
    second_tp.start()

    @pl.when(is_end)
    def _():
        relay(up + raises + 1, 3)

    for index in range(2, raises):
        advance_both(up + raises + index)
    down = up + 2 * raises
    wait_y(3, last_raise)
    for k in range(3, last_raise):
        if k == last_raise - 1:
            advance_both(down)

            @pl.when(is_mid)
            def _():
                skewed(down + 1)

        wait_x(k, k + 1, None, every)

    def lift(which, token_block, *relays):
        def body(step, _):
            for role, *steps in relays:
                advance_at(step, role, *steps)
            matrix = weights[3 + step // 2, step % 2].reshape(width, block)
            total = jnp.dot(normed_mid[token_block], matrix, preferred_element_type=jnp.float32)
            lanes = pl.ds(pl.multiple_of(step * block, block), block)
            activity[which, :, lanes] = jnp.square(jnp.maximum(total, 0.0)).astype(jnp.bfloat16)
            return 0

        lax.fori_loop(0, 2 * raises, body, 0)

    second_tp.wait_recv()
    lift(0, y)

    @pl.when(is_mid)
    def _():
        skewed(down + 2)

    advance_for(is_end, down + 1)

    second_y.wait_recv()
    y_start(lowers, (1,))
    second_pass.start()
    second_pass.wait_recv()
    lift(1, 1 - y, (is_end, down + 2))

    for index in range(3, raises):
        advance(down + index)

    depth = raises * quarter

    def lower(h, m):
        place = 2 * plane(m) + (y if h == 0 else 1 - y)

        def body(which, _):
            matrix = weights[last_raise:chunks, :, place].reshape(depth, block)
            partial[m, h, which] = jnp.dot(
                activity[which], matrix, preferred_element_type=jnp.float32
            ).astype(jnp.bfloat16)
            return 0

        lax.fori_loop(0, 2, body, 0)

    def is_owner(m):
        return low if m < 2 else jnp.logical_not(low)

    def owner_copy(h, m):
        slot = 14 + 2 * (m % 2) + h
        return tp_copy(partial.at[m, h], partial_got.at[m % 2, h], slot)

    def last_copy(h, m):
        slot = 18 + 2 * (m % 2)
        return remote(
            last_send.at[m % 2, h],
            last_got.at[m % 2, 1 - h],
            act_send.at[slot + h],
            act_recv.at[slot + 1 - h],
            y_peer,
        )

    def pass_on(h, m):
        @pl.when(jnp.logical_not(is_owner(m)))
        def _():
            owner_copy(h, m).start()

    def finish(h, m):
        @pl.when(is_owner(m))
        def _():
            owner_copy(h, m).wait_recv()

            def body(step, _):
                rows = pl.ds(pl.multiple_of(step * CHUNK_ROWS, CHUNK_ROWS), CHUNK_ROWS)
                last_send[m % 2, h, rows, :] = (
                    partial[m, h, 1, rows, :].astype(jnp.float32)
                    + partial_got[m % 2, h, 1, rows, :].astype(jnp.float32)
                ).astype(jnp.bfloat16)
                return 0

            lax.fori_loop(0, tokens // CHUNK_ROWS, body, 0)
            last_copy(h, m).start()

    def lanes_of(half):
        return slice(half * (block // 2), (half + 1) * (block // 2))

    def last_part(half, which):
        lanes = lanes_of(half)
        return tp_copy(
            partial.at[1, 1, which, :, lanes],
            partial_got.at[1, 1, which, :, lanes],
            (17, 22, 23, 24)[2 * half + which],
        )

    def last_half(half):
        lanes = lanes_of(half)
        return remote(
            last_send.at[1, 1, :, lanes],
            last_got.at[1, 0, :, lanes],
            act_send.at[(21, 25)[half]],
            act_recv.at[(20, 25)[half]],
            y_peer,
        )

    def half_wait(first, last, half):
        sample = weights.at[first:last, 0, 0, :, lanes_of(0)]
        count_wait(sample, x_recv.at[x_slot(first, 1, 1, half)])

    def send_half(half):
        lanes = lanes_of(half)

        @pl.when(low)
        def _():
            last_part(half, 1).wait_recv()

            def body(step, _):
                rows = pl.ds(pl.multiple_of(step * CHUNK_ROWS, CHUNK_ROWS), CHUNK_ROWS)
                last_send[1, 1, rows, lanes] = (
                    partial[1, 1, 1, rows, lanes].astype(jnp.float32)
                    + partial_got[1, 1, 1, rows, lanes].astype(jnp.float32)
                ).astype(jnp.bfloat16)
                return 0

            lax.fori_loop(0, tokens // CHUNK_ROWS, body, 0)
            last_half(half).start()

    def store_half(half, which, value):
        partial[1, 1, which, :, lanes_of(half)] = value.astype(jnp.bfloat16)

        @pl.when(jnp.logical_not(low))
        def _():
            last_part(half, which).start()

    def lower_last():
        place = 2 * plane(1) + 1 - y
        split = (raises - 1) * quarter
        advance(near + 2 * raises - 1)
        half_wait(last_raise, chunks, 0)
        for which in (1, 0):
            matrix = weights[last_raise:chunks, :, place, :, lanes_of(0)].reshape(depth, block // 2)
            store_half(0, which, jnp.dot(activity[which], matrix, preferred_element_type=jnp.float32))
        send_half(0)
        half_wait(last_raise, chunks - 1, 1)

        def early(which, _):
            matrix = weights[last_raise : chunks - 1, :, place, :, lanes_of(1)].reshape(split, block // 2)
            total[which] = jnp.dot(activity[which, :, :split], matrix, preferred_element_type=jnp.float32)
            return 0

        lax.fori_loop(0, 2, early, 0)
        half_wait(chunks - 1, chunks, 1)
        for which in (1, 0):
            matrix = weights[chunks - 1, :, place, :, lanes_of(1)].reshape(quarter, block // 2)
            term = jnp.dot(activity[which, :, split:], matrix, preferred_element_type=jnp.float32)
            store_half(1, which, total[which] + term)
        send_half(1)

    def close(h, mm):
        owned = mm + 2 * (1 - low.astype(jnp.int32))
        if (h, mm) == (0, 1):

            @pl.when(low)
            def _():
                last_half(0).wait_recv()
                last_half(1).wait_recv()

            @pl.when(jnp.logical_not(low))
            def _():
                last_copy(1, 3).wait_recv()

        else:
            last_copy(1 - h, mm).wait_recv()
        place = 2 * ((z % 2 + mm) % 2) + (y if h == 0 else 1 - y)
        lanes = pl.ds(pl.multiple_of(place * block, block), block)

        def body(step, _):
            rows = pl.ds(pl.multiple_of(step * CHUNK_ROWS, CHUNK_ROWS), CHUNK_ROWS)
            update = (
                partial[owned, h, 0, rows, :].astype(jnp.float32)
                + partial_got[mm, h, 0, rows, :].astype(jnp.float32)
                + last_got[mm, h, rows, :].astype(jnp.float32)
            )
            out_ref[rows, lanes] = (middle[rows, lanes].astype(jnp.float32) + update).astype(jnp.bfloat16)
            return 0

        lax.fori_loop(0, tokens // CHUNK_ROWS, body, 0)

    order = [(0, m) for m in range(4)] + [(1, m) for m in (0, 2, 3, 1)]
    far, near = down + raises, down + 2 * raises

    def first_far(index):
        relay(index, 2)
        start_after(index)

    @pl.when(is_mid)
    def _():
        first_far(far)
        relay(far - 1, 3)
        first_far(far + 1)
        relay(far, 3)

    advance_for(is_end, far)
    wait_y(last_raise, chunks)
    wait_x(last_raise, chunks, 0, every)
    for index, (h, m) in enumerate(order):
        if index == 2:

            @pl.when(is_mid)
            def _():
                first_far(far + 2)
                relay(far + 1, 3)

        if index == 4:

            @pl.when(is_mid)
            def _():
                relay(far + 2, 3)

        if index in (2, 4):
            advance_for(is_end, far + index // 2)
        if (h, m) == (1, 1):
            lower_last()
            continue
        if index >= 5:
            for step in range(raises) if index == 5 else range(raises, 2 * raises - 1):
                advance(near + step)
        if h == 1 and m:
            wait_x(last_raise, chunks, 1, (m,))
        lower(h, m)
        pass_on(h, m)
        if index and index < 5:
            finish(*order[index - 1])
        if index >= 4:
            finish(h, m)
    close(1, 0)
    close(0, 0)

    @pl.when(low)
    def _():
        last_part(0, 0).wait_recv()
        last_part(1, 0).wait_recv()

    close(1, 1)
    close(0, 1)

    count_wait(weights.at[:, :, 0], y_send.at[0])
    count_wait(weights.at[:, 0, 0:6], x_send.at[0])
    count_wait(weights.at[:, 0, 0:4], z_send.at[0])

    @pl.when(is_mid)
    def _():
        count_wait(weights.at[:, 0, 0:4], z_send.at[0])

    for copy in (first_tp, first_y, first_pass, second_tp, second_y, second_pass, offset_copy, mid_copy):
        copy.wait_send()
    for phase in range(2):
        square_copy(phase).wait_send()
        mix_copy(phase).wait_send()
    for h, m in order[:-1]:

        @pl.when(is_owner(m))
        def _():
            last_copy(h, m).wait_send()

        @pl.when(jnp.logical_not(is_owner(m)))
        def _():
            owner_copy(h, m).wait_send()

    @pl.when(low)
    def _():
        for half in range(2):
            last_half(half).wait_send()

    @pl.when(jnp.logical_not(low))
    def _():
        for half in range(2):
            for which in range(2):
                last_part(half, which).wait_send()


def whole_layer(
    stream,
    recurrent_norm_gain,
    feedforward_norm_gain,
    recurrent_input_weight,
    output_gate_weight,
    causal_filter_weight,
    decay_gate_matrix,
    input_gate_matrix,
    channel_decay_param,
    token_decay_offset,
    recurrent_output_weight,
    up_projection_weight,
    down_projection_weight,
):
    tokens, half_width = stream.shape
    width = 2 * half_width
    quarter = half_width // 2
    block, n_fs = quarter // 2, 8
    raises = up_projection_weight.shape[1] // half_width
    chunks = 3 + 2 * raises
    depth = raises * quarter
    tiles = quarter // LANES
    half_type, full_type = jnp.bfloat16, jnp.float32
    vmem = pl.BlockSpec(memory_space=pltpu.VMEM)
    anywhere = pl.BlockSpec(memory_space=pl.ANY)
    dma = pltpu.SemaphoreType.DMA
    return pl.pallas_call(
        whole_kernel,
        out_shape=jax.ShapeDtypeStruct((tokens, half_width), half_type),
        in_specs=[anywhere] * 13,
        out_specs=vmem,
        scratch_shapes=[
            pltpu.VMEM((tokens, half_width), half_type),
            pltpu.VMEM((tokens, half_width), full_type),
            pltpu.VMEM((width // LANES, LANES), full_type),
            pltpu.VMEM((width // LANES, LANES), full_type),
            pltpu.VMEM(causal_filter_weight.shape, half_type),
            pltpu.VMEM(decay_gate_matrix.shape, half_type),
            pltpu.VMEM(input_gate_matrix.shape, half_type),
            pltpu.VMEM((half_width // LANES, LANES), full_type),
            pltpu.VMEM((half_width // LANES, LANES), full_type),
            pltpu.VMEM((chunks, 2, n_fs, block, block), half_type),
            pltpu.VMEM((2, tokens, width), half_type),
            pltpu.VMEM((2, tokens, width), half_type),
            pltpu.VMEM((2, tokens, LANES), full_type),
            pltpu.VMEM((2, tokens, LANES), full_type),
            pltpu.VMEM((2, 4, tokens, block), half_type),
            pltpu.VMEM((2, tokens, quarter), half_type),
            pltpu.VMEM((2, tokens, quarter), half_type),
            pltpu.VMEM((tokens, quarter), half_type),
            pltpu.VMEM((tiles, LANES, 2 * LANES), half_type),
            pltpu.VMEM((2, tokens, half_width), half_type),
            pltpu.VMEM((2, tokens, half_width), half_type),
            pltpu.VMEM((2, tokens, half_width), half_type),
            pltpu.VMEM((tokens, half_width), half_type),
            pltpu.VMEM((tokens, half_width), half_type),
            pltpu.VMEM((tokens, half_width), half_type),
            pltpu.VMEM((2, tokens, depth), half_type),
            pltpu.VMEM((4, 2, 2, tokens, block), half_type),
            pltpu.VMEM((2, 2, 2, tokens, block), half_type),
            pltpu.VMEM((2, tokens, block // 2), full_type),
            pltpu.VMEM((2, 2, tokens, block), half_type),
            pltpu.VMEM((2, 2, tokens, block), half_type),
            dma((1,)),
            dma((1,)),
            dma((chunks + 4,)),
            dma((1,)),
            dma((6 * chunks + raises,)),
            dma((1,)),
            dma((raises + 8,)),
            dma((26,)),
            dma((26,)),
            dma((8,)),
        ],
        compiler_params=pltpu.CompilerParams(
            collective_id=0, has_side_effects=True, vmem_limit_bytes=67043328
        ),
        name="whole_layer",
    )(
        stream,
        token_decay_offset,
        recurrent_norm_gain.reshape(-1, LANES),
        feedforward_norm_gain.reshape(-1, LANES),
        causal_filter_weight,
        decay_gate_matrix,
        input_gate_matrix,
        channel_decay_param.reshape(-1, LANES),
        recurrent_input_weight,
        output_gate_weight,
        recurrent_output_weight,
        up_projection_weight,
        down_projection_weight,
    )


def fits_whole(sizes, stream, up_projection_weight, decay_gate_matrix):
    tokens, half_width = stream.shape
    return (
        sizes == (2, 8, 2)
        and half_width % (8 * LANES) == 0
        and tokens % (4 * SEQ_LEN) == 0
        and up_projection_weight.shape[1] % half_width == 0
        and up_projection_weight.shape[1] // half_width >= 3
        and LANES % decay_gate_matrix.shape[1] == 0
    )


def solution(mesh):
    in_specs = (
        P(("rep", "fs"), "tp"),
        P(),
        P(),
        P("fs", "tp"),
        P("fs", "tp"),
        P(None, "tp"),
        P("tp", None, None),
        P("tp", None, None),
        P("tp"),
        P(("rep", "fs"), "tp"),
        P("tp", "fs"),
        P("fs", "tp"),
        P("tp", "fs"),
    )
    out_specs = P(("rep", "fs"), "tp")
    sizes = tuple(mesh.shape[axis] for axis in ("rep", "fs", "tp"))

    def body(*args):
        if fits_whole(sizes, args[0], args[11], args[6]):
            return whole_layer(*args)
        return shards(sizes, *args)

    return jax.shard_map(
        body, mesh=mesh, in_specs=in_specs, out_specs=out_specs, check_vma=False
    )
```
